512 devices in a mesh: ep: 32 (over z, x), tp: 16 (over y, core).
Axes of the slice: x: 4, y: 8, z: 8, core: 2. Of those that a mesh axis runs over, the one named last changes fastest.
Arguments:
- queries: bfloat16 [8192, 2048], P('ep', 'tp'), may hold values from -9 to 9
- key_rows: bfloat16 [8192, 2048], P('ep', 'tp'), may hold values from -9 to 9
- values: bfloat16 [8192, 2048], P('ep', 'tp'), may hold values from -6 to 6
- second_scale: float32 [16], P('tp'), may hold values from 0.3 to 0.8
- head_gain: float32 [128], replicated, may hold values from 0.1 to 1.9
- out_weight: bfloat16 [2048, 2048], P(None, 'tp'), may hold values from -0.125 to 0.125
- routed_in: bfloat16 [8192, 2048], P('ep'), may hold values from -6 to 6
- routed_gain: float32 [2048], replicated, may hold values from 0.1 to 1.9
- expert_ids: int32 [8192, 2], P('ep'), may hold values from 0 to 31, all different within a row; in each aligned block of 256 rows (0 to 255, 256 to 511, ...) at most 32 rows name the same one
- group_logits: float32 [8192, 8], P('ep'), may hold values from -6 to 6
- inner_logits: float32 [8192, 2], P('ep'), may hold values from -6 to 6
- gate_weight: bfloat16 [32, 2048, 4096], P('ep', None, 'tp'), may hold values from -0.125 to 0.125
- up_weight: bfloat16 [32, 2048, 4096], P('ep', None, 'tp'), may hold values from -0.125 to 0.125
- down_weight: bfloat16 [32, 4096, 2048], P('ep', 'tp'), may hold values from -0.09375 to 0.09375
Outputs:
- mixer_out: bfloat16 [8192, 2048], P('ep', 'tp')
- routed_out: bfloat16 [8192, 2048], P('ep', 'tp')
The draws below stay inside these ranges and needn't reach their ends.
Inputs may be any that keep to these rules, and one draw needn't show every extreme that they name: `expert_ids`: the two ids of a row differ. In the rows of one device (aligned blocks of 256 rows) no expert is named by more than 32 rows, a bound that some block reaches.
All inputs are finite; a program needn't handle non-finite values.
Results may differ from the reference program's by a relative error of at most 0.018.
Values may be sent and summed in bfloat16 or wider, within the bound.
A program may use at most 128 MiB of HBM per device.

```python
import math
import jax
import jax.numpy as jnp
import numpy as np
from jax import lax

D = 2048
HEADS = 16
QK = 64
VD = 128
FF = 4096
TOPK = 2
GROUP_SIZE = 4
TM = 256
LA = 8192
TOKM = 8192
EXPERTS = 32
GROUPS = 8
CAP = 32
N_EP = 32
N_TP = 16


def base_field(key):
    spread = 1.32
    return jnp.clip(jax.random.normal(key, (LA, HEADS * 2 * QK), jnp.float32) * spread, -8.0, 8.0)


def draw_queries(key, part):
    field = base_field(jax.random.fold_in(key, 1))
    return field.astype(jnp.bfloat16)


def draw_key_rows(key, part):
    field = base_field(jax.random.fold_in(key, 2))
    return field.astype(jnp.bfloat16)


def level_of(key, dims, cuts, low, high):
    level, own = 1.0, jax.random.fold_in(key, 6)
    for axis_at, blocks in cuts:
        heights = jnp.exp(jax.random.uniform(jax.random.fold_in(own, axis_at), (blocks,), jnp.float32, low / len(cuts), high / len(cuts)))
        level = level * jnp.repeat(heights, dims[axis_at] // blocks).reshape([-1 if axis == axis_at else 1 for axis in range(len(dims))])
    return level


def shared_out(rng, own, number, rows, amount, top, most, slope):
    sequence = jax.random.permutation(rng, amount)
    heavy_load, ordinary = load_shares(amount, rows * top, most, slope, True), load_shares(amount, rows * top, most, slope, False)
    places = jnp.arange(amount)

    def named(tallies, rotation):
        used = int((tallies > 0).sum())
        fixed = max(1, used // 4)
        moved = fixed + (places - fixed + rotation * (used - fixed)) % max(1, amount - fixed)
        return jnp.zeros((amount,), jnp.int32).at[sequence[jnp.where(places < fixed, places, moved)]].set(jnp.asarray(tallies, jnp.int32))

    tallies = jnp.where(number % 4 == 0, named(heavy_load, number // 4), named(ordinary, number - number // 4 - 1))
    mixed = jax.random.permutation(jax.random.fold_in(own, 3), amount)
    donor, taker = mixed[0:amount // 2 * 2:2], mixed[1:amount // 2 * 2:2]
    room = jnp.minimum(tallies[donor] - 1, most - tallies[taker]) // 2
    room = jnp.where((donor == sequence[0]) | (taker == sequence[0]) | (tallies[taker] == 0), 0, jnp.maximum(room, 0))
    moved = jax.random.randint(jax.random.fold_in(own, 4), (amount // 2,), 0, 1 << 20) % (room + 1)
    tallies = tallies.at[donor].add(-moved).at[taker].add(moved)
    items = jnp.searchsorted(jnp.cumsum(tallies), jnp.arange(rows * top), side="right").astype(jnp.int32)
    listing = items.reshape(top, rows).T
    listing = listing[jax.random.permutation(jax.random.fold_in(own, 1), rows)]
    rotation = jax.random.randint(jax.random.fold_in(own, 2), (rows, 1), 0, top)
    return jnp.take_along_axis(listing, (jnp.arange(top)[None, :] + rotation) % top, axis=1)


def load_shares(number_of, total, reach, skew, full):
    loads = [(1 << 20) // math.isqrt(standing ** skew) + 1 for standing in range(1, number_of + 1)]
    largest = reach if full else min(reach, max(-(-total // number_of), total * loads[0] // sum(loads)))
    least = 1 if total - largest >= number_of - 1 else 0
    given, surplus = [largest] + [least] * (number_of - 1), total - largest - least * (number_of - 1)
    while surplus > 0:
        free = [i for i in range(1, number_of) if given[i] < largest] or [i for i in range(1, number_of) if given[i] < reach]
        whole, budget = sum([loads[i] for i in free]), surplus
        for i in free:
            addition = min(reach - given[i], max(1, budget * loads[i] // whole), surplus)
            given[i] = given[i] + addition
            surplus = surplus - addition
    return np.array(given)


def gaussian(own_key, extent, width, bound, pieces=(), held_as=jnp.bfloat16):
    entries = jax.random.normal(own_key, extent, jnp.float32) * width
    if len(pieces) > 0:
        entries = level_of(own_key, extent, pieces, -0.22, 0.18) * entries
    return jnp.clip(entries, min=-bound, max=bound).astype(held_as)


def setup_inputs(seed: int = 0) -> dict:
    seeds = jax.random.split(jax.random.key(seed), 15)
    queries = draw_queries(jax.random.fold_in(seeds[14], 71), 0)
    key_rows = draw_key_rows(jax.random.fold_in(seeds[14], 71), 0)
    values = gaussian(seeds[2], (LA, HEADS * VD), 1.0, 6.0, ((0, 32), (1, 16)))
    second_scale = jnp.clip(0.3 + 0.5 * jax.random.uniform(seeds[3], (HEADS,), jnp.float32) ** level_of(seeds[3], (HEADS,), ((0, 16),), -0.2, 0.2), 0.3, 0.8)
    head_gain = jnp.clip(1.0 + 0.18 * jax.random.normal(seeds[4], (VD,), jnp.float32), 0.1, 1.9)
    out_weight = gaussian(seeds[5], (HEADS * VD, D), (HEADS * VD) ** -0.5, 0.125, ((1, 16),))
    routed_in = gaussian(seeds[6], (TOKM, D), 1.0, 6.0, ((0, 32),))
    routed_gain = jnp.clip(1.0 + 0.18 * jax.random.normal(seeds[7], (D,), jnp.float32), 0.1, 1.9)
    expert_ids_keys = jax.random.split(jax.random.fold_in(seeds[8], 1), TOKM // TM)
    expert_ids_turns = jax.random.permutation(jax.random.fold_in(seeds[8], 3), TOKM // TM)
    expert_ids = jax.vmap(lambda own, number: shared_out(jax.random.fold_in(seeds[8], 2), own, number, TM, EXPERTS, TOPK, CAP, 2))(expert_ids_keys, expert_ids_turns).reshape((TOKM, TOPK))
    group_logits = gaussian(seeds[9], (TOKM, GROUPS), 1.5, 6.0, ((0, 32),), jnp.float32)
    inner_logits = gaussian(seeds[10], (TOKM, TOPK), 1.0, 6.0, ((0, 32),), jnp.float32)
    gate_weight = gaussian(seeds[11], (EXPERTS, D, FF), D ** -0.5, 0.125, ((0, 32), (2, 16)))
    up_weight = gaussian(seeds[12], (EXPERTS, D, FF), D ** -0.5, 0.125, ((0, 32), (2, 16)))
    down_weight = gaussian(seeds[13], (EXPERTS, FF, D), FF ** -0.5, 0.09375, ((0, 32), (1, 16)))
    return {"queries": queries, "key_rows": key_rows, "values": values, "second_scale": second_scale, "head_gain": head_gain, "out_weight": out_weight, "routed_in": routed_in, "routed_gain": routed_gain, "expert_ids": expert_ids, "group_logits": group_logits, "inner_logits": inner_logits, "gate_weight": gate_weight, "up_weight": up_weight, "down_weight": down_weight}


EPSILON = 1e-05

def head_block(query_block, key_block, value_block, scale_head, first_pos):
    scores = jnp.einsum('qmd,kmd->mqk', query_block, key_block) * QK ** (-0.5)
    query_pos = first_pos + jnp.arange(query_block.shape[0], dtype=jnp.int32)
    key_pos = jnp.arange(key_block.shape[0], dtype=jnp.int32)
    visible = query_pos[:, None] >= key_pos[None, :]
    scores = jnp.where(visible, scores, -jnp.inf)
    row_max = lax.optimization_barrier(jnp.max(scores, axis=-1, keepdims=True))
    exp_terms = jnp.exp(scores - row_max)
    denominator = lax.optimization_barrier(jnp.sum(exp_terms, axis=-1))
    rounded = lax.optimization_barrier(exp_terms.astype(jnp.bfloat16)).astype(jnp.float32)
    weighted = jnp.einsum('mqk,ke->mqe', rounded, value_block)
    mapped = weighted / denominator[..., None]
    return mapped[0] - scale_head * mapped[1]

def reference(queries, key_rows, values, second_scale, head_gain, out_weight, routed_in, routed_gain, expert_ids, group_logits, inner_logits, gate_weight, up_weight, down_weight):
    query_all = jnp.transpose(queries.astype(jnp.float32).reshape(LA, HEADS, 2, QK), (1, 0, 2, 3))
    key_all = jnp.transpose(key_rows.astype(jnp.float32).reshape(LA, HEADS, 2, QK), (1, 0, 2, 3))
    value_all = jnp.transpose(values.astype(jnp.float32).reshape(LA, HEADS, VD), (1, 0, 2))
    block_rows = min(512, LA)
    outputs = []
    for first_pos in range(0, LA, block_rows):
        limit = first_pos + block_rows

        def per_head(operands, first_pos=first_pos):
            query_head, key_head, value_head, scale_head = operands
            return head_block(query_head, key_head, value_head, scale_head, first_pos)
        outputs.append(lax.map(per_head, (query_all[:, first_pos:limit], key_all[:, :limit], value_all[:, :limit], second_scale)))
    difference = jnp.concatenate(outputs, axis=1)
    inv_norm = lax.rsqrt(lax.optimization_barrier(jnp.mean(difference * difference, axis=-1, keepdims=True)) + EPSILON)
    head_out = (difference * inv_norm * head_gain).astype(jnp.bfloat16)
    head_out = jnp.transpose(head_out, (1, 0, 2)).reshape(LA, HEADS * VD)
    mixer_out = jnp.dot(head_out, out_weight, preferred_element_type=jnp.float32).astype(jnp.bfloat16)
    source = routed_in.astype(jnp.float32)
    normed = (source * lax.rsqrt(lax.optimization_barrier(jnp.mean(source * source, axis=-1, keepdims=True)) + EPSILON) * routed_gain).astype(jnp.bfloat16)
    block_ids = expert_ids.reshape(N_EP, TM * TOPK)
    picked = (block_ids[..., None] == jnp.arange(EXPERTS, dtype=jnp.int32)).astype(jnp.int32)
    slot_index = lax.optimization_barrier(jnp.sum(jnp.cumsum(picked, axis=1) * picked, axis=-1)) - 1
    place_index = (jnp.arange(N_EP, dtype=jnp.int32)[:, None] * CAP + slot_index).reshape(-1).astype(jnp.int32)
    flat_ids = expert_ids.reshape(-1).astype(jnp.int32)
    owner_row = (jnp.arange(TOKM * TOPK, dtype=jnp.int32) // TOPK).astype(jnp.int32)
    slot_rows = jnp.zeros((EXPERTS, N_EP * CAP), jnp.int32).at[flat_ids, place_index].set(owner_row)

    def one_expert(operands):
        rows_of, gate_part, up_part, down_part = operands
        gathered = normed[rows_of]
        gate_act = jnp.dot(gathered, gate_part, preferred_element_type=jnp.float32)
        up_act = jnp.dot(gathered, up_part, preferred_element_type=jnp.float32)
        hidden = (jax.nn.silu(gate_act) * up_act).astype(jnp.bfloat16)
        split_hidden = hidden.reshape(N_EP * CAP, N_TP, FF // N_TP).astype(jnp.float32)
        split_down = down_part.reshape(N_TP, FF // N_TP, D).astype(jnp.float32)
        partial_value = jnp.einsum('rtf,tfd->trd', split_hidden, split_down)
        rounded = lax.optimization_barrier(partial_value.astype(jnp.bfloat16)).astype(jnp.float32)
        return lax.optimization_barrier(jnp.sum(rounded, axis=0)).astype(jnp.bfloat16)
    expert_out = lax.map(one_expert, (slot_rows, gate_weight, up_weight, down_weight))
    pair_out = expert_out[flat_ids, place_index].reshape(TOKM, TOPK, D)
    group_prob = jax.nn.softmax(group_logits, axis=-1)
    member = (expert_ids[..., None] // GROUP_SIZE == jnp.arange(GROUPS, dtype=jnp.int32)).astype(jnp.float32)
    group_pick = lax.optimization_barrier(jnp.sum(group_prob[:, None, :] * member, axis=-1))
    route_weight = group_pick * jax.nn.softmax(inner_logits, axis=-1)
    routed_out = lax.optimization_barrier(jnp.sum(route_weight[..., None] * pair_out.astype(jnp.float32), axis=1)).astype(jnp.bfloat16)
    return (mixer_out, routed_out)
```

```python
import jax
import jax.numpy as jnp
from jax import lax
from jax.experimental import pallas as pl
from jax.experimental.pallas import tpu as pltpu
from jax.sharding import Mesh
from jax.sharding import PartitionSpec as P

EPSILON = 1e-05
LOWEST = -1e30
GROUP_SIZE = 4
LANES = 128
CHUNKS = 4
F32 = jnp.float32
BF16 = jnp.bfloat16


def remote(src, dst, send_sem, recv_sem, **where):
    return pltpu.make_async_remote_copy(
        src_ref=src,
        dst_ref=dst,
        send_sem=send_sem,
        recv_sem=recv_sem,
        device_id=where,
        device_id_type=pl.DeviceIdType.MESH,
    )


def loop(first, last, body):
    def step(i, carry):
        body(i)
        return carry

    lax.fori_loop(first, last, step, 0)


def kernel(
    sizes,
    q_ref,
    k_ref,
    v_ref,
    scale_ref,
    hgain_ref,
    ow_hbm,
    rin_ref,
    rgain_ref,
    ids_ref,
    gl_ref,
    il_ref,
    gw_hbm,
    uw_hbm,
    dw_hbm,
    mix_ref,
    rout_ref,
    gw,
    uw,
    dw,
    ow,
    w_sem,
    pos0,
    pos1,
    rw0,
    rw1,
    disp,
    xs,
    parts,
    mate,
    rb_up,
    rb_dn,
    sb_up,
    sb_dn,
    ans,
    ret,
    a_send,
    a_recv,
    up_send,
    up_recv,
    dn_send,
    dn_recv,
    m_send,
    m_recv,
    pm_send,
    pm_recv,
    ru_send,
    ru_recv,
    rd_send,
    rd_recv,
    b_send,
    b_recv,
    qb,
    qs,
    kb,
    vb,
    acc,
    stat,
    o_out,
    o_in,
    stat_in,
    heads,
    q_send,
    q_recv,
    k_send,
    k_recv,
    v_send,
    v_recv,
    o_send,
    o_recv,
    s_send,
    s_recv,
    h_send,
    h_recv,
    hm_send,
    hm_recv,
):
    nz, nx, ny = sizes
    nep = nz * nx
    half_ring = ny // 2
    z, x, y, c = (lax.axis_index(name) for name in ("z", "x", "y", "c"))
    other = 1 - c
    e = z * nx + x
    t = y * 2 + c
    rows = rin_ref.shape[0]
    width = rin_ref.shape[1]
    total = xs.shape[2]
    cap = total // nep
    chunk = total // CHUNKS
    half = chunk // 2
    per_chunk = nep // CHUNKS
    y_next = lax.rem(y + 1, ny)
    y_prev = lax.rem(y + ny - 1, ny)

    def y_at(shift):
        return lax.rem(y + shift + ny, ny)

    def ep_at(shift):
        peer = lax.rem(e + shift, nep)
        return peer, peer // nx, lax.rem(peer, nx)

    barrier = pltpu.get_barrier_semaphore()

    def greet(r):
        _, pz, px = ep_at(r)
        pl.semaphore_signal(
            barrier, inc=1, device_id={"z": pz, "x": px}, device_id_type=pl.DeviceIdType.MESH
        )

    loop(1, nep, greet)

    def greet_y(r):
        pl.semaphore_signal(
            barrier, inc=1, device_id={"y": lax.rem(y + r, ny)}, device_id_type=pl.DeviceIdType.MESH
        )

    loop(1, ny, greet_y)
    pl.semaphore_signal(
        barrier, inc=1, device_id={"c": other}, device_id_type=pl.DeviceIdType.MESH
    )

    weight_copies = [
        pltpu.make_async_copy(src, dst, w_sem.at[i])
        for i, (src, dst) in enumerate(
            ((gw_hbm, gw), (uw_hbm, uw), (dw_hbm, dw), (ow_hbm, ow))
        )
    ]
    for copy in weight_copies:
        copy.start()

    own_cols = pl.ds(pl.multiple_of(t * LANES, LANES), LANES)
    source = rin_ref[...].astype(F32)
    inv = lax.rsqrt(jnp.sum(source * source, axis=-1, keepdims=True) * (1.0 / width) + EPSILON)
    normed = (rin_ref[:, own_cols].astype(F32) * inv * rgain_ref[:, own_cols]).astype(BF16)
    id0 = ids_ref[:, 0:1]
    id1 = ids_ref[:, 1:2]
    lane = lax.broadcasted_iota(jnp.int32, (rows, LANES), 1)
    pick0 = jnp.where(id0 == lane, 1.0, 0.0)
    pick1 = jnp.where(id1 == lane, 1.0, 0.0)
    below = jnp.where(
        lax.broadcasted_iota(jnp.int32, (rows, rows), 0)
        > lax.broadcasted_iota(jnp.int32, (rows, rows), 1),
        1.0,
        0.0,
    ).astype(BF16)
    before0 = jnp.dot(below, pick0.astype(BF16), preferred_element_type=F32)
    before1 = jnp.dot(below, pick1.astype(BF16), preferred_element_type=F32) + jnp.sum(
        pick0, axis=0, keepdims=True
    )
    pos0[...] = id0.astype(F32) * cap + jnp.sum(pick0 * before0, axis=1, keepdims=True)
    pos1[...] = id1.astype(F32) * cap + jnp.sum(pick1 * before1, axis=1, keepdims=True)

    def one_hot(pos):
        slots = lax.broadcasted_iota(jnp.int32, (rows, total), 1).astype(F32)
        return jnp.where(pos[...] == slots, 1.0, 0.0).astype(BF16)

    disp[...] = lax.dot_general(
        one_hot(pos0) + one_hot(pos1),
        normed,
        (((0,), (0,)), ((), ())),
        preferred_element_type=F32,
    ).astype(BF16)
    logits = gl_ref[...]
    group_exp = jnp.exp(logits - jnp.max(logits, axis=-1, keepdims=True))
    group_prob = group_exp / jnp.sum(group_exp, axis=-1, keepdims=True)
    groups = lax.broadcasted_iota(jnp.int32, logits.shape, 1)
    inner = il_ref[...]
    inner_exp = jnp.exp(inner - jnp.max(inner, axis=-1, keepdims=True))
    inner_prob = inner_exp / jnp.sum(inner_exp, axis=-1, keepdims=True)
    for number, weight in ((0, rw0), (1, rw1)):
        chosen = ids_ref[:, number : number + 1] // GROUP_SIZE
        picked = jnp.sum(jnp.where(chosen == groups, group_prob, 0.0), axis=1, keepdims=True)
        weight[...] = picked * inner_prob[:, number : number + 1]

    pl.semaphore_wait(barrier, nep - 1 + ny - 1 + 1)

    def slot_rows(index):
        return pl.ds(pl.multiple_of(index * cap, cap), cap)

    def dispatch(r):
        peer, pz, px = ep_at(r)
        return remote(
            disp.at[slot_rows(peer)],
            xs.at[y, c, slot_rows(e)],
            a_send.at[r],
            a_recv.at[r],
            z=pz,
            x=px,
        )

    loop(1, nep, lambda r: dispatch(r).start())
    xs[y, c, slot_rows(e), :] = disp[slot_rows(e), :]

    def query_copy(r):
        return remote(
            q_ref, qb.at[x], q_send.at[r], q_recv.at[r], x=lax.rem(x + r, nx)
        )

    for r in range(1, nx):
        query_copy(r).start()

    def key_copies(r):
        return (
            remote(k_ref, kb.at[z], k_send.at[r], k_recv.at[r], z=lax.rem(z + r, nz)),
            remote(v_ref, vb.at[z], v_send.at[r], v_recv.at[r], z=lax.rem(z + r, nz)),
        )

    for r in range(1, nz):

        @pl.when(z + r < nz)
        def _(r=r):
            for copy in key_copies(r):
                copy.start()

    maps = 2 * rows
    qk = LANES // 2
    keep_low = lax.broadcasted_iota(jnp.int32, (rows, LANES), 1) < qk

    def stack_query(value, index):
        scaled = value.astype(F32) * (qk ** (-0.5))
        qs[index, 0:rows, :] = jnp.where(keep_low, scaled, 0.0).astype(BF16)
        qs[index, rows:maps, :] = jnp.where(keep_low, 0.0, scaled).astype(BF16)

    def attend(key_block, value_block, masked):
        def one(index):
            scores = lax.dot_general(
                key_block[...],
                qs[index],
                (((1,), (1,)), ((), ())),
                preferred_element_type=F32,
            )
            if masked:
                key_pos = x * rows + lax.broadcasted_iota(jnp.int32, scores.shape, 0)
                column = lax.broadcasted_iota(jnp.int32, scores.shape, 1)
                query_pos = index * rows + jnp.where(column >= rows, column - rows, column)
                visible = query_pos >= key_pos
                scores = jnp.where(visible, scores, LOWEST)
                new_max = jnp.max(scores, axis=0, keepdims=True)
                terms = jnp.where(visible, jnp.exp(scores - new_max), 0.0)
                stat[index, 1:2, :] = jnp.sum(terms, axis=0, keepdims=True)
            else:
                old_max = stat[index, 0:1, :]
                new_max = jnp.maximum(old_max, jnp.max(scores, axis=0, keepdims=True))
                terms = jnp.exp(scores - new_max)
                factor = jnp.exp(old_max - new_max)
                stat[index, 1:2, :] = stat[index, 1:2, :] * factor + jnp.sum(
                    terms, axis=0, keepdims=True
                )
            stat[index, 0:1, :] = new_max
            weighted = lax.dot_general(
                value_block[...],
                terms.astype(BF16),
                (((0,), (0,)), ((), ())),
                preferred_element_type=F32,
            )
            if masked:
                acc[index] = weighted
            else:
                acc[index] = acc[index] * factor + weighted

        loop(0, nx, one)

    stack_query(q_ref[...], x)
    for r in range(1, nx):
        query_copy(r).wait_recv()
        from_x = lax.rem(x + nx - r, nx)
        stack_query(qb[from_x], from_x)
    stat[...] = jnp.zeros_like(stat)
    attend(k_ref, v_ref, True)

    def attend_far(r):
        if r < nz:

            @pl.when(z >= r)
            def _():
                for copy in key_copies(r):
                    copy.wait_recv()
                from_z = jnp.maximum(z - r, 0)
                attend(kb.at[from_z], vb.at[from_z], False)

    def wait_dispatch(r):
        from_e = lax.rem(e + nep - r, nep)
        remote(
            disp.at[slot_rows(0)],
            xs.at[y, c, slot_rows(from_e)],
            a_send.at[r],
            a_recv.at[r],
            z=z,
            x=x,
        ).wait_recv()

    loop(1, nep, wait_dispatch)

    def chunk_rows(k):
        return pl.ds(pl.multiple_of(k * chunk, chunk), chunk)

    def upper_rows(k):
        return pl.ds(pl.multiple_of(k * chunk, half), half)

    def lower_rows(k):
        return pl.ds(pl.multiple_of(k * chunk + half, half), half)

    def up_copy(s, k):
        where = upper_rows(k) if s == half_ring - 1 else chunk_rows(k)
        block = xs.at[y_at(-s), c, where]
        return remote(block, block, up_send.at[k, s], up_recv.at[k, s], y=y_next)

    def dn_copy(s, k):
        where = lower_rows(k) if s == half_ring - 1 else chunk_rows(k)
        block = xs.at[y_at(s), c, where]
        return remote(block, block, dn_send.at[k, s], dn_recv.at[k, s], y=y_prev)

    def up_arrival(s, k):
        where = upper_rows(k) if s == half_ring - 1 else chunk_rows(k)
        block = xs.at[y_at(-s - 1), c, where]
        return remote(block, block, up_send.at[k, s], up_recv.at[k, s], y=y_next)

    def dn_arrival(s, k):
        where = lower_rows(k) if s == half_ring - 1 else chunk_rows(k)
        block = xs.at[y_at(s + 1), c, where]
        return remote(block, block, dn_send.at[k, s], dn_recv.at[k, s], y=y_prev)

    def mate_blocks(k, core):
        blocks = [xs.at[y, core, chunk_rows(k)]]
        for s in range(half_ring):
            last = s == half_ring - 1
            blocks.append(
                xs.at[y_at(-s - 1), core, upper_rows(k) if last else chunk_rows(k)]
            )
            blocks.append(
                xs.at[y_at(s + 1), core, lower_rows(k) if last else chunk_rows(k)]
            )
        return blocks

    def mate_copy(number, k):
        block = mate_blocks(k, c)[number]
        return remote(block, block, m_send.at[k, number], m_recv.at[k, number], c=other)

    def mate_arrival(number, k):
        block = mate_blocks(k, other)[number]
        return remote(block, block, m_send.at[k, number], m_recv.at[k, number], c=other)

    def first_sends(k):
        up_copy(0, k).start()
        dn_copy(0, k).start()
        mate_copy(0, k).start()

    loop(0, CHUNKS, first_sends)
    attend_far(1)
    attend_far(2)
    for s in range(half_ring):

        def pass_on(k, s=s):
            up_arrival(s, k).wait_recv()
            if s + 1 < half_ring:
                up_copy(s + 1, k).start()
            mate_copy(2 * s + 1, k).start()
            dn_arrival(s, k).wait_recv()
            if s + 1 < half_ring:
                dn_copy(s + 1, k).start()
            mate_copy(2 * s + 2, k).start()

        loop(0, CHUNKS, pass_on)
        if s < half_ring - 1:
            attend_far(2 * s + 3)
            attend_far(2 * s + 4)
    for r in range(2 * half_ring + 1, nz):
        attend_far(r)

    def result_copies(r):
        to_x = lax.rem(x + r, nx)
        return (
            remote(o_out.at[to_x], o_in.at[x], o_send.at[r], o_recv.at[r], x=to_x),
            remote(stat.at[to_x], stat_in.at[x], s_send.at[r], s_recv.at[r], x=to_x),
        )

    def result_arrivals(r):
        from_x = lax.rem(x + nx - r, nx)
        return (
            remote(o_out.at[0], o_in.at[from_x], o_send.at[r], o_recv.at[r], x=x),
            remote(stat.at[0], stat_in.at[from_x], s_send.at[r], s_recv.at[r], x=x),
        )

    o_out[...] = acc[...].astype(BF16)
    for r in range(1, nx):
        for copy in result_copies(r):
            copy.start()
    o_in[x] = o_out[x]
    stat_in[x] = stat[x]

    for copy in weight_copies[:3]:
        copy.wait()

    def expert(k):
        for number in range(2 * half_ring + 1):
            mate_arrival(number, k).wait_recv()
        gate = jnp.zeros((chunk, gw.shape[1]), F32)
        up = jnp.zeros((chunk, gw.shape[1]), F32)
        for block in range(ny):
            both = jnp.concatenate(
                [xs[block, 0, chunk_rows(k), :], xs[block, 1, chunk_rows(k), :]], axis=1
            )
            depth = slice(block * 2 * LANES, (block + 1) * 2 * LANES)
            gate += jnp.dot(both, gw[depth, :], preferred_element_type=F32)
            up += jnp.dot(both, uw[depth, :], preferred_element_type=F32)
        hidden = (gate / (1.0 + jnp.exp(-gate)) * up).astype(BF16)
        for block in range(ny):
            columns = slice(block * 2 * LANES, (block + 1) * 2 * LANES)
            value = jnp.dot(hidden, dw[:, columns], preferred_element_type=F32).astype(BF16)
            parts[k, 0, block] = value[:, :LANES]
            parts[k, 1, block] = value[:, LANES:]
        part_copy(k).start()

    def part_copy(k):
        return remote(parts.at[k, other], mate.at[k], pm_send.at[k], pm_recv.at[k], c=other)

    full = slice(0, chunk)
    top = slice(0, half)
    bottom = slice(half, chunk)

    def chip_sum(k, target, where):
        return parts[k, c, target, where, :].astype(F32) + mate[k, target, where, :].astype(F32)

    def sum_up(k, d):
        where = top if d == half_ring else full
        return remote(
            sb_up.at[k, d - 1, where], rb_up.at[k, d - 1, where],
            ru_send.at[k, d - 1], ru_recv.at[k, d - 1], y=y_next,
        )

    def sum_dn(k, d):
        where = bottom if d == half_ring else full
        return remote(
            sb_dn.at[k, d - 1, where], rb_dn.at[k, d - 1, where],
            rd_send.at[k, d - 1], rd_recv.at[k, d - 1], y=y_prev,
        )

    def sum_step(k, d):
        if d == half_ring:
            sb_up[k, d - 1, top] = chip_sum(k, y_at(d), top).astype(BF16)
            sum_up(k, d).start()
            sb_dn[k, d - 1, bottom] = chip_sum(k, y_at(-d), bottom).astype(BF16)
            sum_dn(k, d).start()
            return
        sum_up(k, d + 1).wait_recv()
        if d + 1 == half_ring:
            sb_up[k, d - 1, top] = (
                chip_sum(k, y_at(d), top) + rb_up[k, d, top].astype(F32)
            ).astype(BF16)
            sb_up[k, d - 1, bottom] = chip_sum(k, y_at(d), bottom).astype(BF16)
        else:
            sb_up[k, d - 1] = (
                chip_sum(k, y_at(d), full) + rb_up[k, d].astype(F32)
            ).astype(BF16)
        sum_up(k, d).start()
        sum_dn(k, d + 1).wait_recv()
        if d + 1 == half_ring:
            sb_dn[k, d - 1, bottom] = (
                chip_sum(k, y_at(-d), bottom) + rb_dn[k, d, bottom].astype(F32)
            ).astype(BF16)
            sb_dn[k, d - 1, top] = chip_sum(k, y_at(-d), top).astype(BF16)
        else:
            sb_dn[k, d - 1] = (
                chip_sum(k, y_at(-d), full) + rb_dn[k, d].astype(F32)
            ).astype(BF16)
        sum_dn(k, d).start()

    def answer(k):
        sum_up(k, 1).wait_recv()
        sum_dn(k, 1).wait_recv()
        if half_ring > 1:
            ans[chunk_rows(k), :] = (
                chip_sum(k, y, full) + rb_up[k, 0].astype(F32) + rb_dn[k, 0].astype(F32)
            ).astype(BF16)
        else:
            ans[upper_rows(k), :] = (
                chip_sum(k, y, top) + rb_up[k, 0, top].astype(F32)
            ).astype(BF16)
            ans[lower_rows(k), :] = (
                chip_sum(k, y, bottom) + rb_dn[k, 0, bottom].astype(F32)
            ).astype(BF16)

        def reply(j):
            target = k * per_chunk + j

            @pl.when(target != e)
            def _():
                back_copy(target).start()

        loop(0, per_chunk, reply)

    def back_copy(target):
        return remote(
            ans.at[slot_rows(target)],
            ret.at[slot_rows(e)],
            b_send.at[target],
            b_recv.at[e],
            z=target // nx,
            x=lax.rem(target, nx),
        )

    def first_sum(k):
        part_copy(k).wait_recv()
        sum_step(k, half_ring)

    loop(0, 1, expert)

    def expert_and_sum(k):
        expert(k)
        first_sum(k - 1)

    loop(1, CHUNKS, expert_and_sum)
    loop(CHUNKS - 1, CHUNKS, first_sum)

    def head_copy(r):
        return remote(
            heads.at[y, c], heads.at[y, c], h_send.at[r], h_recv.at[r], y=lax.rem(y + r, ny)
        )

    def head_mate(r):
        block = heads.at[lax.rem(y + ny - r, ny), c]
        return remote(block, block, hm_send.at[r], hm_recv.at[r], c=other)

    def merge():
        for r in range(1, nx):
            for copy in result_arrivals(r):
                copy.wait_recv()
        top_max = stat_in[0, 0:1, :]
        for j in range(1, nx):
            top_max = jnp.maximum(top_max, stat_in[j, 0:1, :])
        denominator = jnp.zeros_like(top_max)
        weighted = jnp.zeros(o_in.shape[1:], F32)
        for j in range(nx):
            factor = jnp.exp(stat_in[j, 0:1, :] - top_max)
            denominator += factor * stat_in[j, 1:2, :]
            weighted += factor * o_in[j].astype(F32)
        mapped = weighted / denominator
        difference = mapped[:, :rows] - scale_ref[0:1, 0:1] * mapped[:, rows:]
        mean = jnp.sum(difference * difference, axis=0, keepdims=True) * (1.0 / LANES)
        head = difference * lax.rsqrt(mean + EPSILON) * hgain_ref[...]
        heads[y, c] = head.T.astype(BF16)
        for r in range(1, ny):
            head_copy(r).start()
        head_mate(0).start()

    merge()

    if half_ring > 1:
        loop(0, CHUNKS, lambda k: sum_step(k, half_ring - 1))

    for r in range(1, ny):
        arrived = heads.at[lax.rem(y + ny - r, ny), c]
        remote(arrived, arrived, h_send.at[r], h_recv.at[r], y=y_next).wait_recv()
        head_mate(r).start()

    for d in range(half_ring - 2, 0, -1):
        loop(0, CHUNKS, lambda k, d=d: sum_step(k, d))
    loop(0, CHUNKS, answer)
    ret[slot_rows(e), :] = ans[slot_rows(e), :]

    weight_copies[3].wait()
    for r in range(ny):
        arrived = heads.at[lax.rem(y + ny - r, ny), other]
        remote(arrived, arrived, hm_send.at[r], hm_recv.at[r], c=other).wait_recv()
    mixed = jnp.zeros((rows, LANES), F32)
    for block in range(ny):
        both = jnp.concatenate([heads[block, 0], heads[block, 1]], axis=1)
        mixed += jnp.dot(
            both, ow[block * 2 * LANES : (block + 1) * 2 * LANES, :], preferred_element_type=F32
        )
    mix_ref[...] = mixed.astype(BF16)

    def wait_back(r):
        from_e = lax.rem(e + nep - r, nep)
        remote(
            ans.at[slot_rows(0)],
            ret.at[slot_rows(from_e)],
            b_send.at[from_e],
            b_recv.at[from_e],
            z=z,
            x=x,
        ).wait_recv()

    loop(1, nep, wait_back)
    first = jnp.dot(one_hot(pos0), ret[...], preferred_element_type=F32)
    second = jnp.dot(one_hot(pos1), ret[...], preferred_element_type=F32)
    rout_ref[...] = (rw0[...] * first + rw1[...] * second).astype(BF16)

    def drain(r):
        dispatch(r).wait_send()
        peer, _, _ = ep_at(r)
        back_copy(peer).wait_send()

    loop(1, nep, drain)

    def drain_chunk(k):
        for s in range(half_ring):
            up_copy(s, k).wait_send()
            dn_copy(s, k).wait_send()
            sum_up(k, s + 1).wait_send()
            sum_dn(k, s + 1).wait_send()
        for number in range(2 * half_ring + 1):
            mate_copy(number, k).wait_send()
        part_copy(k).wait_send()

    loop(0, CHUNKS, drain_chunk)
    for r in range(1, nx):
        query_copy(r).wait_send()
        for copy in result_copies(r):
            copy.wait_send()
    for r in range(1, nz):

        @pl.when(z + r < nz)
        def _(r=r):
            for copy in key_copies(r):
                copy.wait_send()

    for r in range(1, ny):
        head_copy(r).wait_send()
    for r in range(ny):
        head_mate(r).wait_send()


def local(
    sizes,
    queries,
    key_rows,
    values,
    second_scale,
    head_gain,
    out_weight,
    routed_in,
    routed_gain,
    expert_ids,
    group_logits,
    inner_logits,
    gate_weight,
    up_weight,
    down_weight,
):
    nz, nx, ny = sizes
    nep = nz * nx
    rows = routed_in.shape[0]
    width = routed_in.shape[1]
    hidden = gate_weight.shape[2]
    cap = 2 * expert_ids.shape[1] * rows // nep
    total = nep * cap
    chunk = total // CHUNKS
    half_ring = ny // 2
    mates = 2 * half_ring + 1
    dma = pltpu.SemaphoreType.DMA
    vmem = pltpu.VMEM
    scratch = [
        vmem((width, hidden), BF16),
        vmem((width, hidden), BF16),
        vmem((hidden, width), BF16),
        vmem(out_weight.shape, BF16),
        dma((4,)),
        vmem((rows, 1), F32),
        vmem((rows, 1), F32),
        vmem((rows, 1), F32),
        vmem((rows, 1), F32),
        vmem((total, LANES), BF16),
        vmem((ny, 2, total, LANES), BF16),
        vmem((CHUNKS, 2, ny, chunk, LANES), BF16),
        vmem((CHUNKS, ny, chunk, LANES), BF16),
        vmem((CHUNKS, half_ring, chunk, LANES), BF16),
        vmem((CHUNKS, half_ring, chunk, LANES), BF16),
        vmem((CHUNKS, half_ring, chunk, LANES), BF16),
        vmem((CHUNKS, half_ring, chunk, LANES), BF16),
        vmem((total, LANES), BF16),
        vmem((total, LANES), BF16),
        dma((nep,)),
        dma((nep,)),
        dma((CHUNKS, half_ring)),
        dma((CHUNKS, half_ring)),
        dma((CHUNKS, half_ring)),
        dma((CHUNKS, half_ring)),
        dma((CHUNKS, mates)),
        dma((CHUNKS, mates)),
        dma((CHUNKS,)),
        dma((CHUNKS,)),
        dma((CHUNKS, half_ring)),
        dma((CHUNKS, half_ring)),
        dma((CHUNKS, half_ring)),
        dma((CHUNKS, half_ring)),
        dma((nep,)),
        dma((nep,)),
        vmem((nx, rows, LANES), BF16),
        vmem((nx, 2 * rows, LANES), BF16),
        vmem((nz, rows, LANES), BF16),
        vmem((nz, rows, LANES), BF16),
        vmem((nx, LANES, 2 * rows), F32),
        vmem((nx, 8, 2 * rows), F32),
        vmem((nx, LANES, 2 * rows), BF16),
        vmem((nx, LANES, 2 * rows), BF16),
        vmem((nx, 8, 2 * rows), F32),
        vmem((ny, 2, rows, LANES), BF16),
        dma((nx,)),
        dma((nx,)),
        dma((nz,)),
        dma((nz,)),
        dma((nz,)),
        dma((nz,)),
        dma((nx,)),
        dma((nx,)),
        dma((nx,)),
        dma((nx,)),
        dma((ny,)),
        dma((ny,)),
        dma((ny,)),
        dma((ny,)),
    ]
    whole = pl.BlockSpec(memory_space=pltpu.VMEM)
    far = pl.BlockSpec(memory_space=pl.ANY)
    return pl.pallas_call(
        lambda *refs: kernel(sizes, *refs),
        out_shape=(
            jax.ShapeDtypeStruct((rows, LANES), BF16),
            jax.ShapeDtypeStruct((rows, LANES), BF16),
        ),
        in_specs=[whole, whole, whole, whole, whole, far, whole, whole, whole, whole, whole, far, far, far],
        out_specs=(whole, whole),
        scratch_shapes=scratch,
        compiler_params=pltpu.CompilerParams(
            collective_id=0, has_side_effects=True, vmem_limit_bytes=60 * 1024 * 1024
        ),
    )(
        queries,
        key_rows,
        values,
        second_scale.reshape(1, 1),
        head_gain.reshape(-1, 1),
        out_weight,
        routed_in,
        routed_gain.reshape(1, -1),
        expert_ids,
        group_logits,
        inner_logits,
        gate_weight[0],
        up_weight[0],
        down_weight[0],
    )


def build(mesh, sizes):
    nz, nx, ny = sizes
    finer = Mesh(mesh.devices.reshape(nz, nx, ny, 2), ("z", "x", "y", "c"))
    ep, tp = ("z", "x"), ("y", "c")
    placed = (
        P(ep, tp),
        P(ep, tp),
        P(ep, tp),
        P(tp),
        P(),
        P(None, tp),
        P(ep, None),
        P(),
        P(ep, None),
        P(ep, None),
        P(ep, None),
        P(ep, None, tp),
        P(ep, None, tp),
        P(ep, tp, None),
    )
    return jax.shard_map(
        lambda *args: local(sizes, *args),
        mesh=finer,
        in_specs=placed,
        out_specs=(P(ep, tp), P(ep, tp)),
        check_vma=False,
    )


def solution(mesh):
    return build(mesh, (8, 4, mesh.shape["tp"] // 2))
```

```python
import jax
import jax.numpy as jnp
from jax import lax
from jax.experimental import pallas as pl
from jax.experimental.pallas import tpu as pltpu
from jax.sharding import Mesh
from jax.sharding import PartitionSpec as P

EPSILON = 1e-05
LOWEST = -1e30
GROUP_SIZE = 4
LANES = 128
CHUNKS = 4
F32 = jnp.float32
BF16 = jnp.bfloat16


def remote(src, dst, send_sem, recv_sem, **where):
    return pltpu.make_async_remote_copy(
        src_ref=src,
        dst_ref=dst,
        send_sem=send_sem,
        recv_sem=recv_sem,
        device_id=where,
        device_id_type=pl.DeviceIdType.MESH,
    )


def loop(first, last, body):
    def step(i, carry):
        body(i)
        return carry

    lax.fori_loop(first, last, step, 0)


def kernel(
    sizes,
    q_hbm,
    k_hbm,
    v_hbm,
    scale_ref,
    hgain_ref,
    ow_hbm,
    rin_hbm,
    rgain_ref,
    ids_ref,
    gl_ref,
    il_ref,
    gw_hbm,
    uw_hbm,
    dw_hbm,
    mix_ref,
    rout_ref,
    gw,
    uw,
    dw,
    ow,
    rin,
    w_sem,
    i_sem,
    pos,
    weight,
    disp,
    xs,
    parts,
    mate,
    rb_up,
    rb_dn,
    sb_up,
    sb_dn,
    ans,
    ret,
    a_send,
    a_recv,
    up_send,
    up_recv,
    dn_send,
    dn_recv,
    m_send,
    m_recv,
    pm_send,
    pm_recv,
    ru_send,
    ru_recv,
    rd_send,
    rd_recv,
    b_send,
    b_recv,
    qb,
    qs,
    kb,
    vb,
    acc,
    stat,
    o_out,
    o_in,
    stat_in,
    heads,
    q_send,
    q_recv,
    k_send,
    k_recv,
    v_send,
    v_recv,
    o_send,
    o_recv,
    s_send,
    s_recv,
    hu_send,
    hu_recv,
    hd_send,
    hd_recv,
    hm_send,
    hm_recv,
):
    nz, nx, ny = sizes
    nep = nz * nx
    half_ring = ny // 2
    z, x, y, c = (lax.axis_index(name) for name in ("z", "x", "y", "c"))
    other = 1 - c
    e = z * nx + x
    t = y * 2 + c
    rows = rin.shape[0]
    width = rin.shape[1]
    total = xs.shape[2]
    cap = total // nep
    chunk = total // CHUNKS
    half = chunk // 2
    per_chunk = nep // CHUNKS
    y_next = lax.rem(y + 1, ny)
    y_prev = lax.rem(y + ny - 1, ny)

    def y_at(shift):
        return lax.rem(y + shift + ny, ny)

    group = z // (nz // CHUNKS)

    def nearby(j):
        return lax.rem(group + j + j // 2 - 2 * (j // 3), CHUNKS)

    def each_other(first, count, body):
        def one(i):
            @pl.when(first + i != e)
            def _():
                body(first + i)

        loop(0, count, one)

    barrier = pltpu.get_barrier_semaphore()

    def greet(peer):
        pl.semaphore_signal(
            barrier,
            inc=1,
            device_id={"z": peer // nx, "x": lax.rem(peer, nx)},
            device_id_type=pl.DeviceIdType.MESH,
        )

    each_other(0, nep, greet)

    def greet_y(r):
        pl.semaphore_signal(
            barrier, inc=1, device_id={"y": lax.rem(y + r, ny)}, device_id_type=pl.DeviceIdType.MESH
        )

    loop(1, ny, greet_y)
    pl.semaphore_signal(
        barrier, inc=1, device_id={"c": other}, device_id_type=pl.DeviceIdType.MESH
    )

    input_copies = [
        pltpu.make_async_copy(src, dst, i_sem.at[i])
        for i, (src, dst) in enumerate(
            ((rin_hbm, rin), (q_hbm, qb.at[x]), (k_hbm, kb.at[z]), (v_hbm, vb.at[z]))
        )
    ]
    weight_copies = [
        pltpu.make_async_copy(src, dst, w_sem.at[i])
        for i, (src, dst) in enumerate(
            ((gw_hbm, gw), (uw_hbm, uw), (dw_hbm, dw), (ow_hbm, ow))
        )
    ]
    for copy in input_copies + weight_copies:
        copy.start()

    ids = ids_ref[...]
    shape = (nep, rows)
    expert_row = lax.broadcasted_iota(jnp.int32, shape, 0)
    picks = [jnp.where(ids[i : i + 1, :] == expert_row, 1.0, 0.0) for i in range(2)]
    earlier = jnp.where(
        lax.broadcasted_iota(jnp.int32, (rows, rows), 0)
        < lax.broadcasted_iota(jnp.int32, (rows, rows), 1),
        1.0,
        0.0,
    ).astype(BF16)
    before = [jnp.dot(pick.astype(BF16), earlier, preferred_element_type=F32) for pick in picks]
    before[1] += jnp.sum(picks[0], axis=1, keepdims=True)
    logits = gl_ref[...]
    group_exp = jnp.exp(logits - jnp.max(logits, axis=0, keepdims=True))
    group_prob = group_exp / jnp.sum(group_exp, axis=0, keepdims=True)
    group_row = lax.broadcasted_iota(jnp.int32, logits.shape, 0)
    inner = il_ref[...]
    inner_exp = jnp.exp(inner - jnp.max(inner, axis=0, keepdims=True))
    inner_prob = inner_exp / jnp.sum(inner_exp, axis=0, keepdims=True)
    for i in range(2):
        pos[i : i + 1, :] = ids[i : i + 1, :].astype(F32) * cap + jnp.sum(
            picks[i] * before[i], axis=0, keepdims=True
        )
        chosen = ids[i : i + 1, :] // GROUP_SIZE == group_row
        picked = jnp.sum(jnp.where(chosen, group_prob, 0.0), axis=0, keepdims=True)
        weight[i : i + 1, :] = picked * inner_prob[i : i + 1, :]

    def one_hot(i):
        slots = lax.broadcasted_iota(jnp.int32, (total, rows), 0).astype(F32)
        return jnp.where(pos[i : i + 1, :] == slots, 1.0, 0.0).astype(BF16)

    own_cols = pl.ds(pl.multiple_of(t * LANES, LANES), LANES)
    input_copies[0].wait()
    source = rin[...].astype(F32)
    inv = lax.rsqrt(jnp.sum(source * source, axis=-1, keepdims=True) * (1.0 / width) + EPSILON)
    normed = (rin[:, own_cols].astype(F32) * inv * rgain_ref[:, own_cols]).astype(BF16)
    disp[...] = jnp.dot(
        one_hot(0) + one_hot(1), normed, preferred_element_type=F32
    ).astype(BF16)
    for copy in input_copies[1:]:
        copy.wait()

    pl.semaphore_wait(barrier, nep - 1 + ny - 1 + 1)

    def slot_rows(index):
        return pl.ds(pl.multiple_of(index * cap, cap), cap)

    def dispatch(peer):
        return remote(
            disp.at[slot_rows(peer)],
            xs.at[y, c, slot_rows(e)],
            a_send.at[peer],
            a_recv.at[e],
            z=peer // nx,
            x=lax.rem(peer, nx),
        )

    loop(
        0,
        CHUNKS,
        lambda j: each_other(
            nearby(j) * per_chunk, per_chunk, lambda peer: dispatch(peer).start()
        ),
    )
    xs[y, c, slot_rows(e), :] = disp[slot_rows(e), :]

    def query_copy(r):
        return remote(
            qb.at[x], qb.at[x], q_send.at[r], q_recv.at[r], x=lax.rem(x + r, nx)
        )

    reach = nz // 2

    def key_copies(block, r, to_z):
        return (
            remote(kb.at[block], kb.at[block], k_send.at[r], k_recv.at[r], z=to_z),
            remote(vb.at[block], vb.at[block], v_send.at[r], v_recv.at[r], z=to_z),
        )

    def chain_copies(r):
        return key_copies(jnp.maximum(z - r + 1, 0), r, jnp.minimum(z + 1, nz - 1))

    def far_copies(r):
        return key_copies(z, r, lax.rem(z + r, nz))

    def chain_send(r):
        @pl.when((z + 1 < nz) & (z - r + 1 >= 0))
        def _():
            for copy in chain_copies(r):
                copy.start()

    chain_send(1)
    for r in range(reach + 1, nz):

        @pl.when(z + r < nz)
        def _(r=r):
            for copy in far_copies(r):
                copy.start()

    for r in range(1, nx):
        query_copy(r).start()

    maps = 2 * rows
    qk = LANES // 2
    keep_low = lax.broadcasted_iota(jnp.int32, (rows, LANES), 1) < qk

    def stack_query(value, index):
        scaled = value.astype(F32) * (qk ** (-0.5))
        qs[index, 0:rows, :] = jnp.where(keep_low, scaled, 0.0).astype(BF16)
        qs[index, rows:maps, :] = jnp.where(keep_low, 0.0, scaled).astype(BF16)

    def attend(key_block, value_block, masked):
        def one(index):
            scores = lax.dot_general(
                key_block[...],
                qs[index],
                (((1,), (1,)), ((), ())),
                preferred_element_type=F32,
            )
            if masked:
                key_pos = x * rows + lax.broadcasted_iota(jnp.int32, scores.shape, 0)
                column = lax.broadcasted_iota(jnp.int32, scores.shape, 1)
                query_pos = index * rows + jnp.where(column >= rows, column - rows, column)
                visible = query_pos >= key_pos
                scores = jnp.where(visible, scores, LOWEST)
                new_max = jnp.max(scores, axis=0, keepdims=True)
                terms = jnp.where(visible, jnp.exp(scores - new_max), 0.0)
                stat[index, 1:2, :] = jnp.sum(terms, axis=0, keepdims=True)
            else:
                old_max = stat[index, 0:1, :]
                new_max = jnp.maximum(old_max, jnp.max(scores, axis=0, keepdims=True))
                terms = jnp.exp(scores - new_max)
                factor = jnp.exp(old_max - new_max)
                stat[index, 1:2, :] = stat[index, 1:2, :] * factor + jnp.sum(
                    terms, axis=0, keepdims=True
                )
            stat[index, 0:1, :] = new_max
            weighted = lax.dot_general(
                value_block[...],
                terms.astype(BF16),
                (((0,), (0,)), ((), ())),
                preferred_element_type=F32,
            )
            if masked:
                acc[index] = weighted
            else:
                acc[index] = acc[index] * factor + weighted

        loop(0, nx, one)

    def own_attention():
        stack_query(qb[x], x)
        for r in range(1, nx):
            query_copy(r).wait_recv()
            from_x = lax.rem(x + nx - r, nx)
            stack_query(qb[from_x], from_x)
        stat[...] = jnp.zeros_like(stat)
        attend(kb.at[z], vb.at[z], True)

    def attend_far(r):
        @pl.when(z >= r)
        def _():
            from_z = jnp.maximum(z - r, 0)
            for copy in key_copies(from_z, r, z):
                copy.wait_recv()
            if r < reach:
                chain_send(r + 1)
            attend(kb.at[from_z], vb.at[from_z], False)

    def wait_dispatch(peer):
        remote(
            disp.at[slot_rows(0)],
            xs.at[y, c, slot_rows(peer)],
            a_send.at[peer],
            a_recv.at[peer],
            z=z,
            x=x,
        ).wait_recv()

    def chunk_rows(k):
        return pl.ds(pl.multiple_of(k * chunk, chunk), chunk)

    def upper_rows(k):
        return pl.ds(pl.multiple_of(k * chunk, half), half)

    def lower_rows(k):
        return pl.ds(pl.multiple_of(k * chunk + half, half), half)

    def up_copy(s, k):
        where = upper_rows(k) if s == half_ring - 1 else chunk_rows(k)
        block = xs.at[y_at(-s), c, where]
        return remote(block, block, up_send.at[k, s], up_recv.at[k, s], y=y_next)

    def dn_copy(s, k):
        where = lower_rows(k) if s == half_ring - 1 else chunk_rows(k)
        block = xs.at[y_at(s), c, where]
        return remote(block, block, dn_send.at[k, s], dn_recv.at[k, s], y=y_prev)

    def up_arrival(s, k):
        where = upper_rows(k) if s == half_ring - 1 else chunk_rows(k)
        block = xs.at[y_at(-s - 1), c, where]
        return remote(block, block, up_send.at[k, s], up_recv.at[k, s], y=y_next)

    def dn_arrival(s, k):
        where = lower_rows(k) if s == half_ring - 1 else chunk_rows(k)
        block = xs.at[y_at(s + 1), c, where]
        return remote(block, block, dn_send.at[k, s], dn_recv.at[k, s], y=y_prev)

    def mate_blocks(k, core):
        blocks = [xs.at[y, core, chunk_rows(k)]]
        for s in range(half_ring):
            last = s == half_ring - 1
            blocks.append(
                xs.at[y_at(-s - 1), core, upper_rows(k) if last else chunk_rows(k)]
            )
            blocks.append(
                xs.at[y_at(s + 1), core, lower_rows(k) if last else chunk_rows(k)]
            )
        return blocks

    def mate_copy(number, k):
        block = mate_blocks(k, c)[number]
        return remote(block, block, m_send.at[k, number], m_recv.at[k, number], c=other)

    def mate_arrival(number, k):
        block = mate_blocks(k, other)[number]
        return remote(block, block, m_send.at[k, number], m_recv.at[k, number], c=other)

    def first_sends(j):
        k = nearby(j)
        each_other(k * per_chunk, per_chunk, wait_dispatch)
        up_copy(0, k).start()
        dn_copy(0, k).start()
        mate_copy(0, k).start()

    def pass_on(s):
        def one(j):
            k = nearby(j)
            up_arrival(s, k).wait_recv()
            if s + 1 < half_ring:
                up_copy(s + 1, k).start()
            mate_copy(2 * s + 1, k).start()
            dn_arrival(s, k).wait_recv()
            if s + 1 < half_ring:
                dn_copy(s + 1, k).start()
            mate_copy(2 * s + 2, k).start()

        loop(0, CHUNKS, one)

    loop(0, CHUNKS, first_sends)
    own_attention()
    attend_far(1)
    pass_on(0)
    attend_far(2)
    attend_far(3)
    pass_on(1)
    attend_far(4)
    attend_far(5)
    pass_on(2)
    attend_far(6)
    attend_far(7)

    def result_copies(r):
        to_x = lax.rem(x + r, nx)
        return (
            remote(o_out.at[to_x], o_in.at[x], o_send.at[r], o_recv.at[r], x=to_x),
            remote(stat.at[to_x], stat_in.at[x], s_send.at[r], s_recv.at[r], x=to_x),
        )

    def result_arrivals(r):
        from_x = lax.rem(x + nx - r, nx)
        return (
            remote(o_out.at[0], o_in.at[from_x], o_send.at[r], o_recv.at[r], x=x),
            remote(stat.at[0], stat_in.at[from_x], s_send.at[r], s_recv.at[r], x=x),
        )

    o_out[...] = acc[...].astype(BF16)
    for r in range(1, nx):
        for copy in result_copies(r):
            copy.start()
    o_in[x] = o_out[x]
    stat_in[x] = stat[x]

    pass_on(3)
    for copy in weight_copies[:3]:
        copy.wait()

    def expert(j):
        k = nearby(j)
        for number in range(2 * half_ring + 1):
            mate_arrival(number, k).wait_recv()
        gate = jnp.zeros((chunk, gw.shape[1]), F32)
        up = jnp.zeros((chunk, gw.shape[1]), F32)
        for block in range(ny):
            both = jnp.concatenate(
                [xs[block, 0, chunk_rows(k), :], xs[block, 1, chunk_rows(k), :]], axis=1
            )
            depth = slice(block * 2 * LANES, (block + 1) * 2 * LANES)
            gate += jnp.dot(both, gw[depth, :], preferred_element_type=F32)
            up += jnp.dot(both, uw[depth, :], preferred_element_type=F32)
        hidden = (gate / (1.0 + jnp.exp(-gate)) * up).astype(BF16)
        for block in range(ny):
            columns = slice(block * 2 * LANES, (block + 1) * 2 * LANES)
            value = jnp.dot(hidden, dw[:, columns], preferred_element_type=F32).astype(BF16)
            parts[k, 0, block] = value[:, :LANES]
            parts[k, 1, block] = value[:, LANES:]
        part_copy(k).start()

    def part_copy(k):
        return remote(parts.at[k, other], mate.at[k], pm_send.at[k], pm_recv.at[k], c=other)

    full = slice(0, chunk)
    top = slice(0, half)
    bottom = slice(half, chunk)

    def chip_sum(k, target, where):
        return parts[k, c, target, where, :].astype(F32) + mate[k, target, where, :].astype(F32)

    def sum_up(k, d):
        where = top if d == half_ring else full
        return remote(
            sb_up.at[k, d - 1, where], rb_up.at[k, d - 1, where],
            ru_send.at[k, d - 1], ru_recv.at[k, d - 1], y=y_next,
        )

    def sum_dn(k, d):
        where = bottom if d == half_ring else full
        return remote(
            sb_dn.at[k, d - 1, where], rb_dn.at[k, d - 1, where],
            rd_send.at[k, d - 1], rd_recv.at[k, d - 1], y=y_prev,
        )

    def sum_step(k, d):
        if d == half_ring:
            sb_up[k, d - 1, top] = chip_sum(k, y_at(d), top).astype(BF16)
            sum_up(k, d).start()
            sb_dn[k, d - 1, bottom] = chip_sum(k, y_at(-d), bottom).astype(BF16)
            sum_dn(k, d).start()
            return
        sum_up(k, d + 1).wait_recv()
        if d + 1 == half_ring:
            sb_up[k, d - 1, top] = (
                chip_sum(k, y_at(d), top) + rb_up[k, d, top].astype(F32)
            ).astype(BF16)
            sb_up[k, d - 1, bottom] = chip_sum(k, y_at(d), bottom).astype(BF16)
        else:
            sb_up[k, d - 1] = (
                chip_sum(k, y_at(d), full) + rb_up[k, d].astype(F32)
            ).astype(BF16)
        sum_up(k, d).start()
        sum_dn(k, d + 1).wait_recv()
        if d + 1 == half_ring:
            sb_dn[k, d - 1, bottom] = (
                chip_sum(k, y_at(-d), bottom) + rb_dn[k, d, bottom].astype(F32)
            ).astype(BF16)
            sb_dn[k, d - 1, top] = chip_sum(k, y_at(-d), top).astype(BF16)
        else:
            sb_dn[k, d - 1] = (
                chip_sum(k, y_at(-d), full) + rb_dn[k, d].astype(F32)
            ).astype(BF16)
        sum_dn(k, d).start()

    def answer(k):
        sum_up(k, 1).wait_recv()
        sum_dn(k, 1).wait_recv()
        if half_ring > 1:
            ans[chunk_rows(k), :] = (
                chip_sum(k, y, full) + rb_up[k, 0].astype(F32) + rb_dn[k, 0].astype(F32)
            ).astype(BF16)
        else:
            ans[upper_rows(k), :] = (
                chip_sum(k, y, top) + rb_up[k, 0, top].astype(F32)
            ).astype(BF16)
            ans[lower_rows(k), :] = (
                chip_sum(k, y, bottom) + rb_dn[k, 0, bottom].astype(F32)
            ).astype(BF16)

        each_other(k * per_chunk, per_chunk, lambda target: back_copy(target).start())

    def back_copy(target):
        return remote(
            ans.at[slot_rows(target)],
            ret.at[slot_rows(e)],
            b_send.at[target],
            b_recv.at[e],
            z=target // nx,
            x=lax.rem(target, nx),
        )

    def first_sum(j):
        k = nearby(j)
        part_copy(k).wait_recv()
        sum_step(k, half_ring)

    loop(0, 1, expert)

    def expert_and_sum(j):
        expert(j)
        first_sum(j - 1)

    loop(1, CHUNKS, expert_and_sum)
    loop(CHUNKS - 1, CHUNKS, first_sum)

    top_rows = pl.ds(0, rows // 2)
    low_rows = pl.ds(rows // 2, rows // 2)
    all_rows = pl.ds(0, rows)

    def head_up(s, hop):
        where = top_rows if s == half_ring - 1 else all_rows
        block = heads.at[y_at(-s - hop), c, where]
        return remote(block, block, hu_send.at[s], hu_recv.at[s], y=y_next)

    def head_dn(s, hop):
        where = low_rows if s == half_ring - 1 else all_rows
        block = heads.at[y_at(s + hop), c, where]
        return remote(block, block, hd_send.at[s], hd_recv.at[s], y=y_prev)

    def head_mate(number, core):
        s = (number - 1) // 2
        last = number > 0 and s == half_ring - 1
        if number == 0:
            block = heads.at[y, core]
        elif number % 2 == 1:
            block = heads.at[y_at(-s - 1), core, top_rows if last else all_rows]
        else:
            block = heads.at[y_at(s + 1), core, low_rows if last else all_rows]
        return remote(block, block, hm_send.at[number], hm_recv.at[number], c=other)

    def head_pass(s):
        head_up(s, 1).wait_recv()
        if s + 1 < half_ring:
            head_up(s + 1, 0).start()
        head_mate(2 * s + 1, c).start()
        head_dn(s, 1).wait_recv()
        if s + 1 < half_ring:
            head_dn(s + 1, 0).start()
        head_mate(2 * s + 2, c).start()

    def merge():
        for r in range(1, nx):
            for copy in result_arrivals(r):
                copy.wait_recv()
        top_max = stat_in[0, 0:1, :]
        for j in range(1, nx):
            top_max = jnp.maximum(top_max, stat_in[j, 0:1, :])
        denominator = jnp.zeros_like(top_max)
        weighted = jnp.zeros(o_in.shape[1:], F32)
        for j in range(nx):
            factor = jnp.exp(stat_in[j, 0:1, :] - top_max)
            denominator += factor * stat_in[j, 1:2, :]
            weighted += factor * o_in[j].astype(F32)
        mapped = weighted / denominator
        difference = mapped[:, :rows] - scale_ref[0:1, 0:1] * mapped[:, rows:]
        mean = jnp.sum(difference * difference, axis=0, keepdims=True) * (1.0 / LANES)
        head = difference * lax.rsqrt(mean + EPSILON)
        heads[y, c] = (head.T * hgain_ref[...]).astype(BF16)
        head_up(0, 0).start()
        head_dn(0, 0).start()
        head_mate(0, c).start()

    merge()

    def sums(d):
        loop(0, CHUNKS, lambda j: sum_step(nearby(j), d))

    sums(3)
    head_pass(0)
    sums(2)
    head_pass(1)
    sums(1)
    head_pass(2)
    loop(0, CHUNKS, lambda j: answer(nearby(j)))
    ret[slot_rows(e), :] = ans[slot_rows(e), :]
    head_pass(3)

    weight_copies[3].wait()
    for number in range(2 * half_ring + 1):
        head_mate(number, other).wait_recv()
    mixed = jnp.zeros((rows, LANES), F32)
    for block in range(ny):
        both = jnp.concatenate([heads[block, 0], heads[block, 1]], axis=1)
        mixed += jnp.dot(
            both, ow[block * 2 * LANES : (block + 1) * 2 * LANES, :], preferred_element_type=F32
        )
    mix_ref[...] = mixed.astype(BF16)

    def wait_back(peer):
        remote(
            ans.at[slot_rows(0)],
            ret.at[slot_rows(peer)],
            b_send.at[peer],
            b_recv.at[peer],
            z=z,
            x=x,
        ).wait_recv()

    each_other(0, nep, wait_back)
    routed = jnp.zeros((LANES, rows), F32)
    for i in range(2):
        routed += weight[i : i + 1, :] * lax.dot_general(
            ret[...], one_hot(i), (((0,), (0,)), ((), ())), preferred_element_type=F32
        )
    rout_ref[...] = routed.T.astype(BF16)

    def drain(peer):
        dispatch(peer).wait_send()
        back_copy(peer).wait_send()

    each_other(0, nep, drain)

    def drain_chunk(k):
        for s in range(half_ring):
            up_copy(s, k).wait_send()
            dn_copy(s, k).wait_send()
            sum_up(k, s + 1).wait_send()
            sum_dn(k, s + 1).wait_send()
        for number in range(2 * half_ring + 1):
            mate_copy(number, k).wait_send()
        part_copy(k).wait_send()

    loop(0, CHUNKS, drain_chunk)
    for r in range(1, nx):
        query_copy(r).wait_send()
        for copy in result_copies(r):
            copy.wait_send()
    for r in range(1, reach + 1):

        @pl.when((z + 1 < nz) & (z - r + 1 >= 0))
        def _(r=r):
            for copy in chain_copies(r):
                copy.wait_send()

    for r in range(reach + 1, nz):

        @pl.when(z + r < nz)
        def _(r=r):
            for copy in far_copies(r):
                copy.wait_send()

    for s in range(half_ring):
        head_up(s, 0).wait_send()
        head_dn(s, 0).wait_send()
    for number in range(2 * half_ring + 1):
        head_mate(number, c).wait_send()


def local(
    sizes,
    queries,
    key_rows,
    values,
    second_scale,
    head_gain,
    out_weight,
    routed_in,
    routed_gain,
    expert_ids,
    group_logits,
    inner_logits,
    gate_weight,
    up_weight,
    down_weight,
):
    nz, nx, ny = sizes
    nep = nz * nx
    rows = routed_in.shape[0]
    width = routed_in.shape[1]
    hidden = gate_weight.shape[2]
    cap = 2 * expert_ids.shape[1] * rows // nep
    total = nep * cap
    chunk = total // CHUNKS
    half_ring = ny // 2
    mates = 2 * half_ring + 1
    dma = pltpu.SemaphoreType.DMA
    vmem = pltpu.VMEM
    scratch = [
        vmem((width, hidden), BF16),
        vmem((width, hidden), BF16),
        vmem((hidden, width), BF16),
        vmem(out_weight.shape, BF16),
        vmem((rows, width), BF16),
        dma((4,)),
        dma((4,)),
        vmem((8, rows), F32),
        vmem((8, rows), F32),
        vmem((total, LANES), BF16),
        vmem((ny, 2, total, LANES), BF16),
        vmem((CHUNKS, 2, ny, chunk, LANES), BF16),
        vmem((CHUNKS, ny, chunk, LANES), BF16),
        vmem((CHUNKS, half_ring, chunk, LANES), BF16),
        vmem((CHUNKS, half_ring, chunk, LANES), BF16),
        vmem((CHUNKS, half_ring, chunk, LANES), BF16),
        vmem((CHUNKS, half_ring, chunk, LANES), BF16),
        vmem((total, LANES), BF16),
        vmem((total, LANES), BF16),
        dma((nep,)),
        dma((nep,)),
        dma((CHUNKS, half_ring)),
        dma((CHUNKS, half_ring)),
        dma((CHUNKS, half_ring)),
        dma((CHUNKS, half_ring)),
        dma((CHUNKS, mates)),
        dma((CHUNKS, mates)),
        dma((CHUNKS,)),
        dma((CHUNKS,)),
        dma((CHUNKS, half_ring)),
        dma((CHUNKS, half_ring)),
        dma((CHUNKS, half_ring)),
        dma((CHUNKS, half_ring)),
        dma((nep,)),
        dma((nep,)),
        vmem((nx, rows, LANES), BF16),
        vmem((nx, 2 * rows, LANES), BF16),
        vmem((nz, rows, LANES), BF16),
        vmem((nz, rows, LANES), BF16),
        vmem((nx, LANES, 2 * rows), F32),
        vmem((nx, 8, 2 * rows), F32),
        vmem((nx, LANES, 2 * rows), BF16),
        vmem((nx, LANES, 2 * rows), BF16),
        vmem((nx, 8, 2 * rows), F32),
        vmem((ny, 2, rows, LANES), BF16),
        dma((nx,)),
        dma((nx,)),
        dma((nz,)),
        dma((nz,)),
        dma((nz,)),
        dma((nz,)),
        dma((nx,)),
        dma((nx,)),
        dma((nx,)),
        dma((nx,)),
        dma((half_ring,)),
        dma((half_ring,)),
        dma((half_ring,)),
        dma((half_ring,)),
        dma((mates,)),
        dma((mates,)),
    ]
    whole = pl.BlockSpec(memory_space=pltpu.VMEM)
    far = pl.BlockSpec(memory_space=pl.ANY)
    return pl.pallas_call(
        lambda *refs: kernel(sizes, *refs),
        out_shape=(
            jax.ShapeDtypeStruct((rows, LANES), BF16),
            jax.ShapeDtypeStruct((rows, LANES), BF16),
        ),
        in_specs=[far] * 3 + [whole] * 2 + [far] * 2 + [whole] * 4 + [far] * 3,
        out_specs=(whole, whole),
        scratch_shapes=scratch,
        compiler_params=pltpu.CompilerParams(
            collective_id=0, has_side_effects=True, vmem_limit_bytes=60 * 1024 * 1024
        ),
    )(
        queries,
        key_rows,
        values,
        second_scale.reshape(1, 1),
        head_gain.reshape(1, -1),
        out_weight,
        routed_in,
        routed_gain.reshape(1, -1),
        expert_ids.T,
        group_logits.T,
        inner_logits.T,
        gate_weight[0],
        up_weight[0],
        down_weight[0],
    )


def build(mesh, sizes):
    nz, nx, ny = sizes
    finer = Mesh(mesh.devices.reshape(nz, nx, ny, 2), ("z", "x", "y", "c"))
    ep, tp = ("z", "x"), ("y", "c")
    placed = (
        P(ep, tp),
        P(ep, tp),
        P(ep, tp),
        P(tp),
        P(),
        P(None, tp),
        P(ep, None),
        P(),
        P(ep, None),
        P(ep, None),
        P(ep, None),
        P(ep, None, tp),
        P(ep, None, tp),
        P(ep, tp, None),
    )
    return jax.shard_map(
        lambda *args: local(sizes, *args),
        mesh=finer,
        in_specs=placed,
        out_specs=(P(ep, tp), P(ep, tp)),
        check_vma=False,
    )


def solution(mesh):
    return build(mesh, (8, 4, mesh.shape["tp"] // 2))
```

```python
import jax
import jax.numpy as jnp
from jax import lax
from jax.experimental import pallas as pl
from jax.experimental.pallas import tpu as pltpu
from jax.sharding import Mesh
from jax.sharding import PartitionSpec as P

EPSILON = 1e-05
LOWEST = -1e30
GROUP_SIZE = 4
LANES = 128
CHUNKS = 4
F32 = jnp.float32
BF16 = jnp.bfloat16


def remote(src, dst, send_sem, recv_sem, **where):
    return pltpu.make_async_remote_copy(
        src_ref=src,
        dst_ref=dst,
        send_sem=send_sem,
        recv_sem=recv_sem,
        device_id=where,
        device_id_type=pl.DeviceIdType.MESH,
    )


def loop(first, last, body):
    def step(i, carry):
        body(i)
        return carry

    lax.fori_loop(first, last, step, 0)


def kernel(
    sizes,
    q_hbm,
    k_hbm,
    v_hbm,
    scale_hbm,
    hgain_hbm,
    ow_hbm,
    rin_hbm,
    rgain_hbm,
    ids_hbm,
    gl_hbm,
    il_hbm,
    gw_hbm,
    uw_hbm,
    dw_hbm,
    mix_ref,
    rout_ref,
    gw,
    uw,
    dw,
    ow,
    rin,
    scale_ref,
    hgain_ref,
    rgain_ref,
    ids_ref,
    gl_ref,
    il_ref,
    w_sem,
    i_sem,
    pos,
    weight,
    disp,
    xs,
    parts,
    mate,
    rb_up,
    rb_dn,
    sb_up,
    sb_dn,
    ans,
    ret,
    a_send,
    a_recv,
    up_send,
    up_recv,
    dn_send,
    dn_recv,
    m_send,
    m_recv,
    pm_send,
    pm_recv,
    ru_send,
    ru_recv,
    rd_send,
    rd_recv,
    b_send,
    b_recv,
    qb,
    qs,
    kb,
    vb,
    acc,
    stat,
    o_out,
    o_in,
    stat_in,
    heads,
    q_send,
    q_recv,
    k_send,
    k_recv,
    v_send,
    v_recv,
    o_send,
    o_recv,
    s_send,
    s_recv,
    hu_send,
    hu_recv,
    hd_send,
    hd_recv,
    hm_send,
    hm_recv,
):
    nz, nx, ny = sizes
    nep = nz * nx
    half_ring = ny // 2
    z, x, y, c = (lax.axis_index(name) for name in ("z", "x", "y", "c"))
    other = 1 - c
    e = z * nx + x
    t = y * 2 + c
    rows = rin.shape[0]
    width = rin.shape[1]
    total = xs.shape[2]
    cap = total // nep
    chunk = total // CHUNKS
    half = chunk // 2
    per_chunk = nep // CHUNKS
    y_next = lax.rem(y + 1, ny)
    y_prev = lax.rem(y + ny - 1, ny)

    def y_at(shift):
        return lax.rem(y + shift + ny, ny)

    group = z // (nz // CHUNKS)

    def nearby(j):
        return lax.rem(group + (0, 1, 3, 2)[j], CHUNKS)

    def each_other(first, count, body):
        def one(i):
            @pl.when(first + i != e)
            def _():
                body(first + i)

        loop(0, count, one)

    barrier = pltpu.get_barrier_semaphore()

    def greet(peer):
        pl.semaphore_signal(
            barrier,
            inc=1,
            device_id={"z": peer // nx, "x": lax.rem(peer, nx)},
            device_id_type=pl.DeviceIdType.MESH,
        )

    each_other(0, nep, greet)

    def greet_y(r):
        pl.semaphore_signal(
            barrier, inc=1, device_id={"y": lax.rem(y + r, ny)}, device_id_type=pl.DeviceIdType.MESH
        )

    loop(1, ny, greet_y)
    pl.semaphore_signal(
        barrier, inc=1, device_id={"c": other}, device_id_type=pl.DeviceIdType.MESH
    )

    input_copies = [
        pltpu.make_async_copy(src, dst, i_sem.at[i])
        for i, (src, dst) in enumerate(
            (
                (ids_hbm, ids_ref),
                (gl_hbm, gl_ref),
                (il_hbm, il_ref),
                (rgain_hbm, rgain_ref),
                (rin_hbm, rin),
                (q_hbm, qb.at[x]),
                (k_hbm, kb.at[z]),
                (v_hbm, vb.at[z]),
                (scale_hbm, scale_ref),
                (hgain_hbm, hgain_ref),
            )
        )
    ]
    weight_copies = [
        pltpu.make_async_copy(src, dst, w_sem.at[i])
        for i, (src, dst) in enumerate(
            ((gw_hbm, gw), (uw_hbm, uw), (dw_hbm, dw), (ow_hbm, ow))
        )
    ]
    for copy in input_copies + weight_copies:
        copy.start()

    for copy in input_copies[:4]:
        copy.wait()
    ids = ids_ref[...]
    shape = (nep, rows)
    expert_row = lax.broadcasted_iota(jnp.int32, shape, 0)
    picks = [jnp.where(ids[i : i + 1, :] == expert_row, 1.0, 0.0) for i in range(2)]
    earlier = jnp.where(
        lax.broadcasted_iota(jnp.int32, (rows, rows), 0)
        < lax.broadcasted_iota(jnp.int32, (rows, rows), 1),
        1.0,
        0.0,
    ).astype(BF16)
    before = [jnp.dot(pick.astype(BF16), earlier, preferred_element_type=F32) for pick in picks]
    before[1] += jnp.sum(picks[0], axis=1, keepdims=True)
    logits = gl_ref[...]
    group_exp = jnp.exp(logits - jnp.max(logits, axis=0, keepdims=True))
    group_prob = group_exp / jnp.sum(group_exp, axis=0, keepdims=True)
    group_row = lax.broadcasted_iota(jnp.int32, logits.shape, 0)
    inner = il_ref[...]
    inner_exp = jnp.exp(inner - jnp.max(inner, axis=0, keepdims=True))
    inner_prob = inner_exp / jnp.sum(inner_exp, axis=0, keepdims=True)
    for i in range(2):
        pos[i : i + 1, :] = ids[i : i + 1, :].astype(F32) * cap + jnp.sum(
            picks[i] * before[i], axis=0, keepdims=True
        )
        chosen = ids[i : i + 1, :] // GROUP_SIZE == group_row
        picked = jnp.sum(jnp.where(chosen, group_prob, 0.0), axis=0, keepdims=True)
        weight[i : i + 1, :] = picked * inner_prob[i : i + 1, :]

    def one_hot(i):
        slots = lax.broadcasted_iota(jnp.int32, (total, rows), 0).astype(F32)
        return jnp.where(pos[i : i + 1, :] == slots, 1.0, 0.0).astype(BF16)

    own_cols = pl.ds(pl.multiple_of(t * LANES, LANES), LANES)
    input_copies[4].wait()
    source = rin[...].astype(F32)
    inv = lax.rsqrt(jnp.sum(source * source, axis=-1, keepdims=True) * (1.0 / width) + EPSILON)
    normed = (rin[:, own_cols].astype(F32) * inv * rgain_ref[:, own_cols]).astype(BF16)
    disp[...] = jnp.dot(
        one_hot(0) + one_hot(1), normed, preferred_element_type=F32
    ).astype(BF16)
    for copy in input_copies[5:]:
        copy.wait()

    pl.semaphore_wait(barrier, nep - 1 + ny - 1 + 1)

    def slot_rows(index):
        return pl.ds(pl.multiple_of(index * cap, cap), cap)

    def dispatch(peer):
        return remote(
            disp.at[slot_rows(peer)],
            xs.at[y, c, slot_rows(e)],
            a_send.at[peer],
            a_recv.at[e],
            z=peer // nx,
            x=lax.rem(peer, nx),
        )

    for j in range(CHUNKS):
        each_other(nearby(j) * per_chunk, per_chunk, lambda peer: dispatch(peer).start())
    xs[y, c, slot_rows(e), :] = disp[slot_rows(e), :]

    def query_copy(r):
        return remote(
            qb.at[x], qb.at[x], q_send.at[r], q_recv.at[r], x=lax.rem(x + r, nx)
        )

    reach = nz // 2

    def key_copies(block, r, to_z):
        return (
            remote(kb.at[block], kb.at[block], k_send.at[r], k_recv.at[r], z=to_z),
            remote(vb.at[block], vb.at[block], v_send.at[r], v_recv.at[r], z=to_z),
        )

    def chain_copies(r):
        return key_copies(jnp.maximum(z - r + 1, 0), r, jnp.minimum(z + 1, nz - 1))

    def far_copies(r):
        return key_copies(z, r, lax.rem(z + r, nz))

    def chain_send(r):
        @pl.when((z + 1 < nz) & (z - r + 1 >= 0))
        def _():
            for copy in chain_copies(r):
                copy.start()

    def send_queries_and_keys():
        chain_send(1)
        for r in range(reach + 1, nz):

            @pl.when(z + r < nz)
            def _(r=r):
                for copy in far_copies(r):
                    copy.start()

        for r in range(1, nx):
            query_copy(r).start()

    maps = 2 * rows
    qk = LANES // 2
    keep_low = lax.broadcasted_iota(jnp.int32, (rows, LANES), 1) < qk

    def stack_query(value, index):
        scaled = value.astype(F32) * (qk ** (-0.5))
        qs[index, 0:rows, :] = jnp.where(keep_low, scaled, 0.0).astype(BF16)
        qs[index, rows:maps, :] = jnp.where(keep_low, 0.0, scaled).astype(BF16)

    def attend(key_block, value_block, masked):
        def one(index):
            scores = lax.dot_general(
                key_block[...],
                qs[index],
                (((1,), (1,)), ((), ())),
                preferred_element_type=F32,
            )
            if masked:
                key_pos = x * rows + lax.broadcasted_iota(jnp.int32, scores.shape, 0)
                column = lax.broadcasted_iota(jnp.int32, scores.shape, 1)
                query_pos = index * rows + jnp.where(column >= rows, column - rows, column)
                visible = query_pos >= key_pos
                scores = jnp.where(visible, scores, LOWEST)
                new_max = jnp.max(scores, axis=0, keepdims=True)
                terms = jnp.where(visible, jnp.exp(scores - new_max), 0.0)
                stat[index, 1:2, :] = jnp.sum(terms, axis=0, keepdims=True)
            else:
                old_max = stat[index, 0:1, :]
                new_max = jnp.maximum(old_max, jnp.max(scores, axis=0, keepdims=True))
                terms = jnp.exp(scores - new_max)
                factor = jnp.exp(old_max - new_max)
                stat[index, 1:2, :] = stat[index, 1:2, :] * factor + jnp.sum(
                    terms, axis=0, keepdims=True
                )
            stat[index, 0:1, :] = new_max
            weighted = lax.dot_general(
                value_block[...],
                terms.astype(BF16),
                (((0,), (0,)), ((), ())),
                preferred_element_type=F32,
            )
            if masked:
                acc[index] = weighted
            else:
                acc[index] = acc[index] * factor + weighted

        loop(0, nx, one)

    def own_attention():
        stack_query(qb[x], x)
        for r in range(1, nx):
            query_copy(r).wait_recv()
            from_x = lax.rem(x + nx - r, nx)
            stack_query(qb[from_x], from_x)
        stat[...] = jnp.zeros_like(stat)
        attend(kb.at[z], vb.at[z], True)

    def chain_step(r):
        @pl.when(z >= r)
        def _():
            for copy in key_copies(jnp.maximum(z - r, 0), r, z):
                copy.wait_recv()
            if r < reach:
                chain_send(r + 1)

    def attend_far(r):
        @pl.when(z >= r)
        def _():
            from_z = jnp.maximum(z - r, 0)
            if r > reach:
                for copy in key_copies(from_z, r, z):
                    copy.wait_recv()
            attend(kb.at[from_z], vb.at[from_z], False)

    def wait_dispatch(peer):
        remote(
            disp.at[slot_rows(0)],
            xs.at[y, c, slot_rows(peer)],
            a_send.at[peer],
            a_recv.at[peer],
            z=z,
            x=x,
        ).wait_recv()

    def chunk_rows(k):
        return pl.ds(pl.multiple_of(k * chunk, chunk), chunk)

    def upper_rows(k):
        return pl.ds(pl.multiple_of(k * chunk, half), half)

    def lower_rows(k):
        return pl.ds(pl.multiple_of(k * chunk + half, half), half)

    def up_copy(s, k):
        where = upper_rows(k) if s == half_ring - 1 else chunk_rows(k)
        block = xs.at[y_at(-s), c, where]
        return remote(block, block, up_send.at[k, s], up_recv.at[k, s], y=y_next)

    def dn_copy(s, k):
        where = lower_rows(k) if s == half_ring - 1 else chunk_rows(k)
        block = xs.at[y_at(s), c, where]
        return remote(block, block, dn_send.at[k, s], dn_recv.at[k, s], y=y_prev)

    def up_arrival(s, k):
        where = upper_rows(k) if s == half_ring - 1 else chunk_rows(k)
        block = xs.at[y_at(-s - 1), c, where]
        return remote(block, block, up_send.at[k, s], up_recv.at[k, s], y=y_next)

    def dn_arrival(s, k):
        where = lower_rows(k) if s == half_ring - 1 else chunk_rows(k)
        block = xs.at[y_at(s + 1), c, where]
        return remote(block, block, dn_send.at[k, s], dn_recv.at[k, s], y=y_prev)

    def mate_blocks(k, core):
        blocks = [xs.at[y, core, chunk_rows(k)]]
        for s in range(half_ring):
            last = s == half_ring - 1
            blocks.append(
                xs.at[y_at(-s - 1), core, upper_rows(k) if last else chunk_rows(k)]
            )
            blocks.append(
                xs.at[y_at(s + 1), core, lower_rows(k) if last else chunk_rows(k)]
            )
        return blocks

    def mate_copy(number, k):
        block = mate_blocks(k, c)[number]
        return remote(block, block, m_send.at[k, number], m_recv.at[k, number], c=other)

    def mate_arrival(number, k):
        block = mate_blocks(k, other)[number]
        return remote(block, block, m_send.at[k, number], m_recv.at[k, number], c=other)

    def first_sends(k):
        each_other(k * per_chunk, per_chunk, wait_dispatch)
        up_copy(0, k).start()
        dn_copy(0, k).start()
        mate_copy(0, k).start()

    def pass_on(s, k):
        up_arrival(s, k).wait_recv()
        if s + 1 < half_ring:
            up_copy(s + 1, k).start()
        mate_copy(2 * s + 1, k).start()
        dn_arrival(s, k).wait_recv()
        if s + 1 < half_ring:
            dn_copy(s + 1, k).start()
        mate_copy(2 * s + 2, k).start()

    def result_copies(r):
        to_x = lax.rem(x + r, nx)
        return (
            remote(o_out.at[to_x], o_in.at[x], o_send.at[r], o_recv.at[r], x=to_x),
            remote(stat.at[to_x], stat_in.at[x], s_send.at[r], s_recv.at[r], x=to_x),
        )

    def result_arrivals(r):
        from_x = lax.rem(x + nx - r, nx)
        return (
            remote(o_out.at[0], o_in.at[from_x], o_send.at[r], o_recv.at[r], x=x),
            remote(stat.at[0], stat_in.at[from_x], s_send.at[r], s_recv.at[r], x=x),
        )

    def send_results():
        o_out[...] = acc[...].astype(BF16)
        for r in range(1, nx):
            for copy in result_copies(r):
                copy.start()
        o_in[x] = o_out[x]
        stat_in[x] = stat[x]

    def expert(k):
        for number in range(2 * half_ring + 1):
            mate_arrival(number, k).wait_recv()
        gate = jnp.zeros((chunk, gw.shape[1]), F32)
        up = jnp.zeros((chunk, gw.shape[1]), F32)
        for block in range(ny):
            both = jnp.concatenate(
                [xs[block, 0, chunk_rows(k), :], xs[block, 1, chunk_rows(k), :]], axis=1
            )
            depth = slice(block * 2 * LANES, (block + 1) * 2 * LANES)
            gate += jnp.dot(both, gw[depth, :], preferred_element_type=F32)
            up += jnp.dot(both, uw[depth, :], preferred_element_type=F32)
        hidden = (gate / (1.0 + jnp.exp(-gate)) * up).astype(BF16)
        for block in range(ny):
            columns = slice(block * 2 * LANES, (block + 1) * 2 * LANES)
            value = jnp.dot(hidden, dw[:, columns], preferred_element_type=F32).astype(BF16)
            parts[k, 0, block] = value[:, :LANES]
            parts[k, 1, block] = value[:, LANES:]
        part_copy(k).start()

    def part_copy(k):
        return remote(parts.at[k, other], mate.at[k], pm_send.at[k], pm_recv.at[k], c=other)

    full = slice(0, chunk)
    top = slice(0, half)
    bottom = slice(half, chunk)

    def chip_sum(k, target, where):
        return parts[k, c, target, where, :].astype(F32) + mate[k, target, where, :].astype(F32)

    def sum_up(k, d):
        where = top if d == half_ring else full
        return remote(
            sb_up.at[k, d - 1, where], rb_up.at[k, d - 1, where],
            ru_send.at[k, d - 1], ru_recv.at[k, d - 1], y=y_next,
        )

    def sum_dn(k, d):
        where = bottom if d == half_ring else full
        return remote(
            sb_dn.at[k, d - 1, where], rb_dn.at[k, d - 1, where],
            rd_send.at[k, d - 1], rd_recv.at[k, d - 1], y=y_prev,
        )

    def sum_step(k, d):
        if d == half_ring:
            sb_up[k, d - 1, top] = chip_sum(k, y_at(d), top).astype(BF16)
            sum_up(k, d).start()
            sb_dn[k, d - 1, bottom] = chip_sum(k, y_at(-d), bottom).astype(BF16)
            sum_dn(k, d).start()
            return
        sum_up(k, d + 1).wait_recv()
        if d + 1 == half_ring:
            sb_up[k, d - 1, top] = (
                chip_sum(k, y_at(d), top) + rb_up[k, d, top].astype(F32)
            ).astype(BF16)
            sb_up[k, d - 1, bottom] = chip_sum(k, y_at(d), bottom).astype(BF16)
        else:
            sb_up[k, d - 1] = (
                chip_sum(k, y_at(d), full) + rb_up[k, d].astype(F32)
            ).astype(BF16)
        sum_up(k, d).start()
        sum_dn(k, d + 1).wait_recv()
        if d + 1 == half_ring:
            sb_dn[k, d - 1, bottom] = (
                chip_sum(k, y_at(-d), bottom) + rb_dn[k, d, bottom].astype(F32)
            ).astype(BF16)
            sb_dn[k, d - 1, top] = chip_sum(k, y_at(-d), top).astype(BF16)
        else:
            sb_dn[k, d - 1] = (
                chip_sum(k, y_at(-d), full) + rb_dn[k, d].astype(F32)
            ).astype(BF16)
        sum_dn(k, d).start()

    def answer(k):
        sum_up(k, 1).wait_recv()
        sum_dn(k, 1).wait_recv()
        if half_ring > 1:
            ans[chunk_rows(k), :] = (
                chip_sum(k, y, full) + rb_up[k, 0].astype(F32) + rb_dn[k, 0].astype(F32)
            ).astype(BF16)
        else:
            ans[upper_rows(k), :] = (
                chip_sum(k, y, top) + rb_up[k, 0, top].astype(F32)
            ).astype(BF16)
            ans[lower_rows(k), :] = (
                chip_sum(k, y, bottom) + rb_dn[k, 0, bottom].astype(F32)
            ).astype(BF16)

        each_other(k * per_chunk, per_chunk, lambda target: back_copy(target).start())

    def back_copy(target):
        return remote(
            ans.at[slot_rows(target)],
            ret.at[slot_rows(e)],
            b_send.at[target],
            b_recv.at[e],
            z=target // nx,
            x=lax.rem(target, nx),
        )

    def first_sum(k):
        part_copy(k).wait_recv()
        sum_step(k, half_ring)

    top_rows = pl.ds(0, rows // 2)
    low_rows = pl.ds(rows // 2, rows // 2)
    all_rows = pl.ds(0, rows)

    def head_up(s, hop):
        where = top_rows if s == half_ring - 1 else all_rows
        block = heads.at[y_at(-s - hop), c, where]
        return remote(block, block, hu_send.at[s], hu_recv.at[s], y=y_next)

    def head_dn(s, hop):
        where = low_rows if s == half_ring - 1 else all_rows
        block = heads.at[y_at(s + hop), c, where]
        return remote(block, block, hd_send.at[s], hd_recv.at[s], y=y_prev)

    def head_mate(number, core):
        s = (number - 1) // 2
        last = number > 0 and s == half_ring - 1
        if number == 0:
            block = heads.at[y, core]
        elif number % 2 == 1:
            block = heads.at[y_at(-s - 1), core, top_rows if last else all_rows]
        else:
            block = heads.at[y_at(s + 1), core, low_rows if last else all_rows]
        return remote(block, block, hm_send.at[number], hm_recv.at[number], c=other)

    def head_pass(s):
        head_up(s, 1).wait_recv()
        if s + 1 < half_ring:
            head_up(s + 1, 0).start()
        head_mate(2 * s + 1, c).start()
        head_dn(s, 1).wait_recv()
        if s + 1 < half_ring:
            head_dn(s + 1, 0).start()
        head_mate(2 * s + 2, c).start()

    def merge():
        for r in range(1, nx):
            for copy in result_arrivals(r):
                copy.wait_recv()
        top_max = stat_in[0, 0:1, :]
        for j in range(1, nx):
            top_max = jnp.maximum(top_max, stat_in[j, 0:1, :])
        denominator = jnp.zeros_like(top_max)
        weighted = jnp.zeros(o_in.shape[1:], F32)
        for j in range(nx):
            factor = jnp.exp(stat_in[j, 0:1, :] - top_max)
            denominator += factor * stat_in[j, 1:2, :]
            weighted += factor * o_in[j].astype(F32)
        mapped = weighted / denominator
        difference = mapped[:, :rows] - scale_ref[0:1, 0:1] * mapped[:, rows:]
        mean = jnp.sum(difference * difference, axis=0, keepdims=True) * (1.0 / LANES)
        head = difference * lax.rsqrt(mean + EPSILON)
        heads[y, c] = (head.T * hgain_ref[...]).astype(BF16)
        head_up(0, 0).start()
        head_dn(0, 0).start()
        head_mate(0, c).start()

    stages = [first_sends]
    stages += [lambda k, s=s: pass_on(s, k) for s in range(half_ring)]
    stages += [expert, first_sum]
    stages += [lambda k, d=d: sum_step(k, d) for d in range(half_ring - 1, 0, -1)]
    stages += [answer]
    beside = {
        0: [send_queries_and_keys],
        2: [lambda: chain_step(1), own_attention],
        3: [lambda: chain_step(2), lambda: attend_far(1)],
        4: [lambda: chain_step(3), lambda: attend_far(2)],
        5: [lambda: chain_step(4), lambda: attend_far(3)],
        6: [lambda: attend_far(4), lambda: attend_far(5)],
        7: [lambda: attend_far(6), lambda: attend_far(7), send_results],
        9: [merge],
        10: [lambda: head_pass(0)],
        11: [lambda: head_pass(1)],
        12: [lambda: head_pass(2)],
        13: [lambda: head_pass(3)],
    }
    for wave in range(len(stages) + CHUNKS - 1):
        for j in range(CHUNKS):
            if 0 <= wave - j < len(stages):
                if wave - j == half_ring + 1 and j == 0:
                    for copy in weight_copies[:3]:
                        copy.wait()
                stages[wave - j](nearby(j))
        for work in beside.get(wave, []):
            work()
    ret[slot_rows(e), :] = ans[slot_rows(e), :]

    weight_copies[3].wait()
    for number in range(2 * half_ring + 1):
        head_mate(number, other).wait_recv()
    mixed = jnp.zeros((rows, LANES), F32)
    for block in range(ny):
        both = jnp.concatenate([heads[block, 0], heads[block, 1]], axis=1)
        mixed += jnp.dot(
            both, ow[block * 2 * LANES : (block + 1) * 2 * LANES, :], preferred_element_type=F32
        )
    mix_ref[...] = mixed.astype(BF16)

    def wait_back(peer):
        remote(
            ans.at[slot_rows(0)],
            ret.at[slot_rows(peer)],
            b_send.at[peer],
            b_recv.at[peer],
            z=z,
            x=x,
        ).wait_recv()

    each_other(0, nep, wait_back)
    routed = jnp.zeros((LANES, rows), F32)
    for i in range(2):
        routed += weight[i : i + 1, :] * lax.dot_general(
            ret[...], one_hot(i), (((0,), (0,)), ((), ())), preferred_element_type=F32
        )
    rout_ref[...] = routed.T.astype(BF16)

    def drain(peer):
        dispatch(peer).wait_send()
        back_copy(peer).wait_send()

    each_other(0, nep, drain)

    def drain_chunk(k):
        for s in range(half_ring):
            up_copy(s, k).wait_send()
            dn_copy(s, k).wait_send()
            sum_up(k, s + 1).wait_send()
            sum_dn(k, s + 1).wait_send()
        for number in range(2 * half_ring + 1):
            mate_copy(number, k).wait_send()
        part_copy(k).wait_send()

    loop(0, CHUNKS, drain_chunk)
    for r in range(1, nx):
        query_copy(r).wait_send()
        for copy in result_copies(r):
            copy.wait_send()
    for r in range(1, reach + 1):

        @pl.when((z + 1 < nz) & (z - r + 1 >= 0))
        def _(r=r):
            for copy in chain_copies(r):
                copy.wait_send()

    for r in range(reach + 1, nz):

        @pl.when(z + r < nz)
        def _(r=r):
            for copy in far_copies(r):
                copy.wait_send()

    for s in range(half_ring):
        head_up(s, 0).wait_send()
        head_dn(s, 0).wait_send()
    for number in range(2 * half_ring + 1):
        head_mate(number, c).wait_send()


def local(
    sizes,
    queries,
    key_rows,
    values,
    second_scale,
    head_gain,
    out_weight,
    routed_in,
    routed_gain,
    expert_ids,
    group_logits,
    inner_logits,
    gate_weight,
    up_weight,
    down_weight,
):
    nz, nx, ny = sizes
    nep = nz * nx
    rows = routed_in.shape[0]
    width = routed_in.shape[1]
    hidden = gate_weight.shape[2]
    cap = 2 * expert_ids.shape[1] * rows // nep
    total = nep * cap
    chunk = total // CHUNKS
    half_ring = ny // 2
    mates = 2 * half_ring + 1
    dma = pltpu.SemaphoreType.DMA
    vmem = pltpu.VMEM
    scratch = [
        vmem((width, hidden), BF16),
        vmem((width, hidden), BF16),
        vmem((hidden, width), BF16),
        vmem(out_weight.shape, BF16),
        vmem((rows, width), BF16),
        vmem((1, 1), F32),
        vmem((1, LANES), F32),
        vmem((1, width), F32),
        vmem((2, rows), jnp.int32),
        vmem((group_logits.shape[1], rows), F32),
        vmem((2, rows), F32),
        dma((4,)),
        dma((10,)),
        vmem((8, rows), F32),
        vmem((8, rows), F32),
        vmem((total, LANES), BF16),
        vmem((ny, 2, total, LANES), BF16),
        vmem((CHUNKS, 2, ny, chunk, LANES), BF16),
        vmem((CHUNKS, ny, chunk, LANES), BF16),
        vmem((CHUNKS, half_ring, chunk, LANES), BF16),
        vmem((CHUNKS, half_ring, chunk, LANES), BF16),
        vmem((CHUNKS, half_ring, chunk, LANES), BF16),
        vmem((CHUNKS, half_ring, chunk, LANES), BF16),
        vmem((total, LANES), BF16),
        vmem((total, LANES), BF16),
        dma((nep,)),
        dma((nep,)),
        dma((CHUNKS, half_ring)),
        dma((CHUNKS, half_ring)),
        dma((CHUNKS, half_ring)),
        dma((CHUNKS, half_ring)),
        dma((CHUNKS, mates)),
        dma((CHUNKS, mates)),
        dma((CHUNKS,)),
        dma((CHUNKS,)),
        dma((CHUNKS, half_ring)),
        dma((CHUNKS, half_ring)),
        dma((CHUNKS, half_ring)),
        dma((CHUNKS, half_ring)),
        dma((nep,)),
        dma((nep,)),
        vmem((nx, rows, LANES), BF16),
        vmem((nx, 2 * rows, LANES), BF16),
        vmem((nz, rows, LANES), BF16),
        vmem((nz, rows, LANES), BF16),
        vmem((nx, LANES, 2 * rows), F32),
        vmem((nx, 8, 2 * rows), F32),
        vmem((nx, LANES, 2 * rows), BF16),
        vmem((nx, LANES, 2 * rows), BF16),
        vmem((nx, 8, 2 * rows), F32),
        vmem((ny, 2, rows, LANES), BF16),
        dma((nx,)),
        dma((nx,)),
        dma((nz,)),
        dma((nz,)),
        dma((nz,)),
        dma((nz,)),
        dma((nx,)),
        dma((nx,)),
        dma((nx,)),
        dma((nx,)),
        dma((half_ring,)),
        dma((half_ring,)),
        dma((half_ring,)),
        dma((half_ring,)),
        dma((mates,)),
        dma((mates,)),
    ]
    whole = pl.BlockSpec(memory_space=pltpu.VMEM)
    far = pl.BlockSpec(memory_space=pl.ANY)
    return pl.pallas_call(
        lambda *refs: kernel(sizes, *refs),
        out_shape=(
            jax.ShapeDtypeStruct((rows, LANES), BF16),
            jax.ShapeDtypeStruct((rows, LANES), BF16),
        ),
        in_specs=[far] * 14,
        out_specs=(whole, whole),
        scratch_shapes=scratch,
        compiler_params=pltpu.CompilerParams(
            collective_id=0, has_side_effects=True, vmem_limit_bytes=60 * 1024 * 1024
        ),
    )(
        queries,
        key_rows,
        values,
        second_scale.reshape(1, 1),
        head_gain.reshape(1, -1),
        out_weight,
        routed_in,
        routed_gain.reshape(1, -1),
        expert_ids.T,
        group_logits.T,
        inner_logits.T,
        gate_weight[0],
        up_weight[0],
        down_weight[0],
    )


def build(mesh, sizes):
    nz, nx, ny = sizes
    finer = Mesh(mesh.devices.reshape(nz, nx, ny, 2), ("z", "x", "y", "c"))
    ep, tp = ("z", "x"), ("y", "c")
    placed = (
        P(ep, tp),
        P(ep, tp),
        P(ep, tp),
        P(tp),
        P(),
        P(None, tp),
        P(ep, None),
        P(),
        P(ep, None),
        P(ep, None),
        P(ep, None),
        P(ep, None, tp),
        P(ep, None, tp),
        P(ep, tp, None),
    )
    return jax.shard_map(
        lambda *args: local(sizes, *args),
        mesh=finer,
        in_specs=placed,
        out_specs=(P(ep, tp), P(ep, tp)),
        check_vma=False,
    )


def solution(mesh):
    return build(mesh, (8, 4, mesh.shape["tp"] // 2))
```

```python
import jax
import jax.numpy as jnp
from jax import lax
from jax.experimental import pallas as pl
from jax.experimental.pallas import tpu as pltpu
from jax.sharding import Mesh
from jax.sharding import PartitionSpec as P

EPSILON = 1e-05
LOWEST = -1e30
GROUP_SIZE = 4
LANES = 128
CHUNKS = 4
ORDER = (
    ("gather", 0, 0),
    ("inputs",),
    ("gather", 0, 1),
    ("gather", 1, 0),
    ("gather", 0, 2),
    ("gather", 0, 3),
    ("gather", 1, 1),
    ("chain", 1),
    ("own",),
    ("attend", 1),
    ("gather", 1, 2),
    ("gather", 2, 0),
    ("gather", 1, 3),
    ("far", 0),
    ("gather", 2, 1),
    ("chain", 2),
    ("attend", 2),
    ("far", 1),
    ("gather", 2, 2),
    ("far", 2),
    ("gather", 3, 0),
    ("far", 3),
    ("expert", 0),
    ("gather", 2, 3),
    ("chain", 3),
    ("attend", 3),
    ("gather", 3, 1),
    ("sum", 4, 0),
    ("gather", 3, 2),
    ("expert", 1),
    ("gather", 3, 3),
    ("expert", 2),
    ("sum", 3, 0),
    ("expert", 3),
    ("sum", 4, 1),
    ("sum", 4, 2),
    ("chain", 4),
    ("attend", 4),
    ("attend", 5),
    ("sum", 2, 0),
    ("attend", 6),
    ("sum", 3, 1),
    ("sum", 4, 3),
    ("sum", 3, 2),
    ("attend", 7),
    ("results",),
    ("sum", 1, 0),
    ("sum", 2, 1),
    ("sum", 3, 3),
    ("sum", 2, 2),
    ("sum", 0, 0),
    ("sum", 1, 1),
    ("merge",),
    ("sum", 2, 3),
    ("sum", 1, 2),
    ("sum", 0, 1),
    ("heads", 1),
    ("sum", 1, 3),
    ("sum", 0, 2),
    ("heads", 2),
    ("sum", 0, 3),
    ("heads", 3),
    ("heads", 4),
    ("project",),
)
F32 = jnp.float32
BF16 = jnp.bfloat16


def remote(src, dst, send_sem, recv_sem, **where):
    return pltpu.make_async_remote_copy(
        src_ref=src,
        dst_ref=dst,
        send_sem=send_sem,
        recv_sem=recv_sem,
        device_id=where,
        device_id_type=pl.DeviceIdType.MESH,
    )


def loop(first, last, body):
    def step(i, carry):
        body(i)
        return carry

    lax.fori_loop(first, last, step, 0)


def kernel(
    sizes,
    q_hbm,
    k_hbm,
    v_hbm,
    scale_hbm,
    hgain_hbm,
    ow_hbm,
    rin_hbm,
    rgain_hbm,
    ids_hbm,
    gl_hbm,
    il_hbm,
    gw_hbm,
    uw_hbm,
    dw_hbm,
    mix_ref,
    rout_ref,
    gw,
    uw,
    dw,
    ow,
    rin,
    scale_ref,
    hgain_ref,
    rgain_ref,
    ids_ref,
    gl_ref,
    il_ref,
    w_sem,
    i_sem,
    pos,
    weight,
    disp,
    disp_far,
    xs,
    parts,
    mate,
    rb_up,
    rb_dn,
    sb_up,
    sb_dn,
    ans,
    ret,
    a_send,
    a_recv,
    f_send,
    f_recv,
    up_send,
    up_recv,
    dn_send,
    dn_recv,
    m_send,
    m_recv,
    pm_send,
    pm_recv,
    ru_send,
    ru_recv,
    rd_send,
    rd_recv,
    b_send,
    b_recv,
    qb,
    qs,
    kb,
    vb,
    acc,
    stat,
    o_out,
    o_in,
    stat_in,
    heads,
    q_send,
    q_recv,
    k_send,
    k_recv,
    v_send,
    v_recv,
    o_send,
    o_recv,
    s_send,
    s_recv,
    hu_send,
    hu_recv,
    hd_send,
    hd_recv,
    hm_send,
    hm_recv,
):
    nz, nx, ny = sizes
    nep = nz * nx
    half_ring = ny // 2
    z, x, y, c = (lax.axis_index(name) for name in ("z", "x", "y", "c"))
    other = 1 - c
    e = z * nx + x
    t = y * 2 + c
    rows = rin.shape[0]
    width = rin.shape[1]
    total = xs.shape[2]
    cap = total // nep
    chunk = total // CHUNKS
    half = chunk // 2
    per_chunk = nep // CHUNKS
    y_next = lax.rem(y + 1, ny)
    y_prev = lax.rem(y + ny - 1, ny)

    def y_at(shift):
        return lax.rem(y + shift + ny, ny)

    group = z // (nz // CHUNKS)

    def nearby(j):
        return lax.rem(group + (0, 1, 3, 2)[j], CHUNKS)

    def each_other(first, count, body):
        def one(i):
            @pl.when(first + i != e)
            def _():
                body(first + i)

        loop(0, count, one)


    input_copies = [
        pltpu.make_async_copy(src, dst, i_sem.at[i])
        for i, (src, dst) in enumerate(
            (
                (rin_hbm, rin),
                (ids_hbm, ids_ref),
                (gl_hbm, gl_ref),
                (il_hbm, il_ref),
                (rgain_hbm, rgain_ref),
                (q_hbm, qb.at[x]),
                (k_hbm, kb.at[z]),
                (v_hbm, vb.at[z]),
                (scale_hbm, scale_ref),
                (hgain_hbm, hgain_ref),
            )
        )
    ]
    weight_copies = [
        pltpu.make_async_copy(src, dst, w_sem.at[i])
        for i, (src, dst) in enumerate(
            ((gw_hbm, gw), (uw_hbm, uw), (dw_hbm, dw), (ow_hbm, ow))
        )
    ]
    for copy in input_copies:
        copy.start()

    barrier = pltpu.get_barrier_semaphore()

    def greet(peer):
        pl.semaphore_signal(
            barrier,
            inc=1,
            device_id={"z": peer // nx, "x": lax.rem(peer, nx)},
            device_id_type=pl.DeviceIdType.MESH,
        )

    each_other(0, nep, greet)

    def greet_y(r):
        pl.semaphore_signal(
            barrier, inc=1, device_id={"y": lax.rem(y + r, ny)}, device_id_type=pl.DeviceIdType.MESH
        )

    loop(1, ny, greet_y)
    pl.semaphore_signal(
        barrier, inc=1, device_id={"c": other}, device_id_type=pl.DeviceIdType.MESH
    )

    for copy in input_copies[1:5]:
        copy.wait()
    ids = ids_ref[...]
    shape = (nep, rows)
    expert_row = lax.broadcasted_iota(jnp.int32, shape, 0)
    picks = [jnp.where(ids[i : i + 1, :] == expert_row, 1.0, 0.0) for i in range(2)]
    earlier = jnp.where(
        lax.broadcasted_iota(jnp.int32, (rows, rows), 0)
        < lax.broadcasted_iota(jnp.int32, (rows, rows), 1),
        1.0,
        0.0,
    ).astype(BF16)
    before = [jnp.dot(pick.astype(BF16), earlier, preferred_element_type=F32) for pick in picks]
    before[1] += jnp.sum(picks[0], axis=1, keepdims=True)
    logits = gl_ref[...]
    group_exp = jnp.exp(logits - jnp.max(logits, axis=0, keepdims=True))
    group_prob = group_exp / jnp.sum(group_exp, axis=0, keepdims=True)
    group_row = lax.broadcasted_iota(jnp.int32, logits.shape, 0)
    inner = il_ref[...]
    inner_exp = jnp.exp(inner - jnp.max(inner, axis=0, keepdims=True))
    inner_prob = inner_exp / jnp.sum(inner_exp, axis=0, keepdims=True)
    for i in range(2):
        pos[i : i + 1, :] = ids[i : i + 1, :].astype(F32) * cap + jnp.sum(
            picks[i] * before[i], axis=0, keepdims=True
        )
        chosen = ids[i : i + 1, :] // GROUP_SIZE == group_row
        picked = jnp.sum(jnp.where(chosen, group_prob, 0.0), axis=0, keepdims=True)
        weight[i : i + 1, :] = picked * inner_prob[i : i + 1, :]

    def one_hot(i):
        slots = lax.broadcasted_iota(jnp.int32, (total, rows), 0).astype(F32)
        return jnp.where(pos[i : i + 1, :] == slots, 1.0, 0.0).astype(BF16)

    input_copies[0].wait()
    source = rin[...].astype(F32)
    inv = lax.rsqrt(jnp.sum(source * source, axis=-1, keepdims=True) * (1.0 / width) + EPSILON)

    def normed(block):
        columns = pl.ds(pl.multiple_of((block * 2 + c) * LANES, LANES), LANES)
        return (rin[:, columns].astype(F32) * inv * rgain_ref[:, columns]).astype(BF16)

    y_far = y_at(half_ring)
    spread = jnp.dot(
        one_hot(0) + one_hot(1),
        jnp.concatenate([normed(y), normed(y_far)], axis=1),
        preferred_element_type=F32,
    ).astype(BF16)
    disp[...] = spread[:, :LANES]
    disp_far[...] = spread[:, LANES:]
    for copy in input_copies[5:]:
        copy.wait()
    for copy in weight_copies:
        copy.start()

    pl.semaphore_wait(barrier, nep - 1 + ny - 1 + 1)

    def slot_rows(index):
        return pl.ds(pl.multiple_of(index * cap, cap), cap)

    def dispatch(peer):
        return remote(
            disp.at[slot_rows(peer)],
            xs.at[y, c, slot_rows(e)],
            a_send.at[peer],
            a_recv.at[e],
            z=peer // nx,
            x=lax.rem(peer, nx),
        )

    def dispatch_far(peer):
        return remote(
            disp_far.at[slot_rows(peer)],
            xs.at[y_far, c, slot_rows(e)],
            f_send.at[peer],
            f_recv.at[e],
            z=peer // nx,
            x=lax.rem(peer, nx),
        )

    for j in range(CHUNKS):
        each_other(nearby(j) * per_chunk, per_chunk, lambda peer: dispatch(peer).start())
    xs[y, c, slot_rows(e), :] = disp[slot_rows(e), :]
    xs[y_far, c, slot_rows(e), :] = disp_far[slot_rows(e), :]

    def query_copy(r):
        return remote(
            qb.at[x], qb.at[x], q_send.at[r], q_recv.at[r], x=lax.rem(x + r, nx)
        )

    reach = nz // 2

    def key_copies(block, r, to_z):
        return (
            remote(kb.at[block], kb.at[block], k_send.at[r], k_recv.at[r], z=to_z),
            remote(vb.at[block], vb.at[block], v_send.at[r], v_recv.at[r], z=to_z),
        )

    def chain_copies(r):
        return key_copies(jnp.maximum(z - r + 1, 0), r, jnp.minimum(z + 1, nz - 1))

    def far_copies(r):
        return key_copies(z, r, lax.rem(z + r, nz))

    def chain_send(r):
        @pl.when((z + 1 < nz) & (z - r + 1 >= 0))
        def _():
            for copy in chain_copies(r):
                copy.start()

    def send_queries_and_keys():
        chain_send(1)
        for j in range(CHUNKS):
            each_other(nearby(j) * per_chunk, per_chunk, lambda peer: dispatch_far(peer).start())
        for r in range(reach + 1, nz):

            @pl.when(z + r < nz)
            def _(r=r):
                for copy in far_copies(r):
                    copy.start()

        for r in range(1, nx):
            query_copy(r).start()

    maps = 2 * rows
    qk = LANES // 2
    keep_low = lax.broadcasted_iota(jnp.int32, (rows, LANES), 1) < qk

    def stack_query(value, index):
        scaled = value.astype(F32) * (qk ** (-0.5))
        qs[index, 0:rows, :] = jnp.where(keep_low, scaled, 0.0).astype(BF16)
        qs[index, rows:maps, :] = jnp.where(keep_low, 0.0, scaled).astype(BF16)

    def attend(key_block, value_block, masked):
        def one(index):
            scores = lax.dot_general(
                key_block[...],
                qs[index],
                (((1,), (1,)), ((), ())),
                preferred_element_type=F32,
            )
            if masked:
                key_pos = x * rows + lax.broadcasted_iota(jnp.int32, scores.shape, 0)
                column = lax.broadcasted_iota(jnp.int32, scores.shape, 1)
                query_pos = index * rows + jnp.where(column >= rows, column - rows, column)
                visible = query_pos >= key_pos
                scores = jnp.where(visible, scores, LOWEST)
                new_max = jnp.max(scores, axis=0, keepdims=True)
                terms = jnp.where(visible, jnp.exp(scores - new_max), 0.0)
                stat[index, 1:2, :] = jnp.sum(terms, axis=0, keepdims=True)
            else:
                old_max = stat[index, 0:1, :]
                new_max = jnp.maximum(old_max, jnp.max(scores, axis=0, keepdims=True))
                terms = jnp.exp(scores - new_max)
                factor = jnp.exp(old_max - new_max)
                stat[index, 1:2, :] = stat[index, 1:2, :] * factor + jnp.sum(
                    terms, axis=0, keepdims=True
                )
            stat[index, 0:1, :] = new_max
            weighted = lax.dot_general(
                value_block[...],
                terms.astype(BF16),
                (((0,), (0,)), ((), ())),
                preferred_element_type=F32,
            )
            if masked:
                acc[index] = weighted
            else:
                acc[index] = acc[index] * factor + weighted

        loop(0, nx, one)

    def own_attention():
        stack_query(qb[x], x)
        for r in range(1, nx):
            query_copy(r).wait_recv()
            from_x = lax.rem(x + nx - r, nx)
            stack_query(qb[from_x], from_x)
        stat[...] = jnp.zeros_like(stat)
        attend(kb.at[z], vb.at[z], True)

    def chain_step(r):
        @pl.when(z >= r)
        def _():
            for copy in key_copies(jnp.maximum(z - r, 0), r, z):
                copy.wait_recv()
            if r < reach:
                chain_send(r + 1)

    def attend_far(r):
        @pl.when(z >= r)
        def _():
            from_z = jnp.maximum(z - r, 0)
            if r > reach:
                for copy in key_copies(from_z, r, z):
                    copy.wait_recv()
            attend(kb.at[from_z], vb.at[from_z], False)

    def wait_dispatch(peer):
        remote(
            disp.at[slot_rows(0)],
            xs.at[y, c, slot_rows(peer)],
            a_send.at[peer],
            a_recv.at[peer],
            z=z,
            x=x,
        ).wait_recv()

    def chunk_rows(k):
        return pl.ds(pl.multiple_of(k * chunk, chunk), chunk)

    def up_copy(s, k):
        where = chunk_rows(k)
        block = xs.at[y_at(-s), c, where]
        return remote(block, block, up_send.at[k, s], up_recv.at[k, s], y=y_next)

    def dn_copy(s, k):
        where = chunk_rows(k)
        block = xs.at[y_at(s), c, where]
        return remote(block, block, dn_send.at[k, s], dn_recv.at[k, s], y=y_prev)

    def up_arrival(s, k):
        where = chunk_rows(k)
        block = xs.at[y_at(-s - 1), c, where]
        return remote(block, block, up_send.at[k, s], up_recv.at[k, s], y=y_next)

    def dn_arrival(s, k):
        where = chunk_rows(k)
        block = xs.at[y_at(s + 1), c, where]
        return remote(block, block, dn_send.at[k, s], dn_recv.at[k, s], y=y_prev)

    def mate_block(number, k, core):
        shift = (0, -1, 1, -2, 2, -3, 3, half_ring)[number]
        return xs.at[y_at(shift), core, chunk_rows(k)]

    def mate_copy(number, k):
        block = mate_block(number, k, c)
        return remote(block, block, m_send.at[k, number], m_recv.at[k, number], c=other)

    def mate_arrival(number, k):
        block = mate_block(number, k, other)
        return remote(block, block, m_send.at[k, number], m_recv.at[k, number], c=other)

    def first_sends(k):
        each_other(k * per_chunk, per_chunk, wait_dispatch)
        up_copy(0, k).start()
        dn_copy(0, k).start()
        mate_copy(0, k).start()

    def pass_on(s, k):
        up_arrival(s, k).wait_recv()
        if s + 2 < half_ring:
            up_copy(s + 1, k).start()
        mate_copy(2 * s + 1, k).start()
        dn_arrival(s, k).wait_recv()
        if s + 2 < half_ring:
            dn_copy(s + 1, k).start()
        mate_copy(2 * s + 2, k).start()

    def far_rows(k):
        def wait_far(peer):
            remote(
                disp_far.at[slot_rows(0)],
                xs.at[y_far, c, slot_rows(peer)],
                f_send.at[peer],
                f_recv.at[peer],
                z=z,
                x=x,
            ).wait_recv()

        each_other(k * per_chunk, per_chunk, wait_far)
        mate_copy(ny - 1, k).start()

    def result_copies(r):
        to_x = lax.rem(x + r, nx)
        return (
            remote(o_out.at[to_x], o_in.at[x], o_send.at[r], o_recv.at[r], x=to_x),
            remote(stat.at[to_x], stat_in.at[x], s_send.at[r], s_recv.at[r], x=to_x),
        )

    def result_arrivals(r):
        from_x = lax.rem(x + nx - r, nx)
        return (
            remote(o_out.at[0], o_in.at[from_x], o_send.at[r], o_recv.at[r], x=x),
            remote(stat.at[0], stat_in.at[from_x], s_send.at[r], s_recv.at[r], x=x),
        )

    def send_results():
        o_out[...] = acc[...].astype(BF16)
        for r in range(1, nx):
            for copy in result_copies(r):
                copy.start()
        o_in[x] = o_out[x]
        stat_in[x] = stat[x]

    def expert(k):
        for number in range(ny):
            mate_arrival(number, k).wait_recv()
        gate = jnp.zeros((chunk, gw.shape[1]), F32)
        up = jnp.zeros((chunk, gw.shape[1]), F32)
        for block in range(ny):
            both = jnp.concatenate(
                [xs[block, 0, chunk_rows(k), :], xs[block, 1, chunk_rows(k), :]], axis=1
            )
            depth = slice(block * 2 * LANES, (block + 1) * 2 * LANES)
            gate += jnp.dot(both, gw[depth, :], preferred_element_type=F32)
            up += jnp.dot(both, uw[depth, :], preferred_element_type=F32)
        hidden = (gate / (1.0 + jnp.exp(-gate)) * up).astype(BF16)
        for block in range(ny):
            columns = slice(block * 2 * LANES, (block + 1) * 2 * LANES)
            value = jnp.dot(hidden, dw[:, columns], preferred_element_type=F32).astype(BF16)
            parts[k, 0, block] = value[:, :LANES]
            parts[k, 1, block] = value[:, LANES:]
        part_copy(k).start()

    def part_copy(k):
        return remote(parts.at[k, other], mate.at[k], pm_send.at[k], pm_recv.at[k], c=other)

    full = slice(0, chunk)
    top = slice(0, half)
    bottom = slice(half, chunk)

    def chip_sum(k, target, where):
        return parts[k, c, target, where, :].astype(F32) + mate[k, target, where, :].astype(F32)

    def sum_up(k, d):
        where = top if d == half_ring else full
        return remote(
            sb_up.at[k, d - 1, where], rb_up.at[k, d - 1, where],
            ru_send.at[k, d - 1], ru_recv.at[k, d - 1], y=y_next,
        )

    def sum_dn(k, d):
        where = bottom if d == half_ring else full
        return remote(
            sb_dn.at[k, d - 1, where], rb_dn.at[k, d - 1, where],
            rd_send.at[k, d - 1], rd_recv.at[k, d - 1], y=y_prev,
        )

    def sum_step(k, d):
        if d == half_ring:
            sb_up[k, d - 1, top] = chip_sum(k, y_at(d), top).astype(BF16)
            sum_up(k, d).start()
            sb_dn[k, d - 1, bottom] = chip_sum(k, y_at(-d), bottom).astype(BF16)
            sum_dn(k, d).start()
            return
        sum_up(k, d + 1).wait_recv()
        if d + 1 == half_ring:
            sb_up[k, d - 1, top] = (
                chip_sum(k, y_at(d), top) + rb_up[k, d, top].astype(F32)
            ).astype(BF16)
            sb_up[k, d - 1, bottom] = chip_sum(k, y_at(d), bottom).astype(BF16)
        else:
            sb_up[k, d - 1] = (
                chip_sum(k, y_at(d), full) + rb_up[k, d].astype(F32)
            ).astype(BF16)
        sum_up(k, d).start()
        sum_dn(k, d + 1).wait_recv()
        if d + 1 == half_ring:
            sb_dn[k, d - 1, bottom] = (
                chip_sum(k, y_at(-d), bottom) + rb_dn[k, d, bottom].astype(F32)
            ).astype(BF16)
            sb_dn[k, d - 1, top] = chip_sum(k, y_at(-d), top).astype(BF16)
        else:
            sb_dn[k, d - 1] = (
                chip_sum(k, y_at(-d), full) + rb_dn[k, d].astype(F32)
            ).astype(BF16)
        sum_dn(k, d).start()

    def answer(k):
        sum_up(k, 1).wait_recv()
        sum_dn(k, 1).wait_recv()
        ans[chunk_rows(k), :] = (
            chip_sum(k, y, full) + rb_up[k, 0].astype(F32) + rb_dn[k, 0].astype(F32)
        ).astype(BF16)
        each_other(k * per_chunk, per_chunk, lambda target: back_copy(target).start())

    def back_copy(target):
        return remote(
            ans.at[slot_rows(target)],
            ret.at[slot_rows(e)],
            b_send.at[target],
            b_recv.at[e],
            z=target // nx,
            x=lax.rem(target, nx),
        )

    def first_sum(k):
        part_copy(k).wait_recv()
        sum_step(k, half_ring)

    top_rows = pl.ds(0, rows // 2)
    low_rows = pl.ds(rows // 2, rows // 2)
    all_rows = pl.ds(0, rows)

    def head_up(s, hop):
        where = top_rows if s == half_ring - 1 else all_rows
        block = heads.at[y_at(-s - hop), c, where]
        return remote(block, block, hu_send.at[s], hu_recv.at[s], y=y_next)

    def head_dn(s, hop):
        where = low_rows if s == half_ring - 1 else all_rows
        block = heads.at[y_at(s + hop), c, where]
        return remote(block, block, hd_send.at[s], hd_recv.at[s], y=y_prev)

    def head_mate(number, core):
        s = (number - 1) // 2
        last = number > 0 and s == half_ring - 1
        if number == 0:
            block = heads.at[y, core]
        elif number % 2 == 1:
            block = heads.at[y_at(-s - 1), core, top_rows if last else all_rows]
        else:
            block = heads.at[y_at(s + 1), core, low_rows if last else all_rows]
        return remote(block, block, hm_send.at[number], hm_recv.at[number], c=other)

    def head_pass(s):
        head_up(s, 1).wait_recv()
        if s + 1 < half_ring:
            head_up(s + 1, 0).start()
        head_mate(2 * s + 1, c).start()
        head_dn(s, 1).wait_recv()
        if s + 1 < half_ring:
            head_dn(s + 1, 0).start()
        head_mate(2 * s + 2, c).start()

    def merge():
        for r in range(1, nx):
            for copy in result_arrivals(r):
                copy.wait_recv()
        top_max = stat_in[0, 0:1, :]
        for j in range(1, nx):
            top_max = jnp.maximum(top_max, stat_in[j, 0:1, :])
        denominator = jnp.zeros_like(top_max)
        weighted = jnp.zeros(o_in.shape[1:], F32)
        for j in range(nx):
            factor = jnp.exp(stat_in[j, 0:1, :] - top_max)
            denominator += factor * stat_in[j, 1:2, :]
            weighted += factor * o_in[j].astype(F32)
        mapped = weighted / denominator
        difference = mapped[:, :rows] - scale_ref[0:1, 0:1] * mapped[:, rows:]
        mean = jnp.sum(difference * difference, axis=0, keepdims=True) * (1.0 / LANES)
        head = difference * lax.rsqrt(mean + EPSILON)
        heads[y, c] = (head.T * hgain_ref[...]).astype(BF16)
        head_up(0, 0).start()
        head_dn(0, 0).start()
        head_mate(0, c).start()

    def weights_and_expert(k):
        if not weights_here:
            weights_here.append(True)
            for copy in weight_copies[:3]:
                copy.wait()
        expert(k)

    def sum_stage(d, k):
        if d == half_ring:
            first_sum(k)
        elif d > 0:
            sum_step(k, d)
        else:
            answer(k)

    def gather_stage(s, k):
        if s == 0:
            first_sends(k)
        else:
            pass_on(s - 1, k)

    weights_here = []
    stages = {
        "gather": lambda s, j: gather_stage(s, nearby(j)),
        "inputs": send_queries_and_keys,
        "far": lambda j: far_rows(nearby(j)),
        "chain": chain_step,
        "own": own_attention,
        "attend": attend_far,
        "expert": lambda j: weights_and_expert(nearby(j)),
        "sum": lambda d, j: sum_stage(d, nearby(j)),
        "results": send_results,
        "merge": merge,
        "heads": lambda s: head_pass(s - 1),
        "project": lambda: None,
    }
    for stage in ORDER:
        stages[stage[0]](*stage[1:])
    ret[slot_rows(e), :] = ans[slot_rows(e), :]

    weight_copies[3].wait()
    for number in range(2 * half_ring + 1):
        head_mate(number, other).wait_recv()
    mixed = jnp.zeros((rows, LANES), F32)
    for block in range(ny):
        both = jnp.concatenate([heads[block, 0], heads[block, 1]], axis=1)
        mixed += jnp.dot(
            both, ow[block * 2 * LANES : (block + 1) * 2 * LANES, :], preferred_element_type=F32
        )
    mix_ref[...] = mixed.astype(BF16)

    def wait_back(peer):
        remote(
            ans.at[slot_rows(0)],
            ret.at[slot_rows(peer)],
            b_send.at[peer],
            b_recv.at[peer],
            z=z,
            x=x,
        ).wait_recv()

    each_other(0, nep, wait_back)
    routed = jnp.zeros((LANES, rows), F32)
    for i in range(2):
        routed += weight[i : i + 1, :] * lax.dot_general(
            ret[...], one_hot(i), (((0,), (0,)), ((), ())), preferred_element_type=F32
        )
    rout_ref[...] = routed.T.astype(BF16)

    def drain(peer):
        dispatch(peer).wait_send()
        dispatch_far(peer).wait_send()
        back_copy(peer).wait_send()

    each_other(0, nep, drain)

    def drain_chunk(k):
        for s in range(half_ring - 1):
            up_copy(s, k).wait_send()
            dn_copy(s, k).wait_send()
        for d in range(1, half_ring + 1):
            sum_up(k, d).wait_send()
            sum_dn(k, d).wait_send()
        for number in range(ny):
            mate_copy(number, k).wait_send()
        part_copy(k).wait_send()

    loop(0, CHUNKS, drain_chunk)
    for r in range(1, nx):
        query_copy(r).wait_send()
        for copy in result_copies(r):
            copy.wait_send()
    for r in range(1, reach + 1):

        @pl.when((z + 1 < nz) & (z - r + 1 >= 0))
        def _(r=r):
            for copy in chain_copies(r):
                copy.wait_send()

    for r in range(reach + 1, nz):

        @pl.when(z + r < nz)
        def _(r=r):
            for copy in far_copies(r):
                copy.wait_send()

    for s in range(half_ring):
        head_up(s, 0).wait_send()
        head_dn(s, 0).wait_send()
    for number in range(2 * half_ring + 1):
        head_mate(number, c).wait_send()


def local(
    sizes,
    queries,
    key_rows,
    values,
    second_scale,
    head_gain,
    out_weight,
    routed_in,
    routed_gain,
    expert_ids,
    group_logits,
    inner_logits,
    gate_weight,
    up_weight,
    down_weight,
):
    nz, nx, ny = sizes
    nep = nz * nx
    rows = routed_in.shape[0]
    width = routed_in.shape[1]
    hidden = gate_weight.shape[2]
    cap = 2 * expert_ids.shape[1] * rows // nep
    total = nep * cap
    chunk = total // CHUNKS
    half_ring = ny // 2
    mates = 2 * half_ring + 1
    dma = pltpu.SemaphoreType.DMA
    vmem = pltpu.VMEM
    scratch = [
        vmem((width, hidden), BF16),
        vmem((width, hidden), BF16),
        vmem((hidden, width), BF16),
        vmem(out_weight.shape, BF16),
        vmem((rows, width), BF16),
        vmem((1, 1), F32),
        vmem((1, LANES), F32),
        vmem((1, width), F32),
        vmem((2, rows), jnp.int32),
        vmem((group_logits.shape[1], rows), F32),
        vmem((2, rows), F32),
        dma((4,)),
        dma((10,)),
        vmem((8, rows), F32),
        vmem((8, rows), F32),
        vmem((total, LANES), BF16),
        vmem((total, LANES), BF16),
        vmem((ny, 2, total, LANES), BF16),
        vmem((CHUNKS, 2, ny, chunk, LANES), BF16),
        vmem((CHUNKS, ny, chunk, LANES), BF16),
        vmem((CHUNKS, half_ring, chunk, LANES), BF16),
        vmem((CHUNKS, half_ring, chunk, LANES), BF16),
        vmem((CHUNKS, half_ring, chunk, LANES), BF16),
        vmem((CHUNKS, half_ring, chunk, LANES), BF16),
        vmem((total, LANES), BF16),
        vmem((total, LANES), BF16),
        dma((nep,)),
        dma((nep,)),
        dma((nep,)),
        dma((nep,)),
        dma((CHUNKS, half_ring)),
        dma((CHUNKS, half_ring)),
        dma((CHUNKS, half_ring)),
        dma((CHUNKS, half_ring)),
        dma((CHUNKS, mates)),
        dma((CHUNKS, mates)),
        dma((CHUNKS,)),
        dma((CHUNKS,)),
        dma((CHUNKS, half_ring)),
        dma((CHUNKS, half_ring)),
        dma((CHUNKS, half_ring)),
        dma((CHUNKS, half_ring)),
        dma((nep,)),
        dma((nep,)),
        vmem((nx, rows, LANES), BF16),
        vmem((nx, 2 * rows, LANES), BF16),
        vmem((nz, rows, LANES), BF16),
        vmem((nz, rows, LANES), BF16),
        vmem((nx, LANES, 2 * rows), F32),
        vmem((nx, 8, 2 * rows), F32),
        vmem((nx, LANES, 2 * rows), BF16),
        vmem((nx, LANES, 2 * rows), BF16),
        vmem((nx, 8, 2 * rows), F32),
        vmem((ny, 2, rows, LANES), BF16),
        dma((nx,)),
        dma((nx,)),
        dma((nz,)),
        dma((nz,)),
        dma((nz,)),
        dma((nz,)),
        dma((nx,)),
        dma((nx,)),
        dma((nx,)),
        dma((nx,)),
        dma((half_ring,)),
        dma((half_ring,)),
        dma((half_ring,)),
        dma((half_ring,)),
        dma((mates,)),
        dma((mates,)),
    ]
    whole = pl.BlockSpec(memory_space=pltpu.VMEM)
    far = pl.BlockSpec(memory_space=pl.ANY)
    return pl.pallas_call(
        lambda *refs: kernel(sizes, *refs),
        out_shape=(
            jax.ShapeDtypeStruct((rows, LANES), BF16),
            jax.ShapeDtypeStruct((rows, LANES), BF16),
        ),
        in_specs=[far] * 14,
        out_specs=(whole, whole),
        scratch_shapes=scratch,
        compiler_params=pltpu.CompilerParams(
            collective_id=0, has_side_effects=True, vmem_limit_bytes=60 * 1024 * 1024
        ),
    )(
        queries,
        key_rows,
        values,
        second_scale.reshape(1, 1),
        head_gain.reshape(1, -1),
        out_weight,
        routed_in,
        routed_gain.reshape(1, -1),
        expert_ids.T,
        group_logits.T,
        inner_logits.T,
        gate_weight[0],
        up_weight[0],
        down_weight[0],
    )


def build(mesh, sizes):
    nz, nx, ny = sizes
    finer = Mesh(mesh.devices.reshape(nz, nx, ny, 2), ("z", "x", "y", "c"))
    ep, tp = ("z", "x"), ("y", "c")
    placed = (
        P(ep, tp),
        P(ep, tp),
        P(ep, tp),
        P(tp),
        P(),
        P(None, tp),
        P(ep, None),
        P(),
        P(ep, None),
        P(ep, None),
        P(ep, None),
        P(ep, None, tp),
        P(ep, None, tp),
        P(ep, tp, None),
    )
    return jax.shard_map(
        lambda *args: local(sizes, *args),
        mesh=finer,
        in_specs=placed,
        out_specs=(P(ep, tp), P(ep, tp)),
        check_vma=False,
    )


def solution(mesh):
    return build(mesh, (8, 4, mesh.shape["tp"] // 2))
```

```python
import jax
import jax.numpy as jnp
from jax import lax
from jax.experimental import pallas as pl
from jax.experimental.pallas import tpu as pltpu
from jax.sharding import Mesh
from jax.sharding import PartitionSpec as P

EPSILON = 1e-05
LOWEST = -1e30
GROUP_SIZE = 4
LANES = 128
CHUNKS = 4
ORDER = (
    ("gather", 0, 0),
    ("inputs",),
    ("gather", 0, 1),
    ("gather", 1, 0),
    ("gather", 0, 2),
    ("gather", 0, 3),
    ("own",),
    ("gather", 1, 1),
    ("chain", 1),
    ("keys",),
    ("gather", 2, 0),
    ("attend", 1),
    ("gather", 1, 2),
    ("gather", 1, 3),
    ("far", 0),
    ("gather", 2, 1),
    ("far", 1),
    ("gather", 3, 0),
    ("chain", 2),
    ("attend", 2),
    ("gather", 2, 2),
    ("expert", 0),
    ("far", 3),
    ("gather", 2, 3),
    ("far", 2),
    ("gather", 3, 1),
    ("sum", 4, 0),
    ("expert", 1),
    ("chain", 3),
    ("gather", 3, 2),
    ("attend", 3),
    ("gather", 3, 3),
    ("sum", 4, 1),
    ("expert", 2),
    ("expert", 3),
    ("sum", 3, 0),
    ("sum", 4, 2),
    ("sum", 3, 1),
    ("chain", 4),
    ("attend", 4),
    ("attend", 5),
    ("sum", 2, 0),
    ("attend", 6),
    ("attend", 7),
    ("results",),
    ("sum", 4, 3),
    ("sum", 2, 1),
    ("sum", 1, 0),
    ("sum", 3, 2),
    ("sum", 3, 3),
    ("sum", 1, 1),
    ("sum", 0, 0),
    ("merge",),
    ("sum", 2, 2),
    ("sum", 2, 3),
    ("sum", 0, 1),
    ("heads", 1),
    ("sum", 1, 2),
    ("sum", 1, 3),
    ("heads", 2),
    ("sum", 0, 2),
    ("sum", 0, 3),
    ("heads", 3),
    ("heads", 4),
    ("project",),
)
F32 = jnp.float32
BF16 = jnp.bfloat16


def remote(src, dst, send_sem, recv_sem, **where):
    return pltpu.make_async_remote_copy(
        src_ref=src,
        dst_ref=dst,
        send_sem=send_sem,
        recv_sem=recv_sem,
        device_id=where,
        device_id_type=pl.DeviceIdType.MESH,
    )


def loop(first, last, body):
    def step(i, carry):
        body(i)
        return carry

    lax.fori_loop(first, last, step, 0)


def kernel(
    sizes,
    q_hbm,
    k_hbm,
    v_hbm,
    scale_hbm,
    hgain_hbm,
    ow_hbm,
    rin_hbm,
    rgain_hbm,
    ids_hbm,
    gl_hbm,
    il_hbm,
    gw_hbm,
    uw_hbm,
    dw_hbm,
    out_ref,
    gw,
    uw,
    dw,
    ow,
    rin,
    scale_ref,
    hgain_ref,
    rgain_ref,
    ids_ref,
    gl_ref,
    il_ref,
    w_sem,
    i_sem,
    pos,
    weight,
    disp,
    disp_far,
    xs,
    parts,
    mate,
    rb_up,
    rb_dn,
    sb_up,
    sb_dn,
    ans,
    ret,
    a_send,
    a_recv,
    f_send,
    f_recv,
    up_send,
    up_recv,
    dn_send,
    dn_recv,
    m_send,
    m_recv,
    pm_send,
    pm_recv,
    ru_send,
    ru_recv,
    rd_send,
    rd_recv,
    b_send,
    b_recv,
    qb,
    qs,
    kb,
    vb,
    acc,
    stat,
    o_out,
    o_in,
    stat_in,
    heads,
    q_send,
    q_recv,
    k_send,
    k_recv,
    v_send,
    v_recv,
    o_send,
    o_recv,
    s_send,
    s_recv,
    hu_send,
    hu_recv,
    hd_send,
    hd_recv,
    hm_send,
    hm_recv,
):
    nz, nx, ny = sizes
    nep = nz * nx
    half_ring = ny // 2
    z, x, y, c = (lax.axis_index(name) for name in ("z", "x", "y", "c"))
    other = 1 - c
    e = z * nx + x
    t = y * 2 + c
    rows = rin.shape[0]
    width = rin.shape[1]
    total = xs.shape[2]
    cap = total // nep
    chunk = total // CHUNKS
    half = chunk // 2
    per_chunk = nep // CHUNKS
    y_next = lax.rem(y + 1, ny)
    y_prev = lax.rem(y + ny - 1, ny)

    def y_at(shift):
        return lax.rem(y + shift + ny, ny)

    group = z // (nz // CHUNKS)

    def nearby(j):
        return lax.rem(group + (0, 1, 3, 2)[j], CHUNKS)

    def each_other(first, count, body):
        def one(i):
            @pl.when(first + i != e)
            def _():
                body(first + i)

        loop(0, count, one)


    input_copies = [
        pltpu.make_async_copy(src, dst, i_sem.at[i])
        for i, (src, dst) in enumerate(
            (
                (rin_hbm, rin),
                (ids_hbm, ids_ref),
                (gl_hbm, gl_ref),
                (il_hbm, il_ref),
                (rgain_hbm, rgain_ref),
                (q_hbm, qb.at[x]),
                (k_hbm, kb.at[z]),
                (v_hbm, vb.at[z]),
                (scale_hbm, scale_ref),
                (hgain_hbm, hgain_ref),
            )
        )
    ]
    weight_copies = [
        pltpu.make_async_copy(src, dst, w_sem.at[i])
        for i, (src, dst) in enumerate(
            ((gw_hbm, gw), (uw_hbm, uw), (dw_hbm, dw), (ow_hbm, ow))
        )
    ]
    for copy in input_copies:
        copy.start()

    barrier = pltpu.get_barrier_semaphore()

    def greet(**where):
        pl.semaphore_signal(
            barrier, inc=1, device_id=where, device_id_type=pl.DeviceIdType.MESH
        )

    near_z = [lax.rem(z + d, nz) for d in range(nz)]
    near_x = [lax.rem(x + d, nx) for d in range(nx)]
    apart = [(i, j) for i in range(nz) for j in range(nx) if i + j > 0]
    for i, j in sorted(apart, key=lambda ij: -min(ij[0], nz - ij[0]) - min(ij[1], nx - ij[1])):
        greet(z=near_z[i], x=near_x[j])
    greet(y=y_next)
    greet(y=y_prev)
    greet(c=other)

    for copy in input_copies[1:5]:
        copy.wait()
    ids = ids_ref[...]
    shape = (nep, rows)
    expert_row = lax.broadcasted_iota(jnp.int32, shape, 0)
    picks = [jnp.where(ids[i : i + 1, :] == expert_row, 1.0, 0.0) for i in range(2)]
    earlier = jnp.where(
        lax.broadcasted_iota(jnp.int32, (rows, rows), 0)
        < lax.broadcasted_iota(jnp.int32, (rows, rows), 1),
        1.0,
        0.0,
    ).astype(BF16)
    before = [jnp.dot(pick.astype(BF16), earlier, preferred_element_type=F32) for pick in picks]
    before[1] += jnp.sum(picks[0], axis=1, keepdims=True)
    logits = gl_ref[...]
    group_exp = jnp.exp(logits - jnp.max(logits, axis=0, keepdims=True))
    group_prob = group_exp / jnp.sum(group_exp, axis=0, keepdims=True)
    group_row = lax.broadcasted_iota(jnp.int32, logits.shape, 0)
    inner = il_ref[...]
    inner_exp = jnp.exp(inner - jnp.max(inner, axis=0, keepdims=True))
    inner_prob = inner_exp / jnp.sum(inner_exp, axis=0, keepdims=True)
    for i in range(2):
        pos[i : i + 1, :] = ids[i : i + 1, :].astype(F32) * cap + jnp.sum(
            picks[i] * before[i], axis=0, keepdims=True
        )
        chosen = ids[i : i + 1, :] // GROUP_SIZE == group_row
        picked = jnp.sum(jnp.where(chosen, group_prob, 0.0), axis=0, keepdims=True)
        weight[i : i + 1, :] = picked * inner_prob[i : i + 1, :]

    def one_hot(i):
        slots = lax.broadcasted_iota(jnp.int32, (total, rows), 0).astype(F32)
        return jnp.where(pos[i : i + 1, :] == slots, 1.0, 0.0).astype(BF16)

    input_copies[0].wait()
    source = rin[...].astype(F32)
    inv = lax.rsqrt(jnp.sum(source * source, axis=-1, keepdims=True) * (1.0 / width) + EPSILON)

    def normed(block):
        columns = pl.ds(pl.multiple_of((block * 2 + c) * LANES, LANES), LANES)
        return (rin[:, columns].astype(F32) * inv * rgain_ref[:, columns]).astype(BF16)

    y_far = y_at(half_ring)
    spread = jnp.dot(
        one_hot(0) + one_hot(1),
        jnp.concatenate([normed(y), normed(y_far)], axis=1),
        preferred_element_type=F32,
    ).astype(BF16)
    disp[...] = spread[:, :LANES]
    disp_far[...] = spread[:, LANES:]
    for copy in input_copies[5:]:
        copy.wait()
    for copy in weight_copies:
        copy.start()

    pl.semaphore_wait(barrier, nep - 1 + 2 + 1)

    def slot_rows(index):
        return pl.ds(pl.multiple_of(index * cap, cap), cap)

    def dispatch(peer):
        return remote(
            disp.at[slot_rows(peer)],
            xs.at[y, c, slot_rows(e)],
            a_send.at[peer],
            a_recv.at[e],
            z=peer // nx,
            x=lax.rem(peer, nx),
        )

    def dispatch_far(peer):
        return remote(
            disp_far.at[slot_rows(peer)],
            xs.at[y_far, c, slot_rows(e)],
            f_send.at[peer],
            f_recv.at[e],
            z=peer // nx,
            x=lax.rem(peer, nx),
        )

    for j in range(CHUNKS):
        each_other(nearby(j) * per_chunk, per_chunk, lambda peer: dispatch(peer).start())
    xs[y, c, slot_rows(e), :] = disp[slot_rows(e), :]
    xs[y_far, c, slot_rows(e), :] = disp_far[slot_rows(e), :]

    def query_copy(r):
        return remote(
            qb.at[x], qb.at[x], q_send.at[r], q_recv.at[r], x=lax.rem(x + r, nx)
        )

    reach = nz // 2

    def key_copies(block, r, to_z):
        return (
            remote(kb.at[block], kb.at[block], k_send.at[r], k_recv.at[r], z=to_z),
            remote(vb.at[block], vb.at[block], v_send.at[r], v_recv.at[r], z=to_z),
        )

    def chain_copies(r):
        return key_copies(jnp.maximum(z - r + 1, 0), r, jnp.minimum(z + 1, nz - 1))

    def far_copies(r):
        return key_copies(z, r, lax.rem(z + r, nz))

    def chain_send(r):
        @pl.when((z + 1 < nz) & (z - r + 1 >= 0))
        def _():
            for copy in chain_copies(r):
                copy.start()

    def send_inputs():
        for r in range(1, nx):
            query_copy(r).start()
        chain_send(1)
        for j in range(CHUNKS):
            each_other(nearby(j) * per_chunk, per_chunk, lambda peer: dispatch_far(peer).start())

    def send_far_keys():
        for r in range(reach + 1, nz):

            @pl.when(z + r < nz)
            def _(r=r):
                for copy in far_copies(r):
                    copy.start()

    maps = 2 * rows
    qk = LANES // 2
    keep_low = lax.broadcasted_iota(jnp.int32, (rows, LANES), 1) < qk

    def stack_query(value, index):
        scaled = value.astype(F32) * (qk ** (-0.5))
        qs[index, 0:rows, :] = jnp.where(keep_low, scaled, 0.0).astype(BF16)
        qs[index, rows:maps, :] = jnp.where(keep_low, 0.0, scaled).astype(BF16)

    def attend(key_block, value_block, masked):
        keys = key_block[...]
        values = value_block[...].T

        def one(index):
            scores = lax.dot_general(
                keys,
                qs[index],
                (((1,), (1,)), ((), ())),
                preferred_element_type=F32,
            )
            if masked:
                key_pos = x * rows + lax.broadcasted_iota(jnp.int32, scores.shape, 0)
                column = lax.broadcasted_iota(jnp.int32, scores.shape, 1)
                query_pos = index * rows + jnp.where(column >= rows, column - rows, column)
                visible = query_pos >= key_pos
                scores = jnp.where(visible, scores, LOWEST)
                new_max = jnp.max(scores, axis=0, keepdims=True)
                terms = jnp.where(visible, jnp.exp(scores - new_max), 0.0)
                stat[index, 1:2, :] = jnp.sum(terms, axis=0, keepdims=True)
            else:
                old_max = stat[index, 0:1, :]
                new_max = jnp.maximum(old_max, jnp.max(scores, axis=0, keepdims=True))
                terms = jnp.exp(scores - new_max)
                factor = jnp.exp(old_max - new_max)
                stat[index, 1:2, :] = stat[index, 1:2, :] * factor + jnp.sum(
                    terms, axis=0, keepdims=True
                )
            stat[index, 0:1, :] = new_max
            weighted = jnp.dot(values, terms.astype(BF16), preferred_element_type=F32)
            if masked:
                acc[index] = weighted
            else:
                acc[index] = acc[index] * factor + weighted

        for index in range(nx):
            one(index)

    def own_attention():
        stack_query(qb[x], x)
        for r in range(1, nx):
            query_copy(r).wait_recv()
            from_x = lax.rem(x + nx - r, nx)
            stack_query(qb[from_x], from_x)
        stat[...] = jnp.zeros_like(stat)
        attend(kb.at[z], vb.at[z], True)

    def chain_step(r):
        @pl.when(z >= r)
        def _():
            for copy in key_copies(jnp.maximum(z - r, 0), r, z):
                copy.wait_recv()
            if r < reach:
                chain_send(r + 1)

    def attend_far(r):
        @pl.when(z >= r)
        def _():
            from_z = jnp.maximum(z - r, 0)
            if r > reach:
                for copy in key_copies(from_z, r, z):
                    copy.wait_recv()
            attend(kb.at[from_z], vb.at[from_z], False)

    def wait_dispatch(peer):
        remote(
            disp.at[slot_rows(0)],
            xs.at[y, c, slot_rows(peer)],
            a_send.at[peer],
            a_recv.at[peer],
            z=z,
            x=x,
        ).wait_recv()

    def chunk_rows(k):
        return pl.ds(pl.multiple_of(k * chunk, chunk), chunk)

    def up_copy(s, k):
        where = chunk_rows(k)
        block = xs.at[y_at(-s), c, where]
        return remote(block, block, up_send.at[k, s], up_recv.at[k, s], y=y_next)

    def dn_copy(s, k):
        where = chunk_rows(k)
        block = xs.at[y_at(s), c, where]
        return remote(block, block, dn_send.at[k, s], dn_recv.at[k, s], y=y_prev)

    def up_arrival(s, k):
        where = chunk_rows(k)
        block = xs.at[y_at(-s - 1), c, where]
        return remote(block, block, up_send.at[k, s], up_recv.at[k, s], y=y_next)

    def dn_arrival(s, k):
        where = chunk_rows(k)
        block = xs.at[y_at(s + 1), c, where]
        return remote(block, block, dn_send.at[k, s], dn_recv.at[k, s], y=y_prev)

    def mate_block(number, k, core):
        shift = (0, -1, 1, -2, 2, -3, 3, half_ring)[number]
        return xs.at[y_at(shift), core, chunk_rows(k)]

    def mate_copy(number, k):
        block = mate_block(number, k, c)
        return remote(block, block, m_send.at[k, number], m_recv.at[k, number], c=other)

    def mate_arrival(number, k):
        block = mate_block(number, k, other)
        return remote(block, block, m_send.at[k, number], m_recv.at[k, number], c=other)

    def first_sends(k):
        each_other(k * per_chunk, per_chunk, wait_dispatch)
        up_copy(0, k).start()
        dn_copy(0, k).start()
        mate_copy(0, k).start()

    def pass_on(s, k):
        up_arrival(s, k).wait_recv()
        if s + 2 < half_ring:
            up_copy(s + 1, k).start()
        mate_copy(2 * s + 1, k).start()
        dn_arrival(s, k).wait_recv()
        if s + 2 < half_ring:
            dn_copy(s + 1, k).start()
        mate_copy(2 * s + 2, k).start()

    def far_rows(k):
        def wait_far(peer):
            remote(
                disp_far.at[slot_rows(0)],
                xs.at[y_far, c, slot_rows(peer)],
                f_send.at[peer],
                f_recv.at[peer],
                z=z,
                x=x,
            ).wait_recv()

        each_other(k * per_chunk, per_chunk, wait_far)
        mate_copy(ny - 1, k).start()

    def result_copies(r):
        to_x = lax.rem(x + r, nx)
        return (
            remote(o_out.at[to_x], o_in.at[x], o_send.at[r], o_recv.at[r], x=to_x),
            remote(stat.at[to_x], stat_in.at[x], s_send.at[r], s_recv.at[r], x=to_x),
        )

    def result_arrivals(r):
        from_x = lax.rem(x + nx - r, nx)
        return (
            remote(o_out.at[0], o_in.at[from_x], o_send.at[r], o_recv.at[r], x=x),
            remote(stat.at[0], stat_in.at[from_x], s_send.at[r], s_recv.at[r], x=x),
        )

    def send_results():
        o_out[...] = acc[...].astype(BF16)
        for r in range(1, nx):
            for copy in result_copies(r):
                copy.start()
        o_in[x] = o_out[x]
        stat_in[x] = stat[x]

    def expert(k):
        for number in range(ny):
            mate_arrival(number, k).wait_recv()
        gate = jnp.zeros((chunk, gw.shape[1]), F32)
        up = jnp.zeros((chunk, gw.shape[1]), F32)
        for block in range(ny):
            both = jnp.concatenate(
                [xs[block, 0, chunk_rows(k), :], xs[block, 1, chunk_rows(k), :]], axis=1
            )
            depth = slice(block * 2 * LANES, (block + 1) * 2 * LANES)
            gate += jnp.dot(both, gw[depth, :], preferred_element_type=F32)
            up += jnp.dot(both, uw[depth, :], preferred_element_type=F32)
        hidden = (gate / (1.0 + jnp.exp(-gate)) * up).astype(BF16)
        for block in range(ny):
            columns = slice(block * 2 * LANES, (block + 1) * 2 * LANES)
            value = jnp.dot(hidden, dw[:, columns], preferred_element_type=F32).astype(BF16)
            parts[k, 0, block] = value[:, :LANES]
            parts[k, 1, block] = value[:, LANES:]
        part_copy(k).start()

    def part_copy(k):
        return remote(parts.at[k, other], mate.at[k], pm_send.at[k], pm_recv.at[k], c=other)

    full = slice(0, chunk)
    top = slice(0, half)
    bottom = slice(half, chunk)

    def chip_sum(k, target, where):
        return parts[k, c, target, where, :].astype(F32) + mate[k, target, where, :].astype(F32)

    def sum_up(k, d):
        where = top if d == half_ring else full
        return remote(
            sb_up.at[k, d - 1, where], rb_up.at[k, d - 1, where],
            ru_send.at[k, d - 1], ru_recv.at[k, d - 1], y=y_next,
        )

    def sum_dn(k, d):
        where = bottom if d == half_ring else full
        return remote(
            sb_dn.at[k, d - 1, where], rb_dn.at[k, d - 1, where],
            rd_send.at[k, d - 1], rd_recv.at[k, d - 1], y=y_prev,
        )

    def sum_step(k, d):
        if d == half_ring:
            sb_up[k, d - 1, top] = chip_sum(k, y_at(d), top).astype(BF16)
            sum_up(k, d).start()
            sb_dn[k, d - 1, bottom] = chip_sum(k, y_at(-d), bottom).astype(BF16)
            sum_dn(k, d).start()
            return
        sum_up(k, d + 1).wait_recv()
        if d + 1 == half_ring:
            sb_up[k, d - 1, top] = (
                chip_sum(k, y_at(d), top) + rb_up[k, d, top].astype(F32)
            ).astype(BF16)
            sb_up[k, d - 1, bottom] = chip_sum(k, y_at(d), bottom).astype(BF16)
        else:
            sb_up[k, d - 1] = (
                chip_sum(k, y_at(d), full) + rb_up[k, d].astype(F32)
            ).astype(BF16)
        sum_up(k, d).start()
        sum_dn(k, d + 1).wait_recv()
        if d + 1 == half_ring:
            sb_dn[k, d - 1, bottom] = (
                chip_sum(k, y_at(-d), bottom) + rb_dn[k, d, bottom].astype(F32)
            ).astype(BF16)
            sb_dn[k, d - 1, top] = chip_sum(k, y_at(-d), top).astype(BF16)
        else:
            sb_dn[k, d - 1] = (
                chip_sum(k, y_at(-d), full) + rb_dn[k, d].astype(F32)
            ).astype(BF16)
        sum_dn(k, d).start()

    def answer(k):
        sum_up(k, 1).wait_recv()
        sum_dn(k, 1).wait_recv()
        ans[chunk_rows(k), :] = (
            chip_sum(k, y, full) + rb_up[k, 0].astype(F32) + rb_dn[k, 0].astype(F32)
        ).astype(BF16)
        each_other(k * per_chunk, per_chunk, lambda target: back_copy(target).start())

    def back_copy(target):
        return remote(
            ans.at[slot_rows(target)],
            ret.at[slot_rows(e)],
            b_send.at[target],
            b_recv.at[e],
            z=target // nx,
            x=lax.rem(target, nx),
        )

    def first_sum(k):
        part_copy(k).wait_recv()
        sum_step(k, half_ring)

    top_rows = pl.ds(0, rows // 2)
    low_rows = pl.ds(rows // 2, rows // 2)
    all_rows = pl.ds(0, rows)

    def head_up(s, hop):
        where = top_rows if s == half_ring - 1 else all_rows
        block = heads.at[y_at(-s - hop), c, where]
        return remote(block, block, hu_send.at[s], hu_recv.at[s], y=y_next)

    def head_dn(s, hop):
        where = low_rows if s == half_ring - 1 else all_rows
        block = heads.at[y_at(s + hop), c, where]
        return remote(block, block, hd_send.at[s], hd_recv.at[s], y=y_prev)

    def head_mate(number, core):
        s = (number - 1) // 2
        last = number > 0 and s == half_ring - 1
        if number == 0:
            block = heads.at[y, core]
        elif number % 2 == 1:
            block = heads.at[y_at(-s - 1), core, top_rows if last else all_rows]
        else:
            block = heads.at[y_at(s + 1), core, low_rows if last else all_rows]
        return remote(block, block, hm_send.at[number], hm_recv.at[number], c=other)

    def head_pass(s):
        head_up(s, 1).wait_recv()
        if s + 1 < half_ring:
            head_up(s + 1, 0).start()
        head_mate(2 * s + 1, c).start()
        head_dn(s, 1).wait_recv()
        if s + 1 < half_ring:
            head_dn(s + 1, 0).start()
        head_mate(2 * s + 2, c).start()

    def merge():
        for r in range(1, nx):
            for copy in result_arrivals(r):
                copy.wait_recv()
        top_max = stat_in[0, 0:1, :]
        for j in range(1, nx):
            top_max = jnp.maximum(top_max, stat_in[j, 0:1, :])
        denominator = jnp.zeros_like(top_max)
        weighted = jnp.zeros(o_in.shape[1:], F32)
        for j in range(nx):
            factor = jnp.exp(stat_in[j, 0:1, :] - top_max)
            denominator += factor * stat_in[j, 1:2, :]
            weighted += factor * o_in[j].astype(F32)
        mapped = weighted / denominator
        difference = mapped[:, :rows] - scale_ref[0:1, 0:1] * mapped[:, rows:]
        mean = jnp.sum(difference * difference, axis=0, keepdims=True) * (1.0 / LANES)
        head = difference * lax.rsqrt(mean + EPSILON)
        heads[y, c] = (head.T * hgain_ref[...]).astype(BF16)
        head_up(0, 0).start()
        head_dn(0, 0).start()
        head_mate(0, c).start()

    def weights_and_expert(k):
        if not weights_here:
            weights_here.append(True)
            for copy in weight_copies[:3]:
                copy.wait()
        expert(k)

    def sum_stage(d, k):
        if d == half_ring:
            first_sum(k)
        elif d > 0:
            sum_step(k, d)
        else:
            answer(k)

    def gather_stage(s, k):
        if s == 0:
            first_sends(k)
        else:
            pass_on(s - 1, k)

    weights_here = []
    stages = {
        "gather": lambda s, j: gather_stage(s, nearby(j)),
        "inputs": send_inputs,
        "keys": send_far_keys,
        "far": lambda j: far_rows(nearby(j)),
        "chain": chain_step,
        "own": own_attention,
        "attend": attend_far,
        "expert": lambda j: weights_and_expert(nearby(j)),
        "sum": lambda d, j: sum_stage(d, nearby(j)),
        "results": send_results,
        "merge": merge,
        "heads": lambda s: head_pass(s - 1),
        "project": lambda: None,
    }
    for stage in ORDER:
        stages[stage[0]](*stage[1:])
    ret[slot_rows(e), :] = ans[slot_rows(e), :]

    weight_copies[3].wait()
    for number in range(2 * half_ring + 1):
        head_mate(number, other).wait_recv()
    mixed = jnp.zeros((rows, LANES), F32)
    for block in range(ny):
        both = jnp.concatenate([heads[block, 0], heads[block, 1]], axis=1)
        mixed += jnp.dot(
            both, ow[block * 2 * LANES : (block + 1) * 2 * LANES, :], preferred_element_type=F32
        )
    out_ref[0] = mixed.astype(BF16)

    def drain(peer):
        dispatch(peer).wait_send()
        dispatch_far(peer).wait_send()

    each_other(0, nep, drain)

    def drain_chunk(k):
        for s in range(half_ring - 1):
            up_copy(s, k).wait_send()
            dn_copy(s, k).wait_send()
        for d in range(1, half_ring + 1):
            sum_up(k, d).wait_send()
            sum_dn(k, d).wait_send()
        for number in range(ny):
            mate_copy(number, k).wait_send()
        part_copy(k).wait_send()

    loop(0, CHUNKS, drain_chunk)
    for r in range(1, nx):
        query_copy(r).wait_send()
        for copy in result_copies(r):
            copy.wait_send()
    for r in range(1, reach + 1):

        @pl.when((z + 1 < nz) & (z - r + 1 >= 0))
        def _(r=r):
            for copy in chain_copies(r):
                copy.wait_send()

    for r in range(reach + 1, nz):

        @pl.when(z + r < nz)
        def _(r=r):
            for copy in far_copies(r):
                copy.wait_send()

    for s in range(half_ring):
        head_up(s, 0).wait_send()
        head_dn(s, 0).wait_send()
    for number in range(2 * half_ring + 1):
        head_mate(number, c).wait_send()

    def wait_back(peer):
        remote(
            ans.at[slot_rows(0)],
            ret.at[slot_rows(peer)],
            b_send.at[peer],
            b_recv.at[peer],
            z=z,
            x=x,
        ).wait_recv()

    each_other(0, nep, wait_back)
    routed = jnp.zeros((LANES, rows), F32)
    for i in range(2):
        routed += weight[i : i + 1, :] * lax.dot_general(
            ret[...], one_hot(i), (((0,), (0,)), ((), ())), preferred_element_type=F32
        )
    out_ref[1] = routed.T.astype(BF16)

    each_other(0, nep, lambda peer: back_copy(peer).wait_send())


def local(
    sizes,
    queries,
    key_rows,
    values,
    second_scale,
    head_gain,
    out_weight,
    routed_in,
    routed_gain,
    expert_ids,
    group_logits,
    inner_logits,
    gate_weight,
    up_weight,
    down_weight,
):
    nz, nx, ny = sizes
    nep = nz * nx
    rows = routed_in.shape[0]
    width = routed_in.shape[1]
    hidden = gate_weight.shape[2]
    cap = 2 * expert_ids.shape[1] * rows // nep
    total = nep * cap
    chunk = total // CHUNKS
    half_ring = ny // 2
    mates = 2 * half_ring + 1
    dma = pltpu.SemaphoreType.DMA
    vmem = pltpu.VMEM
    scratch = [
        vmem((width, hidden), BF16),
        vmem((width, hidden), BF16),
        vmem((hidden, width), BF16),
        vmem(out_weight.shape, BF16),
        vmem((rows, width), BF16),
        vmem((1, 1), F32),
        vmem((1, LANES), F32),
        vmem((1, width), F32),
        vmem((2, rows), jnp.int32),
        vmem((group_logits.shape[1], rows), F32),
        vmem((2, rows), F32),
        dma((4,)),
        dma((10,)),
        vmem((8, rows), F32),
        vmem((8, rows), F32),
        vmem((total, LANES), BF16),
        vmem((total, LANES), BF16),
        vmem((ny, 2, total, LANES), BF16),
        vmem((CHUNKS, 2, ny, chunk, LANES), BF16),
        vmem((CHUNKS, ny, chunk, LANES), BF16),
        vmem((CHUNKS, half_ring, chunk, LANES), BF16),
        vmem((CHUNKS, half_ring, chunk, LANES), BF16),
        vmem((CHUNKS, half_ring, chunk, LANES), BF16),
        vmem((CHUNKS, half_ring, chunk, LANES), BF16),
        vmem((total, LANES), BF16),
        vmem((total, LANES), BF16),
        dma((nep,)),
        dma((nep,)),
        dma((nep,)),
        dma((nep,)),
        dma((CHUNKS, half_ring)),
        dma((CHUNKS, half_ring)),
        dma((CHUNKS, half_ring)),
        dma((CHUNKS, half_ring)),
        dma((CHUNKS, mates)),
        dma((CHUNKS, mates)),
        dma((CHUNKS,)),
        dma((CHUNKS,)),
        dma((CHUNKS, half_ring)),
        dma((CHUNKS, half_ring)),
        dma((CHUNKS, half_ring)),
        dma((CHUNKS, half_ring)),
        dma((nep,)),
        dma((nep,)),
        vmem((nx, rows, LANES), BF16),
        vmem((nx, 2 * rows, LANES), BF16),
        vmem((nz, rows, LANES), BF16),
        vmem((nz, rows, LANES), BF16),
        vmem((nx, LANES, 2 * rows), F32),
        vmem((nx, 8, 2 * rows), F32),
        vmem((nx, LANES, 2 * rows), BF16),
        vmem((nx, LANES, 2 * rows), BF16),
        vmem((nx, 8, 2 * rows), F32),
        vmem((ny, 2, rows, LANES), BF16),
        dma((nx,)),
        dma((nx,)),
        dma((nz,)),
        dma((nz,)),
        dma((nz,)),
        dma((nz,)),
        dma((nx,)),
        dma((nx,)),
        dma((nx,)),
        dma((nx,)),
        dma((half_ring,)),
        dma((half_ring,)),
        dma((half_ring,)),
        dma((half_ring,)),
        dma((mates,)),
        dma((mates,)),
    ]
    whole = pl.BlockSpec(memory_space=pltpu.VMEM)
    far = pl.BlockSpec(memory_space=pl.ANY)
    both = pl.pallas_call(
        lambda *refs: kernel(sizes, *refs),
        out_shape=jax.ShapeDtypeStruct((2, rows, LANES), BF16),
        in_specs=[far] * 14,
        out_specs=whole,
        scratch_shapes=scratch,
        compiler_params=pltpu.CompilerParams(
            collective_id=0, has_side_effects=True, vmem_limit_bytes=60 * 1024 * 1024
        ),
    )(
        queries,
        key_rows,
        values,
        second_scale.reshape(1, 1),
        head_gain.reshape(1, -1),
        out_weight,
        routed_in,
        routed_gain.reshape(1, -1),
        expert_ids.T,
        group_logits.T,
        inner_logits.T,
        gate_weight[0],
        up_weight[0],
        down_weight[0],
    )
    return both[0], both[1]


def build(mesh, sizes):
    nz, nx, ny = sizes
    finer = Mesh(mesh.devices.reshape(nz, nx, ny, 2), ("z", "x", "y", "c"))
    ep, tp = ("z", "x"), ("y", "c")
    placed = (
        P(ep, tp),
        P(ep, tp),
        P(ep, tp),
        P(tp),
        P(),
        P(None, tp),
        P(ep, None),
        P(),
        P(ep, None),
        P(ep, None),
        P(ep, None),
        P(ep, None, tp),
        P(ep, None, tp),
        P(ep, tp, None),
    )
    return jax.shard_map(
        lambda *args: local(sizes, *args),
        mesh=finer,
        in_specs=placed,
        out_specs=(P(ep, tp), P(ep, tp)),
        check_vma=False,
    )


def solution(mesh):
    return build(mesh, (8, 4, mesh.shape["tp"] // 2))
```

```python
import jax
import jax.numpy as jnp
from jax import lax
from jax.experimental import pallas as pl
from jax.experimental.pallas import tpu as pltpu
from jax.sharding import Mesh
from jax.sharding import PartitionSpec as P

EPSILON = 1e-05
LOWEST = -1e30
GROUP_SIZE = 4
LANES = 128
CHUNKS = 8
ORDER = (
    ("gather", 0, 0),
    ("inputs",),
    ("gather", 0, 1),
    ("gather", 1, 0),
    ("gather", 0, 2),
    ("gather", 0, 3),
    ("gather", 1, 1),
    ("gather", 0, 4),
    ("gather", 2, 0),
    ("gather", 0, 5),
    ("own",),
    ("gather", 1, 3),
    ("chain", 1),
    ("keys",),
    ("gather", 1, 2),
    ("gather", 0, 7),
    ("gather", 2, 1),
    ("attend", 1),
    ("gather", 1, 4),
    ("gather", 3, 0),
    ("gather", 0, 6),
    ("gather", 1, 5),
    ("gather", 2, 3),
    ("far", 0),
    ("gather", 2, 2),
    ("far", 1),
    ("gather", 1, 7),
    ("expert", 0),
    ("far", 2),
    ("gather", 3, 1),
    ("chain", 2),
    ("attend", 2),
    ("sum", 4, 0),
    ("far", 3),
    ("gather", 2, 4),
    ("far", 4),
    ("expert", 1),
    ("gather", 1, 6),
    ("far", 5),
    ("gather", 3, 3),
    ("gather", 2, 5),
    ("far", 6),
    ("far", 7),
    ("gather", 3, 2),
    ("sum", 4, 1),
    ("expert", 3),
    ("gather", 2, 7),
    ("sum", 3, 0),
    ("expert", 2),
    ("gather", 3, 4),
    ("chain", 3),
    ("sum", 4, 3),
    ("attend", 3),
    ("sum", 4, 2),
    ("sum", 3, 1),
    ("expert", 4),
    ("gather", 3, 7),
    ("gather", 3, 5),
    ("gather", 2, 6),
    ("sum", 2, 0),
    ("sum", 3, 3),
    ("expert", 7),
    ("expert", 5),
    ("sum", 2, 1),
    ("sum", 3, 2),
    ("sum", 4, 4),
    ("sum", 4, 7),
    ("gather", 3, 6),
    ("chain", 4),
    ("attend", 4),
    ("sum", 1, 0),
    ("sum", 2, 3),
    ("attend", 5),
    ("attend", 6),
    ("sum", 3, 4),
    ("attend", 7),
    ("results",),
    ("sum", 3, 7),
    ("sum", 1, 3),
    ("sum", 2, 2),
    ("sum", 0, 0),
    ("expert", 6),
    ("sum", 4, 5),
    ("sum", 2, 4),
    ("sum", 1, 1),
    ("sum", 4, 6),
    ("sum", 2, 7),
    ("sum", 0, 3),
    ("sum", 1, 2),
    ("sum", 3, 5),
    ("sum", 1, 4),
    ("sum", 0, 1),
    ("sum", 3, 6),
    ("merge",),
    ("sum", 1, 7),
    ("sum", 0, 2),
    ("sum", 2, 5),
    ("sum", 0, 4),
    ("sum", 2, 6),
    ("heads", 1),
    ("sum", 0, 7),
    ("sum", 1, 5),
    ("sum", 1, 6),
    ("heads", 2),
    ("sum", 0, 5),
    ("sum", 0, 6),
    ("heads", 3),
    ("heads", 4),
    ("project",),
)
F32 = jnp.float32
BF16 = jnp.bfloat16


def remote(src, dst, send_sem, recv_sem, **where):
    return pltpu.make_async_remote_copy(
        src_ref=src,
        dst_ref=dst,
        send_sem=send_sem,
        recv_sem=recv_sem,
        device_id=where,
        device_id_type=pl.DeviceIdType.MESH,
    )


def loop(first, last, body):
    def step(i, carry):
        body(i)
        return carry

    lax.fori_loop(first, last, step, 0)


def kernel(
    sizes,
    q_hbm,
    k_hbm,
    v_hbm,
    scale_hbm,
    hgain_hbm,
    ow_hbm,
    rin_hbm,
    rgain_hbm,
    ids_hbm,
    gl_hbm,
    il_hbm,
    gw_hbm,
    uw_hbm,
    dw_hbm,
    out_ref,
    gw,
    uw,
    dw,
    ow,
    rin,
    scale_ref,
    hgain_ref,
    rgain_ref,
    ids_ref,
    gl_ref,
    il_ref,
    w_sem,
    i_sem,
    pos,
    weight,
    disp,
    disp_far,
    xs,
    parts,
    mate,
    rb_up,
    rb_dn,
    sb_up,
    sb_dn,
    ans,
    ret,
    a_send,
    a_recv,
    f_send,
    f_recv,
    up_send,
    up_recv,
    dn_send,
    dn_recv,
    m_send,
    m_recv,
    pm_send,
    pm_recv,
    ru_send,
    ru_recv,
    rd_send,
    rd_recv,
    b_send,
    b_recv,
    qb,
    qs,
    kvb,
    acc,
    stat,
    o_out,
    o_in,
    stat_in,
    heads,
    q_send,
    q_recv,
    k_send,
    k_recv,
    o_send,
    o_recv,
    s_send,
    s_recv,
    hu_send,
    hu_recv,
    hd_send,
    hd_recv,
    hm_send,
    hm_recv,
):
    nz, nx, ny = sizes
    nep = nz * nx
    half_ring = ny // 2
    z, x, y, c = (lax.axis_index(name) for name in ("z", "x", "y", "c"))
    other = 1 - c
    e = z * nx + x
    t = y * 2 + c
    rows = rin.shape[0]
    width = rin.shape[1]
    total = xs.shape[2]
    cap = total // nep
    chunk = total // CHUNKS
    half = chunk // 2
    per_chunk = nep // CHUNKS
    y_next = lax.rem(y + 1, ny)
    y_prev = lax.rem(y + ny - 1, ny)

    def y_at(shift):
        return lax.rem(y + shift + ny, ny)

    group = z // (nz // CHUNKS)

    def nearby(j):
        return lax.rem(group + (0, 1, 7, 2, 6, 3, 5, 4)[j], CHUNKS)

    def wait_sent(block, sem):
        remote(block, block, sem, sem, c=other).wait_send()

    def wait_arrived(block, sem):
        remote(block, block, sem, sem, c=other).wait_recv()

    def each_other(first, count, body):
        def one(i):
            @pl.when(first + i != e)
            def _():
                body(first + i)

        loop(0, count, one)


    input_copies = [
        pltpu.make_async_copy(src, dst, i_sem.at[i])
        for i, (src, dst) in enumerate(
            (
                (rin_hbm, rin),
                (ids_hbm, ids_ref),
                (gl_hbm, gl_ref),
                (il_hbm, il_ref),
                (rgain_hbm, rgain_ref),
                (q_hbm, qb.at[x]),
                (k_hbm, kvb.at[z, 0]),
                (v_hbm, kvb.at[z, 1]),
                (scale_hbm, scale_ref),
                (hgain_hbm, hgain_ref),
            )
        )
    ]
    weight_copies = [
        pltpu.make_async_copy(src, dst, w_sem.at[i])
        for i, (src, dst) in enumerate(
            ((gw_hbm, gw), (uw_hbm, uw), (dw_hbm, dw), (ow_hbm, ow))
        )
    ]
    for copy in input_copies:
        copy.start()

    barrier = pltpu.get_barrier_semaphore()

    def greet(**where):
        pl.semaphore_signal(
            barrier, inc=1, device_id=where, device_id_type=pl.DeviceIdType.MESH
        )

    near_z = [lax.rem(z + d, nz) for d in range(nz)]
    near_x = [lax.rem(x + d, nx) for d in range(nx)]
    apart = [(i, j) for i in range(nz) for j in range(nx) if i + j > 0]
    for i, j in sorted(apart, key=lambda ij: -min(ij[0], nz - ij[0]) - min(ij[1], nx - ij[1])):
        greet(z=near_z[i], x=near_x[j])
    greet(y=y_next)
    greet(y=y_prev)
    greet(c=other)

    for copy in input_copies[1:5]:
        copy.wait()
    ids = ids_ref[...]
    shape = (nep, rows)
    expert_row = lax.broadcasted_iota(jnp.int32, shape, 0)
    picks = [jnp.where(ids[i : i + 1, :] == expert_row, 1.0, 0.0) for i in range(2)]
    earlier = jnp.where(
        lax.broadcasted_iota(jnp.int32, (rows, rows), 0)
        < lax.broadcasted_iota(jnp.int32, (rows, rows), 1),
        1.0,
        0.0,
    ).astype(BF16)
    before = [jnp.dot(pick.astype(BF16), earlier, preferred_element_type=F32) for pick in picks]
    before[1] += jnp.sum(picks[0], axis=1, keepdims=True)
    logits = gl_ref[...]
    group_exp = jnp.exp(logits - jnp.max(logits, axis=0, keepdims=True))
    group_prob = group_exp / jnp.sum(group_exp, axis=0, keepdims=True)
    group_row = lax.broadcasted_iota(jnp.int32, logits.shape, 0)
    inner = il_ref[...]
    inner_exp = jnp.exp(inner - jnp.max(inner, axis=0, keepdims=True))
    inner_prob = inner_exp / jnp.sum(inner_exp, axis=0, keepdims=True)
    for i in range(2):
        pos[i : i + 1, :] = ids[i : i + 1, :].astype(F32) * cap + jnp.sum(
            picks[i] * before[i], axis=0, keepdims=True
        )
        chosen = ids[i : i + 1, :] // GROUP_SIZE == group_row
        picked = jnp.sum(jnp.where(chosen, group_prob, 0.0), axis=0, keepdims=True)
        weight[i : i + 1, :] = picked * inner_prob[i : i + 1, :]

    def one_hot(i):
        slots = lax.broadcasted_iota(jnp.int32, (total, rows), 0).astype(F32)
        return jnp.where(pos[i : i + 1, :] == slots, 1.0, 0.0).astype(BF16)

    input_copies[0].wait()
    source = rin[...].astype(F32)
    inv = lax.rsqrt(jnp.sum(source * source, axis=-1, keepdims=True) * (1.0 / width) + EPSILON)

    def normed(block):
        columns = pl.ds(pl.multiple_of((block * 2 + c) * LANES, LANES), LANES)
        return (rin[:, columns].astype(F32) * inv * rgain_ref[:, columns]).astype(BF16)

    y_far = y_at(half_ring)
    spread = jnp.dot(
        one_hot(0) + one_hot(1),
        jnp.concatenate([normed(y), normed(y_far)], axis=1),
        preferred_element_type=F32,
    ).astype(BF16)
    disp[...] = spread[:, :LANES]
    disp_far[...] = spread[:, LANES:]
    for copy in input_copies[5:]:
        copy.wait()
    for copy in weight_copies:
        copy.start()

    pl.semaphore_wait(barrier, nep - 1 + 2 + 1)

    def slot_rows(index):
        return pl.ds(pl.multiple_of(index * cap, cap), cap)

    def dispatch(peer):
        return remote(
            disp.at[slot_rows(peer)],
            xs.at[y, c, slot_rows(e)],
            a_send.at[0],
            a_recv.at[group],
            z=peer // nx,
            x=lax.rem(peer, nx),
        )

    def dispatch_far(peer):
        return remote(
            disp_far.at[slot_rows(peer)],
            xs.at[y_far, c, slot_rows(e)],
            f_send.at[0],
            f_recv.at[group],
            z=peer // nx,
            x=lax.rem(peer, nx),
        )

    for j in range(CHUNKS):
        each_other(nearby(j) * per_chunk, per_chunk, lambda peer: dispatch(peer).start())
    xs[y, c, slot_rows(e), :] = disp[slot_rows(e), :]
    xs[y_far, c, slot_rows(e), :] = disp_far[slot_rows(e), :]

    def query_copy(r):
        return remote(
            qb.at[x], qb.at[x], q_send.at[0], q_recv.at[0], x=lax.rem(x + r, nx)
        )

    reach = nz // 2

    def key_copy(block, r, to_z):
        return remote(kvb.at[block], kvb.at[block], k_send.at[r], k_recv.at[r], z=to_z)

    def chain_copy(r):
        return key_copy(jnp.maximum(z - r + 1, 0), r, jnp.minimum(z + 1, nz - 1))

    def far_copy(r):
        return key_copy(z, r, lax.rem(z + r, nz))

    def chain_send(r):
        @pl.when((z + 1 < nz) & (z - r + 1 >= 0))
        def _():
            chain_copy(r).start()

    def send_inputs():
        for r in range(1, nx):
            query_copy(r).start()
        chain_send(1)
        for j in range(CHUNKS):
            each_other(nearby(j) * per_chunk, per_chunk, lambda peer: dispatch_far(peer).start())

    def send_far_keys():
        for r in range(reach + 1, nz):

            @pl.when(z + r < nz)
            def _(r=r):
                far_copy(r).start()

    maps = 2 * rows
    qk = LANES // 2
    keep_low = lax.broadcasted_iota(jnp.int32, (rows, LANES), 1) < qk

    def stack_query(value, index):
        scaled = value.astype(F32) * (qk ** (-0.5))
        qs[index, 0:rows, :] = jnp.where(keep_low, scaled, 0.0).astype(BF16)
        qs[index, rows:maps, :] = jnp.where(keep_low, 0.0, scaled).astype(BF16)

    pieces = [(i, j * LANES) for i in range(nx) for j in range(maps // LANES)]

    def attend(key_block, value_block, masked):
        keys = key_block[...]
        values = value_block[...].T

        def score(index, first):
            return lax.dot_general(
                keys,
                qs[index, first : first + LANES, :],
                (((1,), (1,)), ((), ())),
                preferred_element_type=F32,
            )

        ahead = score(*pieces[0])
        for number, (index, first) in enumerate(pieces):
            scores = ahead
            if number + 1 < len(pieces):
                ahead = score(*pieces[number + 1])
            columns = slice(first, first + LANES)
            if masked:
                key_pos = x * rows + lax.broadcasted_iota(jnp.int32, scores.shape, 0)
                query_pos = lax.broadcasted_iota(jnp.int32, scores.shape, 1) + (
                    index * rows + first % rows
                )
                visible = query_pos >= key_pos
                scores = jnp.where(visible, scores, LOWEST)
                new_max = jnp.max(scores, axis=0, keepdims=True)
                terms = jnp.where(visible, jnp.exp(scores - new_max), 0.0)
            else:
                old_max = stat[index, 0:1, columns]
                new_max = jnp.maximum(old_max, jnp.max(scores, axis=0, keepdims=True))
                terms = jnp.exp(scores - new_max)
                factor = jnp.exp(old_max - new_max)
            total_terms = jnp.sum(terms, axis=0, keepdims=True)
            weighted = jnp.dot(values, terms.astype(BF16), preferred_element_type=F32)
            if masked:
                stat[index, 1:2, columns] = total_terms
                acc[index, :, columns] = weighted
            else:
                stat[index, 1:2, columns] = stat[index, 1:2, columns] * factor + total_terms
                acc[index, :, columns] = acc[index, :, columns] * factor + weighted
            stat[index, 0:1, columns] = new_max

    def own_attention():
        wait_arrived(qb.at[pl.ds(0, nx - 1)], q_recv.at[0])
        for index in range(nx):
            stack_query(qb[index], index)
        stat[...] = jnp.zeros_like(stat)
        attend(kvb.at[z, 0], kvb.at[z, 1], True)

    def chain_step(r):
        @pl.when(z >= r)
        def _():
            key_copy(jnp.maximum(z - r, 0), r, z).wait_recv()
            if r < reach:
                chain_send(r + 1)

    def attend_far(r):
        @pl.when(z >= r)
        def _():
            from_z = jnp.maximum(z - r, 0)
            if r > reach:
                key_copy(from_z, r, z).wait_recv()
            attend(kvb.at[from_z, 0], kvb.at[from_z, 1], False)

    def wait_rows(block, j, recv_sems):
        k = nearby(j)
        count = per_chunk - 1 if j == 0 else per_chunk
        span = pl.ds(pl.multiple_of(k * chunk, chunk), count * cap)
        wait_arrived(xs.at[block, c, span], recv_sems.at[k])

    def chunk_rows(k):
        return pl.ds(pl.multiple_of(k * chunk, chunk), chunk)

    def up_copy(s, k):
        where = chunk_rows(k)
        block = xs.at[y_at(-s), c, where]
        return remote(block, block, up_send.at[0], up_recv.at[k, s], y=y_next)

    def dn_copy(s, k):
        where = chunk_rows(k)
        block = xs.at[y_at(s), c, where]
        return remote(block, block, dn_send.at[0], dn_recv.at[k, s], y=y_prev)

    def up_arrival(s, k):
        where = chunk_rows(k)
        block = xs.at[y_at(-s - 1), c, where]
        return remote(block, block, up_send.at[0], up_recv.at[k, s], y=y_next)

    def dn_arrival(s, k):
        where = chunk_rows(k)
        block = xs.at[y_at(s + 1), c, where]
        return remote(block, block, dn_send.at[0], dn_recv.at[k, s], y=y_prev)

    def mate_block(number, k, core):
        shift = (0, -1, 1, -2, 2, -3, 3, half_ring)[number]
        return xs.at[y_at(shift), core, chunk_rows(k)]

    def mate_copy(number, k):
        block = mate_block(number, k, c)
        return remote(block, block, m_send.at[0], m_recv.at[k], c=other)

    def first_sends(j):
        wait_rows(y, j, a_recv)
        k = nearby(j)
        up_copy(0, k).start()
        dn_copy(0, k).start()
        mate_copy(0, k).start()

    def pass_on(s, k):
        up_arrival(s, k).wait_recv()
        if s + 2 < half_ring:
            up_copy(s + 1, k).start()
        mate_copy(2 * s + 1, k).start()
        dn_arrival(s, k).wait_recv()
        if s + 2 < half_ring:
            dn_copy(s + 1, k).start()
        mate_copy(2 * s + 2, k).start()

    def far_rows(j):
        wait_rows(y_far, j, f_recv)
        mate_copy(ny - 1, nearby(j)).start()

    def result_copies(r):
        to_x = lax.rem(x + r, nx)
        return (
            remote(o_out.at[to_x], o_in.at[x], o_send.at[0], o_recv.at[0], x=to_x),
            remote(stat.at[to_x], stat_in.at[x], s_send.at[0], s_recv.at[0], x=to_x),
        )

    def send_results():
        o_out[...] = acc[...].astype(BF16)
        for r in range(1, nx):
            for copy in result_copies(r):
                copy.start()
        o_in[x] = o_out[x]
        stat_in[x] = stat[x]

    def expert(k):
        wait_arrived(xs.at[:, other, chunk_rows(k)], m_recv.at[k])
        gate = jnp.zeros((chunk, gw.shape[1]), F32)
        up = jnp.zeros((chunk, gw.shape[1]), F32)
        for block in range(ny):
            both = jnp.concatenate(
                [xs[block, 0, chunk_rows(k), :], xs[block, 1, chunk_rows(k), :]], axis=1
            )
            depth = slice(block * 2 * LANES, (block + 1) * 2 * LANES)
            gate += jnp.dot(both, gw[depth, :], preferred_element_type=F32)
            up += jnp.dot(both, uw[depth, :], preferred_element_type=F32)
        hidden = (gate / (1.0 + jnp.exp(-gate)) * up).astype(BF16)
        for block in range(ny):
            columns = slice(block * 2 * LANES, (block + 1) * 2 * LANES)
            value = jnp.dot(hidden, dw[:, columns], preferred_element_type=F32).astype(BF16)
            parts[k, 0, block] = value[:, :LANES]
            parts[k, 1, block] = value[:, LANES:]
        part_copy(k).start()

    def part_copy(k):
        return remote(parts.at[k, other], mate.at[k], pm_send.at[0], pm_recv.at[k], c=other)

    full = slice(0, chunk)
    top = slice(0, half)
    bottom = slice(half, chunk)

    def chip_sum(k, target, where):
        return parts[k, c, target, where, :].astype(F32) + mate[k, target, where, :].astype(F32)

    def sum_up(k, d):
        where = top if d == half_ring else full
        return remote(
            sb_up.at[k, d - 1, where], rb_up.at[k, d - 1, where],
            ru_send.at[d // half_ring], ru_recv.at[k, d - 1], y=y_next,
        )

    def sum_dn(k, d):
        where = bottom if d == half_ring else full
        return remote(
            sb_dn.at[k, d - 1, where], rb_dn.at[k, d - 1, where],
            rd_send.at[d // half_ring], rd_recv.at[k, d - 1], y=y_prev,
        )

    def sum_step(k, d):
        if d == half_ring:
            sb_up[k, d - 1, top] = chip_sum(k, y_at(d), top).astype(BF16)
            sum_up(k, d).start()
            sb_dn[k, d - 1, bottom] = chip_sum(k, y_at(-d), bottom).astype(BF16)
            sum_dn(k, d).start()
            return
        sum_up(k, d + 1).wait_recv()
        if d + 1 == half_ring:
            sb_up[k, d - 1, top] = (
                chip_sum(k, y_at(d), top) + rb_up[k, d, top].astype(F32)
            ).astype(BF16)
            sb_up[k, d - 1, bottom] = chip_sum(k, y_at(d), bottom).astype(BF16)
        else:
            sb_up[k, d - 1] = (
                chip_sum(k, y_at(d), full) + rb_up[k, d].astype(F32)
            ).astype(BF16)
        sum_up(k, d).start()
        sum_dn(k, d + 1).wait_recv()
        if d + 1 == half_ring:
            sb_dn[k, d - 1, bottom] = (
                chip_sum(k, y_at(-d), bottom) + rb_dn[k, d, bottom].astype(F32)
            ).astype(BF16)
            sb_dn[k, d - 1, top] = chip_sum(k, y_at(-d), top).astype(BF16)
        else:
            sb_dn[k, d - 1] = (
                chip_sum(k, y_at(-d), full) + rb_dn[k, d].astype(F32)
            ).astype(BF16)
        sum_dn(k, d).start()

    def answer(k):
        sum_up(k, 1).wait_recv()
        sum_dn(k, 1).wait_recv()
        ans[chunk_rows(k), :] = (
            chip_sum(k, y, full) + rb_up[k, 0].astype(F32) + rb_dn[k, 0].astype(F32)
        ).astype(BF16)
        each_other(k * per_chunk, per_chunk, lambda target: back_copy(target).start())

    def back_copy(target):
        return remote(
            ans.at[slot_rows(target)],
            ret.at[slot_rows(e)],
            b_send.at[0],
            b_recv.at[0],
            z=target // nx,
            x=lax.rem(target, nx),
        )

    def first_sum(k):
        part_copy(k).wait_recv()
        sum_step(k, half_ring)

    top_rows = pl.ds(0, rows // 2)
    low_rows = pl.ds(rows // 2, rows // 2)
    all_rows = pl.ds(0, rows)

    def head_up(s, hop):
        where = top_rows if s == half_ring - 1 else all_rows
        block = heads.at[y_at(-s - hop), c, where]
        return remote(block, block, hu_send.at[(s + 1) // half_ring], hu_recv.at[s], y=y_next)

    def head_dn(s, hop):
        where = low_rows if s == half_ring - 1 else all_rows
        block = heads.at[y_at(s + hop), c, where]
        return remote(block, block, hd_send.at[(s + 1) // half_ring], hd_recv.at[s], y=y_prev)

    def head_mate(number, core):
        s = (number - 1) // 2
        last = number > 0 and s == half_ring - 1
        if number == 0:
            block = heads.at[y, core]
        elif number % 2 == 1:
            block = heads.at[y_at(-s - 1), core, top_rows if last else all_rows]
        else:
            block = heads.at[y_at(s + 1), core, low_rows if last else all_rows]
        return remote(block, block, hm_send.at[0], hm_recv.at[0], c=other)

    def head_pass(s):
        head_up(s, 1).wait_recv()
        if s + 1 < half_ring:
            head_up(s + 1, 0).start()
        head_mate(2 * s + 1, c).start()
        head_dn(s, 1).wait_recv()
        if s + 1 < half_ring:
            head_dn(s + 1, 0).start()
        head_mate(2 * s + 2, c).start()

    def merge():
        wait_arrived(o_in.at[pl.ds(0, nx - 1)], o_recv.at[0])
        wait_arrived(stat_in.at[pl.ds(0, nx - 1)], s_recv.at[0])
        top_max = stat_in[0, 0:1, :]
        for j in range(1, nx):
            top_max = jnp.maximum(top_max, stat_in[j, 0:1, :])
        denominator = jnp.zeros_like(top_max)
        weighted = jnp.zeros(o_in.shape[1:], F32)
        for j in range(nx):
            factor = jnp.exp(stat_in[j, 0:1, :] - top_max)
            denominator += factor * stat_in[j, 1:2, :]
            weighted += factor * o_in[j].astype(F32)
        mapped = weighted / denominator
        difference = mapped[:, :rows] - scale_ref[0:1, 0:1] * mapped[:, rows:]
        mean = jnp.sum(difference * difference, axis=0, keepdims=True) * (1.0 / LANES)
        head = difference * lax.rsqrt(mean + EPSILON)
        heads[y, c] = (head.T * hgain_ref[...]).astype(BF16)
        head_up(0, 0).start()
        head_dn(0, 0).start()
        head_mate(0, c).start()

    def weights_and_expert(k):
        if not weights_here:
            weights_here.append(True)
            for copy in weight_copies[:3]:
                copy.wait()
        expert(k)

    def sum_stage(d, k):
        if d == half_ring:
            first_sum(k)
        elif d > 0:
            sum_step(k, d)
        else:
            answer(k)

    def gather_stage(s, j):
        if s == 0:
            first_sends(j)
        else:
            pass_on(s - 1, nearby(j))

    weights_here = []
    stages = {
        "gather": gather_stage,
        "inputs": send_inputs,
        "keys": send_far_keys,
        "far": far_rows,
        "chain": chain_step,
        "own": own_attention,
        "attend": attend_far,
        "expert": lambda j: weights_and_expert(nearby(j)),
        "sum": lambda d, j: sum_stage(d, nearby(j)),
        "results": send_results,
        "merge": merge,
        "heads": lambda s: head_pass(s - 1),
        "project": lambda: None,
    }
    for stage in ORDER:
        stages[stage[0]](*stage[1:])
    ret[slot_rows(e), :] = ans[slot_rows(e), :]

    weight_copies[3].wait()
    wait_arrived(heads.at[:, other], hm_recv.at[0])
    mixed = jnp.zeros((rows, LANES), F32)
    for block in range(ny):
        both = jnp.concatenate([heads[block, 0], heads[block, 1]], axis=1)
        mixed += jnp.dot(
            both, ow[block * 2 * LANES : (block + 1) * 2 * LANES, :], preferred_element_type=F32
        )
    out_ref[0] = mixed.astype(BF16)

    others = pl.ds(0, (nep - 1) * cap)
    wait_sent(disp.at[others], a_send.at[0])
    wait_sent(disp_far.at[others], f_send.at[0])
    wait_sent(xs.at[pl.ds(0, half_ring - 1), c], up_send.at[0])
    wait_sent(xs.at[pl.ds(0, half_ring - 1), c], dn_send.at[0])
    wait_sent(xs.at[:, c], m_send.at[0])
    wait_sent(mate, pm_send.at[0])
    wait_sent(sb_up.at[:, pl.ds(0, half_ring - 1)], ru_send.at[0])
    wait_sent(sb_up.at[:, half_ring - 1, top], ru_send.at[1])
    wait_sent(sb_dn.at[:, pl.ds(0, half_ring - 1)], rd_send.at[0])
    wait_sent(sb_dn.at[:, half_ring - 1, bottom], rd_send.at[1])
    wait_sent(qb.at[pl.ds(0, nx - 1)], q_send.at[0])
    wait_sent(o_out.at[pl.ds(0, nx - 1)], o_send.at[0])
    wait_sent(stat.at[pl.ds(0, nx - 1)], s_send.at[0])
    for r in range(1, reach + 1):

        @pl.when((z + 1 < nz) & (z - r + 1 >= 0))
        def _(r=r):
            chain_copy(r).wait_send()

    for r in range(reach + 1, nz):

        @pl.when(z + r < nz)
        def _(r=r):
            far_copy(r).wait_send()

    wait_sent(heads.at[pl.ds(0, half_ring - 1), c], hu_send.at[0])
    wait_sent(heads.at[0, c, top_rows], hu_send.at[1])
    wait_sent(heads.at[pl.ds(0, half_ring - 1), c], hd_send.at[0])
    wait_sent(heads.at[0, c, low_rows], hd_send.at[1])
    wait_sent(heads.at[:, c], hm_send.at[0])

    wait_arrived(ret.at[pl.ds(0, (nep - 1) * cap)], b_recv.at[0])
    routed = jnp.zeros((LANES, rows), F32)
    for i in range(2):
        routed += weight[i : i + 1, :] * lax.dot_general(
            ret[...], one_hot(i), (((0,), (0,)), ((), ())), preferred_element_type=F32
        )
    out_ref[1] = routed.T.astype(BF16)

    wait_sent(ans.at[pl.ds(0, (nep - 1) * cap)], b_send.at[0])


def local(
    sizes,
    queries,
    key_rows,
    values,
    second_scale,
    head_gain,
    out_weight,
    routed_in,
    routed_gain,
    expert_ids,
    group_logits,
    inner_logits,
    gate_weight,
    up_weight,
    down_weight,
):
    nz, nx, ny = sizes
    nep = nz * nx
    rows = routed_in.shape[0]
    width = routed_in.shape[1]
    hidden = gate_weight.shape[2]
    cap = 2 * expert_ids.shape[1] * rows // nep
    total = nep * cap
    chunk = total // CHUNKS
    half_ring = ny // 2
    dma = pltpu.SemaphoreType.DMA
    vmem = pltpu.VMEM
    scratch = [
        vmem((width, hidden), BF16),
        vmem((width, hidden), BF16),
        vmem((hidden, width), BF16),
        vmem(out_weight.shape, BF16),
        vmem((rows, width), BF16),
        vmem((1, 1), F32),
        vmem((1, LANES), F32),
        vmem((1, width), F32),
        vmem((2, rows), jnp.int32),
        vmem((group_logits.shape[1], rows), F32),
        vmem((2, rows), F32),
        dma((4,)),
        dma((10,)),
        vmem((8, rows), F32),
        vmem((8, rows), F32),
        vmem((total, LANES), BF16),
        vmem((total, LANES), BF16),
        vmem((ny, 2, total, LANES), BF16),
        vmem((CHUNKS, 2, ny, chunk, LANES), BF16),
        vmem((CHUNKS, ny, chunk, LANES), BF16),
        vmem((CHUNKS, half_ring, chunk, LANES), BF16),
        vmem((CHUNKS, half_ring, chunk, LANES), BF16),
        vmem((CHUNKS, half_ring, chunk, LANES), BF16),
        vmem((CHUNKS, half_ring, chunk, LANES), BF16),
        vmem((total, LANES), BF16),
        vmem((total, LANES), BF16),
        dma((1,)),
        dma((CHUNKS,)),
        dma((1,)),
        dma((CHUNKS,)),
        dma((1,)),
        dma((CHUNKS, half_ring - 1)),
        dma((1,)),
        dma((CHUNKS, half_ring - 1)),
        dma((1,)),
        dma((CHUNKS,)),
        dma((1,)),
        dma((CHUNKS,)),
        dma((2,)),
        dma((CHUNKS, half_ring)),
        dma((2,)),
        dma((CHUNKS, half_ring)),
        dma((1,)),
        dma((1,)),
        vmem((nx, rows, LANES), BF16),
        vmem((nx, 2 * rows, LANES), BF16),
        vmem((nz, 2, rows, LANES), BF16),
        vmem((nx, LANES, 2 * rows), F32),
        vmem((nx, 8, 2 * rows), F32),
        vmem((nx, LANES, 2 * rows), BF16),
        vmem((nx, LANES, 2 * rows), BF16),
        vmem((nx, 8, 2 * rows), F32),
        vmem((ny, 2, rows, LANES), BF16),
        dma((1,)),
        dma((1,)),
        dma((nz,)),
        dma((nz,)),
        dma((1,)),
        dma((1,)),
        dma((1,)),
        dma((1,)),
        dma((2,)),
        dma((half_ring,)),
        dma((2,)),
        dma((half_ring,)),
        dma((1,)),
        dma((1,)),
    ]
    whole = pl.BlockSpec(memory_space=pltpu.VMEM)
    far = pl.BlockSpec(memory_space=pl.ANY)
    both = pl.pallas_call(
        lambda *refs: kernel(sizes, *refs),
        out_shape=jax.ShapeDtypeStruct((2, rows, LANES), BF16),
        in_specs=[far] * 14,
        out_specs=whole,
        scratch_shapes=scratch,
        compiler_params=pltpu.CompilerParams(
            collective_id=0, has_side_effects=True, vmem_limit_bytes=60 * 1024 * 1024
        ),
    )(
        queries,
        key_rows,
        values,
        second_scale.reshape(1, 1),
        head_gain.reshape(1, -1),
        out_weight,
        routed_in,
        routed_gain.reshape(1, -1),
        expert_ids.T,
        group_logits.T,
        inner_logits.T,
        gate_weight[0],
        up_weight[0],
        down_weight[0],
    )
    return both[0], both[1]


def build(mesh, sizes):
    nz, nx, ny = sizes
    finer = Mesh(mesh.devices.reshape(nz, nx, ny, 2), ("z", "x", "y", "c"))
    ep, tp = ("z", "x"), ("y", "c")
    placed = (
        P(ep, tp),
        P(ep, tp),
        P(ep, tp),
        P(tp),
        P(),
        P(None, tp),
        P(ep, None),
        P(),
        P(ep, None),
        P(ep, None),
        P(ep, None),
        P(ep, None, tp),
        P(ep, None, tp),
        P(ep, tp, None),
    )
    return jax.shard_map(
        lambda *args: local(sizes, *args),
        mesh=finer,
        in_specs=placed,
        out_specs=(P(ep, tp), P(ep, tp)),
        check_vma=False,
    )


def solution(mesh):
    return build(mesh, (8, 4, mesh.shape["tp"] // 2))
```

```python
import jax
import jax.numpy as jnp
from jax import lax
from jax.experimental import pallas as pl
from jax.experimental.pallas import tpu as pltpu
from jax.sharding import Mesh
from jax.sharding import PartitionSpec as P

EPSILON = 1e-05
LOWEST = -1e30
GROUP_SIZE = 4
LANES = 128
CHUNKS = 8
ORDER = (
    ("gather", 0, 0),
    ("inputs",),
    ("gather", 0, 1),
    ("gather", 1, 0),
    ("gather", 0, 2),
    ("gather", 0, 3),
    ("gather", 1, 1),
    ("gather", 0, 4),
    ("gather", 2, 0),
    ("gather", 0, 5),
    ("own",),
    ("gather", 1, 3),
    ("chain", 1),
    ("keys",),
    ("gather", 1, 2),
    ("gather", 0, 7),
    ("gather", 2, 1),
    ("attend", 1),
    ("gather", 1, 4),
    ("gather", 3, 0),
    ("gather", 0, 6),
    ("gather", 1, 5),
    ("gather", 2, 3),
    ("far", 0),
    ("gather", 2, 2),
    ("far", 1),
    ("gather", 1, 7),
    ("expert", 0),
    ("far", 2),
    ("gather", 3, 1),
    ("chain", 2),
    ("attend", 2),
    ("sum", 4, 0),
    ("far", 3),
    ("gather", 2, 4),
    ("far", 4),
    ("expert", 1),
    ("gather", 1, 6),
    ("far", 5),
    ("gather", 3, 3),
    ("gather", 2, 5),
    ("far", 6),
    ("far", 7),
    ("gather", 3, 2),
    ("sum", 4, 1),
    ("expert", 3),
    ("gather", 2, 7),
    ("sum", 3, 0),
    ("expert", 2),
    ("gather", 3, 4),
    ("chain", 3),
    ("sum", 4, 3),
    ("attend", 3),
    ("sum", 4, 2),
    ("sum", 3, 1),
    ("expert", 4),
    ("gather", 3, 7),
    ("gather", 3, 5),
    ("gather", 2, 6),
    ("sum", 2, 0),
    ("sum", 3, 3),
    ("expert", 7),
    ("expert", 5),
    ("sum", 2, 1),
    ("sum", 3, 2),
    ("sum", 4, 4),
    ("sum", 4, 7),
    ("gather", 3, 6),
    ("chain", 4),
    ("attend", 4),
    ("sum", 1, 0),
    ("sum", 2, 3),
    ("attend", 5),
    ("attend", 6),
    ("sum", 3, 4),
    ("attend", 7),
    ("results",),
    ("sum", 3, 7),
    ("sum", 1, 3),
    ("sum", 2, 2),
    ("sum", 0, 0),
    ("expert", 6),
    ("sum", 4, 5),
    ("sum", 2, 4),
    ("sum", 1, 1),
    ("sum", 4, 6),
    ("sum", 2, 7),
    ("sum", 0, 3),
    ("sum", 1, 2),
    ("sum", 3, 5),
    ("sum", 1, 4),
    ("sum", 0, 1),
    ("sum", 3, 6),
    ("merge",),
    ("sum", 1, 7),
    ("sum", 0, 2),
    ("sum", 2, 5),
    ("sum", 0, 4),
    ("sum", 2, 6),
    ("heads", 1),
    ("sum", 0, 7),
    ("sum", 1, 5),
    ("sum", 1, 6),
    ("heads", 2),
    ("sum", 0, 5),
    ("sum", 0, 6),
    ("heads", 3),
    ("drain",),
    ("project",),
    ("heads", 4),
)
F32 = jnp.float32
BF16 = jnp.bfloat16


def remote(src, dst, send_sem, recv_sem, **where):
    return pltpu.make_async_remote_copy(
        src_ref=src,
        dst_ref=dst,
        send_sem=send_sem,
        recv_sem=recv_sem,
        device_id=where,
        device_id_type=pl.DeviceIdType.MESH,
    )


def loop(first, last, body):
    def step(i, carry):
        body(i)
        return carry

    lax.fori_loop(first, last, step, 0)


def kernel(
    sizes,
    q_hbm,
    k_hbm,
    v_hbm,
    scale_hbm,
    hgain_hbm,
    ow_hbm,
    rin_hbm,
    rgain_hbm,
    ids_hbm,
    gl_hbm,
    il_hbm,
    gw_hbm,
    uw_hbm,
    dw_hbm,
    out_ref,
    gw,
    uw,
    dw,
    ow,
    rin,
    scale_ref,
    hgain_ref,
    rgain_ref,
    ids_ref,
    gl_ref,
    il_ref,
    w_sem,
    i_sem,
    pos,
    weight,
    disp,
    disp_far,
    xs,
    parts,
    mate,
    rb_up,
    rb_dn,
    sb_up,
    sb_dn,
    ans,
    ret,
    a_send,
    a_recv,
    f_send,
    f_recv,
    g_send,
    g_recv,
    m_send,
    m_recv,
    pm_send,
    pm_recv,
    r_send,
    r_recv,
    b_send,
    b_recv,
    qb,
    qs,
    kvb,
    acc,
    stat,
    o_out,
    o_in,
    stat_in,
    heads,
    mixed,
    q_send,
    q_recv,
    k_send,
    k_recv,
    o_send,
    o_recv,
    s_send,
    s_recv,
    h_send,
    h_recv,
    hm_send,
    hm_recv,
):
    nz, nx, ny = sizes
    nep = nz * nx
    half_ring = ny // 2
    z, x, y, c = (lax.axis_index(name) for name in ("z", "x", "y", "c"))
    other = 1 - c
    e = z * nx + x
    t = y * 2 + c
    rows = rin.shape[0]
    width = rin.shape[1]
    total = xs.shape[2]
    cap = total // nep
    chunk = total // CHUNKS
    half = chunk // 2
    per_chunk = nep // CHUNKS
    y_next = lax.rem(y + 1, ny)
    y_prev = lax.rem(y + ny - 1, ny)

    def y_at(shift):
        return lax.rem(y + shift + ny, ny)

    group = z // (nz // CHUNKS)

    def nearby(j):
        return lax.rem(group + (0, 1, 7, 2, 6, 3, 5, 4)[j], CHUNKS)

    def wait_sent(block, sem):
        remote(block, block, sem, sem, c=other).wait_send()

    def wait_arrived(block, sem):
        remote(block, block, sem, sem, c=other).wait_recv()

    def each_other(first, count, body):
        def one(i):
            @pl.when(first + i != e)
            def _():
                body(first + i)

        loop(0, count, one)


    input_copies = [
        pltpu.make_async_copy(src, dst, i_sem.at[i])
        for i, (src, dst) in enumerate(
            (
                (rin_hbm, rin),
                (ids_hbm, ids_ref),
                (gl_hbm, gl_ref),
                (il_hbm, il_ref),
                (rgain_hbm, rgain_ref),
                (q_hbm, qb.at[x]),
                (k_hbm, kvb.at[z, 0]),
                (v_hbm, kvb.at[z, 1]),
                (scale_hbm, scale_ref),
                (hgain_hbm, hgain_ref),
            )
        )
    ]
    weight_copies = [
        pltpu.make_async_copy(src, dst, w_sem.at[i])
        for i, (src, dst) in enumerate(
            ((gw_hbm, gw), (uw_hbm, uw), (dw_hbm, dw), (ow_hbm, ow))
        )
    ]
    for copy in input_copies:
        copy.start()

    barrier = pltpu.get_barrier_semaphore()

    def greet(**where):
        pl.semaphore_signal(
            barrier, inc=1, device_id=where, device_id_type=pl.DeviceIdType.MESH
        )

    near_z = [lax.rem(z + d, nz) for d in range(nz)]
    near_x = [lax.rem(x + d, nx) for d in range(nx)]
    apart = [(i, j) for i in range(nz) for j in range(nx) if i + j > 0]
    for i, j in sorted(apart, key=lambda ij: -min(ij[0], nz - ij[0]) - min(ij[1], nx - ij[1])):
        greet(z=near_z[i], x=near_x[j])
    greet(y=y_next)
    greet(y=y_prev)
    greet(c=other)

    for copy in input_copies[1:5]:
        copy.wait()
    ids = ids_ref[...]
    shape = (nep, rows)
    expert_row = lax.broadcasted_iota(jnp.int32, shape, 0)
    picks = [jnp.where(ids[i : i + 1, :] == expert_row, 1.0, 0.0) for i in range(2)]
    earlier = jnp.where(
        lax.broadcasted_iota(jnp.int32, (rows, rows), 0)
        < lax.broadcasted_iota(jnp.int32, (rows, rows), 1),
        1.0,
        0.0,
    ).astype(BF16)
    before = [jnp.dot(pick.astype(BF16), earlier, preferred_element_type=F32) for pick in picks]
    before[1] += jnp.sum(picks[0], axis=1, keepdims=True)
    logits = gl_ref[...]
    group_exp = jnp.exp(logits - jnp.max(logits, axis=0, keepdims=True))
    group_prob = group_exp / jnp.sum(group_exp, axis=0, keepdims=True)
    group_row = lax.broadcasted_iota(jnp.int32, logits.shape, 0)
    inner = il_ref[...]
    inner_exp = jnp.exp(inner - jnp.max(inner, axis=0, keepdims=True))
    inner_prob = inner_exp / jnp.sum(inner_exp, axis=0, keepdims=True)
    for i in range(2):
        pos[i : i + 1, :] = ids[i : i + 1, :].astype(F32) * cap + jnp.sum(
            picks[i] * before[i], axis=0, keepdims=True
        )
        chosen = ids[i : i + 1, :] // GROUP_SIZE == group_row
        picked = jnp.sum(jnp.where(chosen, group_prob, 0.0), axis=0, keepdims=True)
        weight[i : i + 1, :] = picked * inner_prob[i : i + 1, :]

    def one_hot(i):
        slots = lax.broadcasted_iota(jnp.int32, (total, rows), 0).astype(F32)
        return jnp.where(pos[i : i + 1, :] == slots, 1.0, 0.0).astype(BF16)

    input_copies[0].wait()
    source = rin[...].astype(F32)
    inv = lax.rsqrt(jnp.sum(source * source, axis=-1, keepdims=True) * (1.0 / width) + EPSILON)

    def normed(block):
        columns = pl.ds(pl.multiple_of((block * 2 + c) * LANES, LANES), LANES)
        return (rin[:, columns].astype(F32) * inv * rgain_ref[:, columns]).astype(BF16)

    y_far = y_at(half_ring)
    spread = jnp.dot(
        one_hot(0) + one_hot(1),
        jnp.concatenate([normed(y), normed(y_far)], axis=1),
        preferred_element_type=F32,
    ).astype(BF16)
    disp[...] = spread[:, :LANES]
    disp_far[...] = spread[:, LANES:]
    for copy in input_copies[5:]:
        copy.wait()
    for copy in weight_copies:
        copy.start()

    pl.semaphore_wait(barrier, nep - 1 + 2 + 1)

    def slot_rows(index):
        return pl.ds(pl.multiple_of(index * cap, cap), cap)

    def dispatch(peer):
        return remote(
            disp.at[slot_rows(peer)],
            xs.at[y, c, slot_rows(e)],
            a_send.at[0],
            a_recv.at[group],
            z=peer // nx,
            x=lax.rem(peer, nx),
        )

    def dispatch_far(peer):
        return remote(
            disp_far.at[slot_rows(peer)],
            xs.at[y_far, c, slot_rows(e)],
            f_send.at[0],
            f_recv.at[group],
            z=peer // nx,
            x=lax.rem(peer, nx),
        )

    for j in range(CHUNKS):
        each_other(nearby(j) * per_chunk, per_chunk, lambda peer: dispatch(peer).start())
    xs[y, c, slot_rows(e), :] = disp[slot_rows(e), :]
    xs[y_far, c, slot_rows(e), :] = disp_far[slot_rows(e), :]

    def query_copy(r):
        return remote(
            qb.at[x], qb.at[x], q_send.at[0], q_recv.at[0], x=lax.rem(x + r, nx)
        )

    reach = nz // 2

    def key_copy(block, r, to_z):
        return remote(kvb.at[block], kvb.at[block], k_send.at[r], k_recv.at[r], z=to_z)

    def chain_copy(r):
        return key_copy(jnp.maximum(z - r + 1, 0), r, jnp.minimum(z + 1, nz - 1))

    def far_copy(r):
        return key_copy(z, r, lax.rem(z + r, nz))

    def chain_send(r):
        @pl.when((z + 1 < nz) & (z - r + 1 >= 0))
        def _():
            chain_copy(r).start()

    def send_inputs():
        for r in range(1, nx):
            query_copy(r).start()
        chain_send(1)
        for j in range(CHUNKS):
            each_other(nearby(j) * per_chunk, per_chunk, lambda peer: dispatch_far(peer).start())

    def send_far_keys():
        for r in range(reach + 1, nz):

            @pl.when(z + r < nz)
            def _(r=r):
                far_copy(r).start()

    maps = 2 * rows
    qk = LANES // 2
    keep_low = lax.broadcasted_iota(jnp.int32, (rows, LANES), 1) < qk

    def stack_query(value, index):
        scaled = value.astype(F32) * (qk ** (-0.5))
        qs[index, 0:rows, :] = jnp.where(keep_low, scaled, 0.0).astype(BF16)
        qs[index, rows:maps, :] = jnp.where(keep_low, 0.0, scaled).astype(BF16)

    pieces = [(i, j * LANES) for i in range(nx) for j in range(maps // LANES)]

    def attend(key_block, value_block, masked):
        keys = key_block[...]
        values = value_block[...].T

        def score(index, first):
            return lax.dot_general(
                keys,
                qs[index, first : first + LANES, :],
                (((1,), (1,)), ((), ())),
                preferred_element_type=F32,
            )

        ahead = score(*pieces[0])
        for number, (index, first) in enumerate(pieces):
            scores = ahead
            if number + 1 < len(pieces):
                ahead = score(*pieces[number + 1])
            columns = slice(first, first + LANES)
            if masked:
                key_pos = x * rows + lax.broadcasted_iota(jnp.int32, scores.shape, 0)
                query_pos = lax.broadcasted_iota(jnp.int32, scores.shape, 1) + (
                    index * rows + first % rows
                )
                visible = query_pos >= key_pos
                scores = jnp.where(visible, scores, LOWEST)
                new_max = jnp.max(scores, axis=0, keepdims=True)
                terms = jnp.where(visible, jnp.exp(scores - new_max), 0.0)
            else:
                old_max = stat[index, 0:1, columns]
                new_max = jnp.maximum(old_max, jnp.max(scores, axis=0, keepdims=True))
                terms = jnp.exp(scores - new_max)
                factor = jnp.exp(old_max - new_max)
            total_terms = jnp.sum(terms, axis=0, keepdims=True)
            weighted = jnp.dot(values, terms.astype(BF16), preferred_element_type=F32)
            if masked:
                stat[index, 1:2, columns] = total_terms
                acc[index, :, columns] = weighted
            else:
                stat[index, 1:2, columns] = stat[index, 1:2, columns] * factor + total_terms
                acc[index, :, columns] = acc[index, :, columns] * factor + weighted
            stat[index, 0:1, columns] = new_max

    def own_attention():
        wait_arrived(qb.at[pl.ds(0, nx - 1)], q_recv.at[0])
        for index in range(nx):
            stack_query(qb[index], index)
        stat[...] = jnp.zeros_like(stat)
        attend(kvb.at[z, 0], kvb.at[z, 1], True)

    def chain_step(r):
        @pl.when(z >= r)
        def _():
            key_copy(jnp.maximum(z - r, 0), r, z).wait_recv()
            if r < reach:
                chain_send(r + 1)

    def attend_far(r):
        @pl.when(z >= r)
        def _():
            from_z = jnp.maximum(z - r, 0)
            if r > reach:
                key_copy(from_z, r, z).wait_recv()
            attend(kvb.at[from_z, 0], kvb.at[from_z, 1], False)

    def wait_rows(block, j, recv_sems):
        k = nearby(j)
        count = per_chunk - 1 if j == 0 else per_chunk
        span = pl.ds(pl.multiple_of(k * chunk, chunk), count * cap)
        wait_arrived(xs.at[block, c, span], recv_sems.at[k])

    def chunk_rows(k):
        return pl.ds(pl.multiple_of(k * chunk, chunk), chunk)

    def up_copy(s, k):
        where = chunk_rows(k)
        block = xs.at[y_at(-s), c, where]
        return remote(block, block, g_send.at[0], g_recv.at[0, k, s], y=y_next)

    def dn_copy(s, k):
        where = chunk_rows(k)
        block = xs.at[y_at(s), c, where]
        return remote(block, block, g_send.at[0], g_recv.at[1, k, s], y=y_prev)

    def mate_block(number, k, core):
        shift = (0, -1, 1, -2, 2, -3, 3, half_ring)[number]
        return xs.at[y_at(shift), core, chunk_rows(k)]

    def mate_copy(number, k):
        block = mate_block(number, k, c)
        return remote(block, block, m_send.at[0], m_recv.at[k], c=other)

    def first_sends(j):
        wait_rows(y, j, a_recv)
        k = nearby(j)
        up_copy(0, k).start()
        dn_copy(0, k).start()
        mate_copy(0, k).start()

    def pass_on(s, k):
        wait_arrived(xs.at[y_at(-s - 1), c, chunk_rows(k)], g_recv.at[0, k, s])
        if s + 2 < half_ring:
            up_copy(s + 1, k).start()
        mate_copy(2 * s + 1, k).start()
        wait_arrived(xs.at[y_at(s + 1), c, chunk_rows(k)], g_recv.at[1, k, s])
        if s + 2 < half_ring:
            dn_copy(s + 1, k).start()
        mate_copy(2 * s + 2, k).start()

    def far_rows(j):
        wait_rows(y_far, j, f_recv)
        mate_copy(ny - 1, nearby(j)).start()

    def result_copies(r):
        to_x = lax.rem(x + r, nx)
        return (
            remote(o_out.at[to_x], o_in.at[x], o_send.at[0], o_recv.at[0], x=to_x),
            remote(stat.at[to_x], stat_in.at[x], s_send.at[0], s_recv.at[0], x=to_x),
        )

    def send_results():
        o_out[...] = acc[...].astype(BF16)
        for r in range(1, nx):
            for copy in result_copies(r):
                copy.start()
        o_in[x] = o_out[x]
        stat_in[x] = stat[x]

    def expert(k):
        wait_arrived(xs.at[:, other, chunk_rows(k)], m_recv.at[k])
        gate = jnp.zeros((chunk, gw.shape[1]), F32)
        up = jnp.zeros((chunk, gw.shape[1]), F32)
        for block in range(ny):
            both = jnp.concatenate(
                [xs[block, 0, chunk_rows(k), :], xs[block, 1, chunk_rows(k), :]], axis=1
            )
            depth = slice(block * 2 * LANES, (block + 1) * 2 * LANES)
            gate += jnp.dot(both, gw[depth, :], preferred_element_type=F32)
            up += jnp.dot(both, uw[depth, :], preferred_element_type=F32)
        hidden = (gate / (1.0 + jnp.exp(-gate)) * up).astype(BF16)
        for block in range(ny):
            columns = slice(block * 2 * LANES, (block + 1) * 2 * LANES)
            value = jnp.dot(hidden, dw[:, columns], preferred_element_type=F32).astype(BF16)
            parts[k, 0, block] = value[:, :LANES]
            parts[k, 1, block] = value[:, LANES:]
        part_copy(k).start()

    def part_copy(k):
        return remote(parts.at[k, other], mate.at[k], pm_send.at[0], pm_recv.at[k], c=other)

    full = slice(0, chunk)
    top = slice(0, half)
    bottom = slice(half, chunk)

    def chip_sum(k, target, where):
        return parts[k, c, target, where, :].astype(F32) + mate[k, target, where, :].astype(F32)

    def sum_up(k, d):
        where = top if d == half_ring else full
        return remote(
            sb_up.at[k, d - 1, where], rb_up.at[k, d - 1, where],
            r_send.at[d // half_ring], r_recv.at[0, k, d - 1], y=y_next,
        )

    def sum_dn(k, d):
        where = bottom if d == half_ring else full
        return remote(
            sb_dn.at[k, d - 1, where], rb_dn.at[k, d - 1, where],
            r_send.at[d // half_ring], r_recv.at[1, k, d - 1], y=y_prev,
        )

    def sum_step(k, d):
        if d == half_ring:
            sb_up[k, d - 1, top] = chip_sum(k, y_at(d), top).astype(BF16)
            sum_up(k, d).start()
            sb_dn[k, d - 1, bottom] = chip_sum(k, y_at(-d), bottom).astype(BF16)
            sum_dn(k, d).start()
            return
        sum_up(k, d + 1).wait_recv()
        if d + 1 == half_ring:
            sb_up[k, d - 1, top] = (
                chip_sum(k, y_at(d), top) + rb_up[k, d, top].astype(F32)
            ).astype(BF16)
            sb_up[k, d - 1, bottom] = chip_sum(k, y_at(d), bottom).astype(BF16)
        else:
            sb_up[k, d - 1] = (
                chip_sum(k, y_at(d), full) + rb_up[k, d].astype(F32)
            ).astype(BF16)
        sum_up(k, d).start()
        sum_dn(k, d + 1).wait_recv()
        if d + 1 == half_ring:
            sb_dn[k, d - 1, bottom] = (
                chip_sum(k, y_at(-d), bottom) + rb_dn[k, d, bottom].astype(F32)
            ).astype(BF16)
            sb_dn[k, d - 1, top] = chip_sum(k, y_at(-d), top).astype(BF16)
        else:
            sb_dn[k, d - 1] = (
                chip_sum(k, y_at(-d), full) + rb_dn[k, d].astype(F32)
            ).astype(BF16)
        sum_dn(k, d).start()

    def answer(k):
        sum_up(k, 1).wait_recv()
        sum_dn(k, 1).wait_recv()
        ans[chunk_rows(k), :] = (
            chip_sum(k, y, full) + rb_up[k, 0].astype(F32) + rb_dn[k, 0].astype(F32)
        ).astype(BF16)
        each_other(k * per_chunk, per_chunk, lambda target: back_copy(target).start())

    def back_copy(target):
        return remote(
            ans.at[slot_rows(target)],
            ret.at[slot_rows(e)],
            b_send.at[0],
            b_recv.at[0],
            z=target // nx,
            x=lax.rem(target, nx),
        )

    def first_sum(k):
        part_copy(k).wait_recv()
        sum_step(k, half_ring)

    top_rows = pl.ds(0, rows // 2)
    low_rows = pl.ds(rows // 2, rows // 2)
    all_rows = pl.ds(0, rows)

    def head_up(s):
        where = top_rows if s == half_ring - 1 else all_rows
        block = heads.at[y_at(-s), c, where]
        return remote(block, block, h_send.at[(s + 1) // half_ring], h_recv.at[0, s], y=y_next)

    def head_dn(s):
        where = low_rows if s == half_ring - 1 else all_rows
        block = heads.at[y_at(s), c, where]
        return remote(block, block, h_send.at[(s + 1) // half_ring], h_recv.at[1, s], y=y_prev)

    def head_mate(number, core):
        s = (number - 1) // 2
        last = number > 0 and s == half_ring - 1
        if number == 0:
            block = heads.at[y, core]
        elif number % 2 == 1:
            block = heads.at[y_at(-s - 1), core, top_rows if last else all_rows]
        else:
            block = heads.at[y_at(s + 1), core, low_rows if last else all_rows]
        return remote(block, block, hm_send.at[0], hm_recv.at[1 if last else 0], c=other)

    def head_pass(s):
        last = s == half_ring - 1
        wait_arrived(heads.at[y_at(-s - 1), c, top_rows if last else all_rows], h_recv.at[0, s])
        if not last:
            head_up(s + 1).start()
        head_mate(2 * s + 1, c).start()
        wait_arrived(heads.at[y_at(s + 1), c, low_rows if last else all_rows], h_recv.at[1, s])
        if not last:
            head_dn(s + 1).start()
        head_mate(2 * s + 2, c).start()

    def merge():
        wait_arrived(o_in.at[pl.ds(0, nx - 1)], o_recv.at[0])
        wait_arrived(stat_in.at[pl.ds(0, nx - 1)], s_recv.at[0])
        top_max = stat_in[0, 0:1, :]
        for j in range(1, nx):
            top_max = jnp.maximum(top_max, stat_in[j, 0:1, :])
        denominator = jnp.zeros_like(top_max)
        weighted = jnp.zeros(o_in.shape[1:], F32)
        for j in range(nx):
            factor = jnp.exp(stat_in[j, 0:1, :] - top_max)
            denominator += factor * stat_in[j, 1:2, :]
            weighted += factor * o_in[j].astype(F32)
        mapped = weighted / denominator
        difference = mapped[:, :rows] - scale_ref[0:1, 0:1] * mapped[:, rows:]
        mean = jnp.sum(difference * difference, axis=0, keepdims=True) * (1.0 / LANES)
        head = difference * lax.rsqrt(mean + EPSILON)
        heads[y, c] = (head.T * hgain_ref[...]).astype(BF16)
        head_up(0).start()
        head_dn(0).start()
        head_mate(0, c).start()

    def weights_and_expert(k):
        if not weights_here:
            weights_here.append(True)
            for copy in weight_copies[:3]:
                copy.wait()
        expert(k)

    def sum_stage(d, k):
        if d == half_ring:
            first_sum(k)
        elif d > 0:
            sum_step(k, d)
        else:
            answer(k)

    def gather_stage(s, j):
        if s == 0:
            first_sends(j)
        else:
            pass_on(s - 1, nearby(j))

    def project_block(block):
        both = jnp.concatenate([heads[block, 0], heads[block, 1]], axis=1)
        depth = pl.ds(pl.multiple_of(block * 2 * LANES, 2 * LANES), 2 * LANES)
        return jnp.dot(both, ow[depth, :], preferred_element_type=F32)

    def project_most():
        weight_copies[3].wait()
        wait_arrived(heads.at[pl.ds(0, ny - 1), other], hm_recv.at[0])
        total_so_far = project_block(y)
        for shift in range(1, half_ring):
            total_so_far += project_block(y_at(shift)) + project_block(y_at(-shift))
        mixed[...] = total_so_far

    def drain():
        others = pl.ds(0, (nep - 1) * cap)
        wait_sent(disp.at[others], a_send.at[0])
        wait_sent(disp_far.at[others], f_send.at[0])
        wait_sent(xs.at[pl.ds(0, 2 * half_ring - 2), c], g_send.at[0])
        wait_sent(xs.at[:, c], m_send.at[0])
        wait_sent(mate, pm_send.at[0])
        wait_sent(mate.at[:, pl.ds(0, 2 * half_ring - 2)], r_send.at[0])
        wait_sent(sb_up.at[:, 0], r_send.at[1])
        wait_sent(qb.at[pl.ds(0, nx - 1)], q_send.at[0])
        wait_sent(o_out.at[pl.ds(0, nx - 1)], o_send.at[0])
        wait_sent(stat.at[pl.ds(0, nx - 1)], s_send.at[0])
        for r in range(1, reach + 1):

            @pl.when((z + 1 < nz) & (z - r + 1 >= 0))
            def _(r=r):
                chain_copy(r).wait_send()

        for r in range(reach + 1, nz):

            @pl.when(z + r < nz)
            def _(r=r):
                far_copy(r).wait_send()

    weights_here = []
    stages = {
        "gather": gather_stage,
        "inputs": send_inputs,
        "keys": send_far_keys,
        "far": far_rows,
        "chain": chain_step,
        "own": own_attention,
        "attend": attend_far,
        "expert": lambda j: weights_and_expert(nearby(j)),
        "sum": lambda d, j: sum_stage(d, nearby(j)),
        "results": send_results,
        "merge": merge,
        "heads": lambda s: head_pass(s - 1),
        "drain": drain,
        "project": project_most,
    }
    for stage in ORDER:
        stages[stage[0]](*stage[1:])
    ret[slot_rows(e), :] = ans[slot_rows(e), :]

    wait_arrived(heads.at[0, other], hm_recv.at[1])
    out_ref[0] = (mixed[...] + project_block(y_far)).astype(BF16)

    wait_sent(heads.at[pl.ds(0, 2 * half_ring - 2), c], h_send.at[0])
    wait_sent(heads.at[0, c], h_send.at[1])
    wait_sent(heads.at[:, c], hm_send.at[0])

    wait_arrived(ret.at[pl.ds(0, (nep - 1) * cap)], b_recv.at[0])
    routed = jnp.zeros((LANES, rows), F32)
    for i in range(2):
        routed += weight[i : i + 1, :] * lax.dot_general(
            ret[...], one_hot(i), (((0,), (0,)), ((), ())), preferred_element_type=F32
        )
    out_ref[1] = routed.T.astype(BF16)

    wait_sent(ans.at[pl.ds(0, (nep - 1) * cap)], b_send.at[0])


def local(
    sizes,
    queries,
    key_rows,
    values,
    second_scale,
    head_gain,
    out_weight,
    routed_in,
    routed_gain,
    expert_ids,
    group_logits,
    inner_logits,
    gate_weight,
    up_weight,
    down_weight,
):
    nz, nx, ny = sizes
    nep = nz * nx
    rows = routed_in.shape[0]
    width = routed_in.shape[1]
    hidden = gate_weight.shape[2]
    cap = 2 * expert_ids.shape[1] * rows // nep
    total = nep * cap
    chunk = total // CHUNKS
    half_ring = ny // 2
    dma = pltpu.SemaphoreType.DMA
    vmem = pltpu.VMEM
    scratch = [
        vmem((width, hidden), BF16),
        vmem((width, hidden), BF16),
        vmem((hidden, width), BF16),
        vmem(out_weight.shape, BF16),
        vmem((rows, width), BF16),
        vmem((1, 1), F32),
        vmem((1, LANES), F32),
        vmem((1, width), F32),
        vmem((2, rows), jnp.int32),
        vmem((group_logits.shape[1], rows), F32),
        vmem((2, rows), F32),
        dma((4,)),
        dma((10,)),
        vmem((8, rows), F32),
        vmem((8, rows), F32),
        vmem((total, LANES), BF16),
        vmem((total, LANES), BF16),
        vmem((ny, 2, total, LANES), BF16),
        vmem((CHUNKS, 2, ny, chunk, LANES), BF16),
        vmem((CHUNKS, ny, chunk, LANES), BF16),
        vmem((CHUNKS, half_ring, chunk, LANES), BF16),
        vmem((CHUNKS, half_ring, chunk, LANES), BF16),
        vmem((CHUNKS, half_ring, chunk, LANES), BF16),
        vmem((CHUNKS, half_ring, chunk, LANES), BF16),
        vmem((total, LANES), BF16),
        vmem((total, LANES), BF16),
        dma((1,)),
        dma((CHUNKS,)),
        dma((1,)),
        dma((CHUNKS,)),
        dma((1,)),
        dma((2, CHUNKS, half_ring - 1)),
        dma((1,)),
        dma((CHUNKS,)),
        dma((1,)),
        dma((CHUNKS,)),
        dma((2,)),
        dma((2, CHUNKS, half_ring)),
        dma((1,)),
        dma((1,)),
        vmem((nx, rows, LANES), BF16),
        vmem((nx, 2 * rows, LANES), BF16),
        vmem((nz, 2, rows, LANES), BF16),
        vmem((nx, LANES, 2 * rows), F32),
        vmem((nx, 8, 2 * rows), F32),
        vmem((nx, LANES, 2 * rows), BF16),
        vmem((nx, LANES, 2 * rows), BF16),
        vmem((nx, 8, 2 * rows), F32),
        vmem((ny, 2, rows, LANES), BF16),
        vmem((rows, LANES), F32),
        dma((1,)),
        dma((1,)),
        dma((nz,)),
        dma((nz,)),
        dma((1,)),
        dma((1,)),
        dma((1,)),
        dma((1,)),
        dma((2,)),
        dma((2, half_ring)),
        dma((1,)),
        dma((2,)),
    ]
    whole = pl.BlockSpec(memory_space=pltpu.VMEM)
    far = pl.BlockSpec(memory_space=pl.ANY)
    both = pl.pallas_call(
        lambda *refs: kernel(sizes, *refs),
        out_shape=pltpu.VMEM((2, rows, LANES), BF16),
        in_specs=[far] * 14,
        out_specs=whole,
        scratch_shapes=scratch,
        compiler_params=pltpu.CompilerParams(
            collective_id=0, has_side_effects=True, vmem_limit_bytes=60 * 1024 * 1024
        ),
    )(
        queries,
        key_rows,
        values,
        second_scale.reshape(1, 1),
        head_gain.reshape(1, -1),
        out_weight,
        routed_in,
        routed_gain.reshape(1, -1),
        expert_ids.T,
        group_logits.T,
        inner_logits.T,
        gate_weight[0],
        up_weight[0],
        down_weight[0],
    )
    return both[0], both[1]


def build(mesh, sizes):
    nz, nx, ny = sizes
    finer = Mesh(mesh.devices.reshape(nz, nx, ny, 2), ("z", "x", "y", "c"))
    ep, tp = ("z", "x"), ("y", "c")
    placed = (
        P(ep, tp),
        P(ep, tp),
        P(ep, tp),
        P(tp),
        P(),
        P(None, tp),
        P(ep, None),
        P(),
        P(ep, None),
        P(ep, None),
        P(ep, None),
        P(ep, None, tp),
        P(ep, None, tp),
        P(ep, tp, None),
    )
    return jax.shard_map(
        lambda *args: local(sizes, *args),
        mesh=finer,
        in_specs=placed,
        out_specs=(P(ep, tp), P(ep, tp)),
        check_vma=False,
    )


def solution(mesh):
    return build(mesh, (8, 4, mesh.shape["tp"] // 2))
```

```python
import jax
import jax.numpy as jnp
from jax import lax
from jax.experimental import pallas as pl
from jax.experimental.pallas import tpu as pltpu
from jax.sharding import Mesh
from jax.sharding import PartitionSpec as P

EPSILON = 1e-05
LOWEST = -1e30
GROUP_SIZE = 4
LANES = 128
CHUNKS = 8
ORDER = (
    ("gather", 0, 0),
    ("inputs",),
    ("gather", 0, 1),
    ("gather", 1, 0),
    ("gather", 0, 2),
    ("gather", 0, 3),
    ("gather", 1, 1),
    ("gather", 0, 4),
    ("gather", 2, 0),
    ("gather", 0, 5),
    ("own",),
    ("gather", 1, 3),
    ("chain", 1),
    ("keys",),
    ("gather", 1, 2),
    ("gather", 0, 7),
    ("gather", 2, 1),
    ("attend", 1),
    ("gather", 1, 4),
    ("gather", 3, 0),
    ("gather", 0, 6),
    ("gather", 1, 5),
    ("gather", 2, 3),
    ("far", 0),
    ("gather", 2, 2),
    ("far", 1),
    ("gather", 1, 7),
    ("expert", 0),
    ("far", 2),
    ("gather", 3, 1),
    ("chain", 2),
    ("attend", 2),
    ("sum", 4, 0),
    ("far", 3),
    ("gather", 2, 4),
    ("far", 4),
    ("expert", 1),
    ("gather", 1, 6),
    ("far", 5),
    ("gather", 3, 3),
    ("gather", 2, 5),
    ("far", 6),
    ("far", 7),
    ("gather", 3, 2),
    ("sum", 4, 1),
    ("expert", 3),
    ("gather", 2, 7),
    ("sum", 3, 0),
    ("expert", 2),
    ("gather", 3, 4),
    ("chain", 3),
    ("sum", 4, 3),
    ("attend", 3),
    ("sum", 4, 2),
    ("sum", 3, 1),
    ("expert", 4),
    ("gather", 3, 7),
    ("gather", 3, 5),
    ("gather", 2, 6),
    ("sum", 2, 0),
    ("sum", 3, 3),
    ("expert", 7),
    ("expert", 5),
    ("sum", 2, 1),
    ("sum", 3, 2),
    ("sum", 4, 4),
    ("sum", 4, 7),
    ("gather", 3, 6),
    ("chain", 4),
    ("attend", 4),
    ("sum", 1, 0),
    ("sum", 2, 3),
    ("attend", 5),
    ("attend", 6),
    ("sum", 3, 4),
    ("attend", 7),
    ("results",),
    ("sum", 3, 7),
    ("sum", 1, 3),
    ("sum", 2, 2),
    ("sum", 0, 0),
    ("expert", 6),
    ("sum", 4, 5),
    ("sum", 2, 4),
    ("sum", 1, 1),
    ("sum", 4, 6),
    ("sum", 2, 7),
    ("sum", 0, 3),
    ("sum", 1, 2),
    ("sum", 3, 5),
    ("sum", 1, 4),
    ("sum", 0, 1),
    ("sum", 3, 6),
    ("merge",),
    ("sum", 1, 7),
    ("sum", 0, 2),
    ("sum", 2, 5),
    ("sum", 0, 4),
    ("sum", 2, 6),
    ("heads", 1),
    ("sum", 0, 7),
    ("sum", 1, 5),
    ("sum", 1, 6),
    ("heads", 2),
    ("sum", 0, 5),
    ("sum", 0, 6),
    ("heads", 3),
    ("drain",),
    ("project",),
    ("heads", 4),
)
F32 = jnp.float32
BF16 = jnp.bfloat16


def remote(src, dst, send_sem, recv_sem, **where):
    return pltpu.make_async_remote_copy(
        src_ref=src,
        dst_ref=dst,
        send_sem=send_sem,
        recv_sem=recv_sem,
        device_id=where,
        device_id_type=pl.DeviceIdType.MESH,
    )


def loop(first, last, body):
    def step(i, carry):
        body(i)
        return carry

    lax.fori_loop(first, last, step, 0)


def kernel(
    sizes,
    q_hbm,
    k_hbm,
    v_hbm,
    scale_hbm,
    hgain_hbm,
    ow_hbm,
    rin_hbm,
    rgain_hbm,
    ids_hbm,
    gl_hbm,
    il_hbm,
    gw_hbm,
    uw_hbm,
    dw_hbm,
    out_ref,
    gw,
    uw,
    dw,
    ow,
    rin,
    scale_ref,
    hgain_ref,
    rgain_ref,
    ids_ref,
    gl_ref,
    il_ref,
    w_sem,
    i_sem,
    pos,
    weight,
    disp,
    disp_far,
    xs,
    parts,
    mate,
    rb_up,
    rb_dn,
    sb_up,
    sb_dn,
    ans,
    ret,
    a_send,
    a_recv,
    f_send,
    f_recv,
    g_send,
    g_recv,
    m_send,
    m_recv,
    pm_send,
    pm_recv,
    r_send,
    r_recv,
    b_send,
    b_recv,
    qb,
    qs,
    kvb,
    acc,
    stat,
    o_out,
    o_in,
    stat_in,
    heads,
    mixed,
    q_send,
    q_recv,
    k_send,
    k_recv,
    o_send,
    o_recv,
    s_send,
    s_recv,
    h_send,
    h_recv,
    hm_send,
    hm_recv,
):
    nz, nx, ny = sizes
    nep = nz * nx
    half_ring = ny // 2
    z, x, y, c = (lax.axis_index(name) for name in ("z", "x", "y", "c"))
    other = 1 - c
    e = z * nx + x
    t = y * 2 + c
    rows = rin.shape[0]
    width = rin.shape[1]
    total = xs.shape[2]
    cap = total // nep
    chunk = total // CHUNKS
    half = chunk // 2
    per_chunk = nep // CHUNKS
    y_next = lax.rem(y + 1, ny)
    y_prev = lax.rem(y + ny - 1, ny)

    def y_at(shift):
        return lax.rem(y + shift + ny, ny)

    group = z // (nz // CHUNKS)

    def nearby(j):
        return lax.rem(group + (0, 1, 7, 2, 6, 3, 5, 4)[j], CHUNKS)

    def wait_sent(block, sem):
        remote(block, block, sem, sem, c=other).wait_send()

    def wait_arrived(block, sem):
        remote(block, block, sem, sem, c=other).wait_recv()

    def each_other(first, count, body):
        def one(i):
            @pl.when(first + i != e)
            def _():
                body(first + i)

        loop(0, count, one)


    input_copies = [
        pltpu.make_async_copy(src, dst, i_sem.at[i])
        for i, (src, dst) in enumerate(
            (
                (rin_hbm, rin),
                (ids_hbm, ids_ref),
                (gl_hbm, gl_ref),
                (il_hbm, il_ref),
                (rgain_hbm, rgain_ref),
                (q_hbm, qb.at[x]),
                (k_hbm, kvb.at[z, 0]),
                (v_hbm, kvb.at[z, 1]),
                (scale_hbm, scale_ref),
                (hgain_hbm, hgain_ref),
            )
        )
    ]
    weight_copies = [
        pltpu.make_async_copy(src, dst, w_sem.at[i])
        for i, (src, dst) in enumerate(
            ((gw_hbm, gw), (uw_hbm, uw), (dw_hbm, dw), (ow_hbm, ow))
        )
    ]
    for copy in input_copies:
        copy.start()

    barrier = pltpu.get_barrier_semaphore()

    def greet(**where):
        pl.semaphore_signal(
            barrier, inc=1, device_id=where, device_id_type=pl.DeviceIdType.MESH
        )

    near_z = [lax.rem(z + d, nz) for d in range(nz)]
    near_x = [lax.rem(x + d, nx) for d in range(nx)]
    apart = [(i, j) for i in range(nz) for j in range(nx) if i + j > 0]
    for i, j in sorted(apart, key=lambda ij: -min(ij[0], nz - ij[0]) - min(ij[1], nx - ij[1])):
        greet(z=near_z[i], x=near_x[j])
    greet(y=y_next)
    greet(y=y_prev)
    greet(c=other)

    for copy in input_copies[1:5]:
        copy.wait()
    ids = ids_ref[...]
    shape = (nep, rows)
    expert_row = lax.broadcasted_iota(jnp.int32, shape, 0)
    picks = [jnp.where(ids[i : i + 1, :] == expert_row, 1.0, 0.0) for i in range(2)]
    earlier = jnp.where(
        lax.broadcasted_iota(jnp.int32, (rows, rows), 0)
        < lax.broadcasted_iota(jnp.int32, (rows, rows), 1),
        1.0,
        0.0,
    ).astype(BF16)
    before = [jnp.dot(pick.astype(BF16), earlier, preferred_element_type=F32) for pick in picks]
    before[1] += jnp.sum(picks[0], axis=1, keepdims=True)
    logits = gl_ref[...]
    group_exp = jnp.exp(logits - jnp.max(logits, axis=0, keepdims=True))
    group_prob = group_exp / jnp.sum(group_exp, axis=0, keepdims=True)
    group_row = lax.broadcasted_iota(jnp.int32, logits.shape, 0)
    inner = il_ref[...]
    inner_exp = jnp.exp(inner - jnp.max(inner, axis=0, keepdims=True))
    inner_prob = inner_exp / jnp.sum(inner_exp, axis=0, keepdims=True)
    for i in range(2):
        pos[i : i + 1, :] = ids[i : i + 1, :].astype(F32) * cap + jnp.sum(
            picks[i] * before[i], axis=0, keepdims=True
        )
        chosen = ids[i : i + 1, :] // GROUP_SIZE == group_row
        picked = jnp.sum(jnp.where(chosen, group_prob, 0.0), axis=0, keepdims=True)
        weight[i : i + 1, :] = picked * inner_prob[i : i + 1, :]

    def one_hot(i):
        slots = lax.broadcasted_iota(jnp.int32, (total, rows), 0).astype(F32)
        return jnp.where(pos[i : i + 1, :] == slots, 1.0, 0.0).astype(BF16)

    input_copies[0].wait()
    source = rin[...].astype(F32)
    inv = lax.rsqrt(jnp.sum(source * source, axis=-1, keepdims=True) * (1.0 / width) + EPSILON)

    def normed(block):
        columns = pl.ds(pl.multiple_of((block * 2 + c) * LANES, LANES), LANES)
        return (rin[:, columns].astype(F32) * inv * rgain_ref[:, columns]).astype(BF16)

    y_far = y_at(half_ring)
    spread = jnp.dot(
        one_hot(0) + one_hot(1),
        jnp.concatenate([normed(y), normed(y_far)], axis=1),
        preferred_element_type=F32,
    ).astype(BF16)
    disp[...] = spread[:, :LANES]
    disp_far[...] = spread[:, LANES:]
    for copy in input_copies[5:]:
        copy.wait()
    for copy in weight_copies:
        copy.start()

    pl.semaphore_wait(barrier, nep - 1 + 2 + 1)

    def slot_rows(index):
        return pl.ds(pl.multiple_of(index * cap, cap), cap)

    def dispatch(peer):
        return remote(
            disp.at[slot_rows(peer)],
            xs.at[y, c, slot_rows(e)],
            a_send.at[0],
            a_recv.at[group],
            z=peer // nx,
            x=lax.rem(peer, nx),
        )

    def dispatch_far(peer):
        return remote(
            disp_far.at[slot_rows(peer)],
            xs.at[y_far, c, slot_rows(e)],
            f_send.at[0],
            f_recv.at[group],
            z=peer // nx,
            x=lax.rem(peer, nx),
        )

    for j in range(CHUNKS):
        each_other(nearby(j) * per_chunk, per_chunk, lambda peer: dispatch(peer).start())
    xs[y, c, slot_rows(e), :] = disp[slot_rows(e), :]
    xs[y_far, c, slot_rows(e), :] = disp_far[slot_rows(e), :]

    def query_copy(r):
        return remote(
            qb.at[x], qb.at[x], q_send.at[0], q_recv.at[0], x=lax.rem(x + r, nx)
        )

    reach = nz // 2

    def key_copy(block, r, to_z):
        return remote(kvb.at[block], kvb.at[block], k_send.at[r], k_recv.at[r], z=to_z)

    def chain_copy(r):
        return key_copy(jnp.maximum(z - r + 1, 0), r, jnp.minimum(z + 1, nz - 1))

    def far_copy(r):
        return key_copy(z, r, lax.rem(z + r, nz))

    def chain_send(r):
        @pl.when((z + 1 < nz) & (z - r + 1 >= 0))
        def _():
            chain_copy(r).start()

    def send_inputs():
        for r in range(1, nx):
            query_copy(r).start()
        chain_send(1)
        for j in range(CHUNKS):
            each_other(nearby(j) * per_chunk, per_chunk, lambda peer: dispatch_far(peer).start())

    def send_far_keys():
        for r in range(reach + 1, nz):

            @pl.when(z + r < nz)
            def _(r=r):
                far_copy(r).start()

    maps = 2 * rows
    qk = LANES // 2
    keep_low = lax.broadcasted_iota(jnp.int32, (rows, LANES), 1) < qk

    def stack_query(value, index):
        scaled = value.astype(F32) * (qk ** (-0.5))
        qs[index, 0:rows, :] = jnp.where(keep_low, scaled, 0.0).astype(BF16)
        qs[index, rows:maps, :] = jnp.where(keep_low, 0.0, scaled).astype(BF16)

    pieces = [(i, j * LANES) for i in range(nx) for j in range(maps // LANES)]

    def attend(key_block, value_block, masked):
        keys = key_block[...]
        values = value_block[...].T

        def score(index, first):
            return lax.dot_general(
                keys,
                qs[index, first : first + LANES, :],
                (((1,), (1,)), ((), ())),
                preferred_element_type=F32,
            )

        ahead = score(*pieces[0])
        for number, (index, first) in enumerate(pieces):
            scores = ahead
            if number + 1 < len(pieces):
                ahead = score(*pieces[number + 1])
            columns = slice(first, first + LANES)
            sums_at = slice(maps + first, maps + first + LANES)
            if masked:
                key_pos = x * rows + lax.broadcasted_iota(jnp.int32, scores.shape, 0)
                query_pos = lax.broadcasted_iota(jnp.int32, scores.shape, 1) + (
                    index * rows + first % rows
                )
                visible = query_pos >= key_pos
                scores = jnp.where(visible, scores, LOWEST)
                new_max = jnp.max(scores, axis=0, keepdims=True)
                terms = jnp.where(visible, jnp.exp(scores - new_max), 0.0)
            else:
                old_max = stat[index, 0:1, columns]
                new_max = jnp.maximum(old_max, jnp.max(scores, axis=0, keepdims=True))
                terms = jnp.exp(scores - new_max)
                factor = jnp.exp(old_max - new_max)
            total_terms = jnp.sum(terms, axis=0, keepdims=True)
            weighted = jnp.dot(values, terms.astype(BF16), preferred_element_type=F32)
            if masked:
                stat[index, 0:1, sums_at] = total_terms
                acc[index, :, columns] = weighted
            else:
                stat[index, 0:1, sums_at] = stat[index, 0:1, sums_at] * factor + total_terms
                acc[index, :, columns] = acc[index, :, columns] * factor + weighted
            stat[index, 0:1, columns] = new_max

    def own_attention():
        wait_arrived(qb.at[pl.ds(0, nx - 1)], q_recv.at[0])
        for index in range(nx):
            stack_query(qb[index], index)
        stat[...] = jnp.zeros_like(stat)
        attend(kvb.at[z, 0], kvb.at[z, 1], True)

    def chain_step(r):
        @pl.when(z >= r)
        def _():
            key_copy(jnp.maximum(z - r, 0), r, z).wait_recv()
            if r < reach:
                chain_send(r + 1)

    def attend_far(r):
        @pl.when(z >= r)
        def _():
            from_z = jnp.maximum(z - r, 0)
            if r > reach:
                key_copy(from_z, r, z).wait_recv()
            attend(kvb.at[from_z, 0], kvb.at[from_z, 1], False)

    def wait_rows(block, j, recv_sems):
        k = nearby(j)
        count = per_chunk - 1 if j == 0 else per_chunk
        span = pl.ds(pl.multiple_of(k * chunk, chunk), count * cap)
        wait_arrived(xs.at[block, c, span], recv_sems.at[k])

    def chunk_rows(k):
        return pl.ds(pl.multiple_of(k * chunk, chunk), chunk)

    def up_copy(s, k):
        where = chunk_rows(k)
        block = xs.at[y_at(-s), c, where]
        return remote(block, block, g_send.at[0], g_recv.at[0, k, s], y=y_next)

    def dn_copy(s, k):
        where = chunk_rows(k)
        block = xs.at[y_at(s), c, where]
        return remote(block, block, g_send.at[0], g_recv.at[1, k, s], y=y_prev)

    def mate_block(number, k, core):
        shift = (0, -1, 1, -2, 2, -3, 3, half_ring)[number]
        return xs.at[y_at(shift), core, chunk_rows(k)]

    def mate_copy(number, k):
        block = mate_block(number, k, c)
        return remote(block, block, m_send.at[0], m_recv.at[k], c=other)

    def first_sends(j):
        wait_rows(y, j, a_recv)
        k = nearby(j)
        up_copy(0, k).start()
        dn_copy(0, k).start()
        mate_copy(0, k).start()

    def pass_on(s, k):
        wait_arrived(xs.at[y_at(-s - 1), c, chunk_rows(k)], g_recv.at[0, k, s])
        if s + 2 < half_ring:
            up_copy(s + 1, k).start()
        mate_copy(2 * s + 1, k).start()
        wait_arrived(xs.at[y_at(s + 1), c, chunk_rows(k)], g_recv.at[1, k, s])
        if s + 2 < half_ring:
            dn_copy(s + 1, k).start()
        mate_copy(2 * s + 2, k).start()

    def far_rows(j):
        wait_rows(y_far, j, f_recv)
        mate_copy(ny - 1, nearby(j)).start()

    def result_copies(r):
        to_x = lax.rem(x + r, nx)
        return (
            remote(o_out.at[to_x], o_in.at[x], o_send.at[0], o_recv.at[0], x=to_x),
            remote(stat.at[to_x], stat_in.at[x], s_send.at[0], s_recv.at[0], x=to_x),
        )

    def send_results():
        o_out[...] = acc[...].astype(BF16)
        for r in range(1, nx):
            for copy in result_copies(r):
                copy.start()
        o_in[x] = o_out[x]
        stat_in[x] = stat[x]

    def expert(k):
        wait_arrived(xs.at[:, other, chunk_rows(k)], m_recv.at[k])
        gate = jnp.zeros((chunk, gw.shape[1]), F32)
        up = jnp.zeros((chunk, gw.shape[1]), F32)
        for block in range(ny):
            both = jnp.concatenate(
                [xs[block, 0, chunk_rows(k), :], xs[block, 1, chunk_rows(k), :]], axis=1
            )
            depth = slice(block * 2 * LANES, (block + 1) * 2 * LANES)
            gate += jnp.dot(both, gw[depth, :], preferred_element_type=F32)
            up += jnp.dot(both, uw[depth, :], preferred_element_type=F32)
        hidden = (gate / (1.0 + jnp.exp(-gate)) * up).astype(BF16)
        for block in range(ny):
            columns = slice(block * 2 * LANES, (block + 1) * 2 * LANES)
            value = jnp.dot(hidden, dw[:, columns], preferred_element_type=F32).astype(BF16)
            parts[k, 0, block] = value[:, :LANES]
            parts[k, 1, block] = value[:, LANES:]
        part_copy(k).start()

    def part_copy(k):
        return remote(parts.at[k, other], mate.at[k], pm_send.at[0], pm_recv.at[k], c=other)

    full = slice(0, chunk)
    top = slice(0, half)
    bottom = slice(half, chunk)

    def chip_sum(k, target, where):
        return parts[k, c, target, where, :].astype(F32) + mate[k, target, where, :].astype(F32)

    def sum_up(k, d):
        where = top if d == half_ring else full
        return remote(
            sb_up.at[k, d - 1, where], rb_up.at[k, d - 1, where],
            r_send.at[d // half_ring], r_recv.at[0, k, d - 1], y=y_next,
        )

    def sum_dn(k, d):
        where = bottom if d == half_ring else full
        return remote(
            sb_dn.at[k, d - 1, where], rb_dn.at[k, d - 1, where],
            r_send.at[d // half_ring], r_recv.at[1, k, d - 1], y=y_prev,
        )

    def sum_step(k, d):
        if d == half_ring:
            sb_up[k, d - 1, top] = chip_sum(k, y_at(d), top).astype(BF16)
            sum_up(k, d).start()
            sb_dn[k, d - 1, bottom] = chip_sum(k, y_at(-d), bottom).astype(BF16)
            sum_dn(k, d).start()
            return
        sum_up(k, d + 1).wait_recv()
        if d + 1 == half_ring:
            sb_up[k, d - 1, top] = (
                chip_sum(k, y_at(d), top) + rb_up[k, d, top].astype(F32)
            ).astype(BF16)
            sb_up[k, d - 1, bottom] = chip_sum(k, y_at(d), bottom).astype(BF16)
        else:
            sb_up[k, d - 1] = (
                chip_sum(k, y_at(d), full) + rb_up[k, d].astype(F32)
            ).astype(BF16)
        sum_up(k, d).start()
        sum_dn(k, d + 1).wait_recv()
        if d + 1 == half_ring:
            sb_dn[k, d - 1, bottom] = (
                chip_sum(k, y_at(-d), bottom) + rb_dn[k, d, bottom].astype(F32)
            ).astype(BF16)
            sb_dn[k, d - 1, top] = chip_sum(k, y_at(-d), top).astype(BF16)
        else:
            sb_dn[k, d - 1] = (
                chip_sum(k, y_at(-d), full) + rb_dn[k, d].astype(F32)
            ).astype(BF16)
        sum_dn(k, d).start()

    def answer(k):
        sum_up(k, 1).wait_recv()
        sum_dn(k, 1).wait_recv()
        ans[chunk_rows(k), :] = (
            chip_sum(k, y, full) + rb_up[k, 0].astype(F32) + rb_dn[k, 0].astype(F32)
        ).astype(BF16)
        each_other(k * per_chunk, per_chunk, lambda target: back_copy(target).start())

    def back_copy(target):
        return remote(
            ans.at[slot_rows(target)],
            ret.at[slot_rows(e)],
            b_send.at[0],
            b_recv.at[0],
            z=target // nx,
            x=lax.rem(target, nx),
        )

    def first_sum(k):
        part_copy(k).wait_recv()
        sum_step(k, half_ring)

    top_rows = pl.ds(0, rows // 2)
    low_rows = pl.ds(rows // 2, rows // 2)
    all_rows = pl.ds(0, rows)

    def head_up(s):
        where = top_rows if s == half_ring - 1 else all_rows
        block = heads.at[y_at(-s), c, where]
        return remote(block, block, h_send.at[(s + 1) // half_ring], h_recv.at[0, s], y=y_next)

    def head_dn(s):
        where = low_rows if s == half_ring - 1 else all_rows
        block = heads.at[y_at(s), c, where]
        return remote(block, block, h_send.at[(s + 1) // half_ring], h_recv.at[1, s], y=y_prev)

    def head_mate(number, core):
        s = (number - 1) // 2
        last = number > 0 and s == half_ring - 1
        if number == 0:
            block = heads.at[y, core]
        elif number % 2 == 1:
            block = heads.at[y_at(-s - 1), core, top_rows if last else all_rows]
        else:
            block = heads.at[y_at(s + 1), core, low_rows if last else all_rows]
        return remote(block, block, hm_send.at[0], hm_recv.at[1 if last else 0], c=other)

    def head_pass(s):
        last = s == half_ring - 1
        wait_arrived(heads.at[y_at(-s - 1), c, top_rows if last else all_rows], h_recv.at[0, s])
        if not last:
            head_up(s + 1).start()
        head_mate(2 * s + 1, c).start()
        wait_arrived(heads.at[y_at(s + 1), c, low_rows if last else all_rows], h_recv.at[1, s])
        if not last:
            head_dn(s + 1).start()
        head_mate(2 * s + 2, c).start()

    def merge():
        wait_arrived(o_in.at[pl.ds(0, nx - 1)], o_recv.at[0])
        wait_arrived(stat_in.at[pl.ds(0, nx - 1)], s_recv.at[0])
        top_max = stat_in[0, 0:1, :maps]
        for j in range(1, nx):
            top_max = jnp.maximum(top_max, stat_in[j, 0:1, :maps])
        denominator = jnp.zeros_like(top_max)
        weighted = jnp.zeros(o_in.shape[1:], F32)
        for j in range(nx):
            factor = jnp.exp(stat_in[j, 0:1, :maps] - top_max)
            denominator += factor * stat_in[j, 0:1, maps:]
            weighted += factor * o_in[j].astype(F32)
        mapped = weighted / denominator
        difference = mapped[:, :rows] - scale_ref[0:1, 0:1] * mapped[:, rows:]
        mean = jnp.sum(difference * difference, axis=0, keepdims=True) * (1.0 / LANES)
        head = difference * lax.rsqrt(mean + EPSILON)
        heads[y, c] = (head.T * hgain_ref[...]).astype(BF16)
        head_up(0).start()
        head_dn(0).start()
        head_mate(0, c).start()

    def weights_and_expert(k):
        if not weights_here:
            weights_here.append(True)
            for copy in weight_copies[:3]:
                copy.wait()
        expert(k)

    def sum_stage(d, k):
        if d == half_ring:
            first_sum(k)
        elif d > 0:
            sum_step(k, d)
        else:
            answer(k)

    def gather_stage(s, j):
        if s == 0:
            first_sends(j)
        else:
            pass_on(s - 1, nearby(j))

    def project_block(block):
        both = jnp.concatenate([heads[block, 0], heads[block, 1]], axis=1)
        depth = pl.ds(pl.multiple_of(block * 2 * LANES, 2 * LANES), 2 * LANES)
        return jnp.dot(both, ow[depth, :], preferred_element_type=F32)

    def project_most():
        weight_copies[3].wait()
        wait_arrived(heads.at[pl.ds(0, ny - 1), other], hm_recv.at[0])
        total_so_far = project_block(y)
        for shift in range(1, half_ring):
            total_so_far += project_block(y_at(shift)) + project_block(y_at(-shift))
        mixed[...] = total_so_far

    def drain():
        others = pl.ds(0, (nep - 1) * cap)
        wait_sent(disp.at[others], a_send.at[0])
        wait_sent(disp_far.at[others], f_send.at[0])
        wait_sent(xs.at[pl.ds(0, 2 * half_ring - 2), c], g_send.at[0])
        wait_sent(xs.at[:, c], m_send.at[0])
        wait_sent(mate, pm_send.at[0])
        wait_sent(mate.at[:, pl.ds(0, 2 * half_ring - 2)], r_send.at[0])
        wait_sent(sb_up.at[:, 0], r_send.at[1])
        wait_sent(qb.at[pl.ds(0, nx - 1)], q_send.at[0])
        wait_sent(o_out.at[pl.ds(0, nx - 1)], o_send.at[0])
        wait_sent(stat.at[pl.ds(0, nx - 1)], s_send.at[0])
        for r in range(1, reach + 1):

            @pl.when((z + 1 < nz) & (z - r + 1 >= 0))
            def _(r=r):
                chain_copy(r).wait_send()

        for r in range(reach + 1, nz):

            @pl.when(z + r < nz)
            def _(r=r):
                far_copy(r).wait_send()

    weights_here = []
    stages = {
        "gather": gather_stage,
        "inputs": send_inputs,
        "keys": send_far_keys,
        "far": far_rows,
        "chain": chain_step,
        "own": own_attention,
        "attend": attend_far,
        "expert": lambda j: weights_and_expert(nearby(j)),
        "sum": lambda d, j: sum_stage(d, nearby(j)),
        "results": send_results,
        "merge": merge,
        "heads": lambda s: head_pass(s - 1),
        "drain": drain,
        "project": project_most,
    }
    for stage in ORDER:
        stages[stage[0]](*stage[1:])
    ret[slot_rows(e), :] = ans[slot_rows(e), :]

    wait_arrived(heads.at[0, other], hm_recv.at[1])
    out_ref[0] = (mixed[...] + project_block(y_far)).astype(BF16)

    wait_sent(heads.at[pl.ds(0, 2 * half_ring - 2), c], h_send.at[0])
    wait_sent(heads.at[0, c], h_send.at[1])
    wait_sent(heads.at[:, c], hm_send.at[0])

    wait_arrived(ret.at[pl.ds(0, (nep - 1) * cap)], b_recv.at[0])
    routed = jnp.zeros((LANES, rows), F32)
    for i in range(2):
        routed += weight[i : i + 1, :] * lax.dot_general(
            ret[...], one_hot(i), (((0,), (0,)), ((), ())), preferred_element_type=F32
        )
    out_ref[1] = routed.T.astype(BF16)

    wait_sent(ans.at[pl.ds(0, (nep - 1) * cap)], b_send.at[0])


def local(
    sizes,
    queries,
    key_rows,
    values,
    second_scale,
    head_gain,
    out_weight,
    routed_in,
    routed_gain,
    expert_ids,
    group_logits,
    inner_logits,
    gate_weight,
    up_weight,
    down_weight,
):
    nz, nx, ny = sizes
    nep = nz * nx
    rows = routed_in.shape[0]
    width = routed_in.shape[1]
    hidden = gate_weight.shape[2]
    cap = 2 * expert_ids.shape[1] * rows // nep
    total = nep * cap
    chunk = total // CHUNKS
    half_ring = ny // 2
    dma = pltpu.SemaphoreType.DMA
    vmem = pltpu.VMEM
    scratch = [
        vmem((width, hidden), BF16),
        vmem((width, hidden), BF16),
        vmem((hidden, width), BF16),
        vmem(out_weight.shape, BF16),
        vmem((rows, width), BF16),
        vmem((1, 1), F32),
        vmem((1, LANES), F32),
        vmem((1, width), F32),
        vmem((2, rows), jnp.int32),
        vmem((group_logits.shape[1], rows), F32),
        vmem((2, rows), F32),
        dma((4,)),
        dma((10,)),
        vmem((8, rows), F32),
        vmem((8, rows), F32),
        vmem((total, LANES), BF16),
        vmem((total, LANES), BF16),
        vmem((ny, 2, total, LANES), BF16),
        vmem((CHUNKS, 2, ny, chunk, LANES), BF16),
        vmem((CHUNKS, ny, chunk, LANES), BF16),
        vmem((CHUNKS, half_ring, chunk, LANES), BF16),
        vmem((CHUNKS, half_ring, chunk, LANES), BF16),
        vmem((CHUNKS, half_ring, chunk, LANES), BF16),
        vmem((CHUNKS, half_ring, chunk, LANES), BF16),
        vmem((total, LANES), BF16),
        vmem((total, LANES), BF16),
        dma((1,)),
        dma((CHUNKS,)),
        dma((1,)),
        dma((CHUNKS,)),
        dma((1,)),
        dma((2, CHUNKS, half_ring - 1)),
        dma((1,)),
        dma((CHUNKS,)),
        dma((1,)),
        dma((CHUNKS,)),
        dma((2,)),
        dma((2, CHUNKS, half_ring)),
        dma((1,)),
        dma((1,)),
        vmem((nx, rows, LANES), BF16),
        vmem((nx, 2 * rows, LANES), BF16),
        vmem((nz, 2, rows, LANES), BF16),
        vmem((nx, LANES, 2 * rows), F32),
        vmem((nx, 1, 4 * rows), F32),
        vmem((nx, LANES, 2 * rows), BF16),
        vmem((nx, LANES, 2 * rows), BF16),
        vmem((nx, 1, 4 * rows), F32),
        vmem((ny, 2, rows, LANES), BF16),
        vmem((rows, LANES), F32),
        dma((1,)),
        dma((1,)),
        dma((nz,)),
        dma((nz,)),
        dma((1,)),
        dma((1,)),
        dma((1,)),
        dma((1,)),
        dma((2,)),
        dma((2, half_ring)),
        dma((1,)),
        dma((2,)),
    ]
    whole = pl.BlockSpec(memory_space=pltpu.VMEM)
    far = pl.BlockSpec(memory_space=pl.ANY)
    both = pl.pallas_call(
        lambda *refs: kernel(sizes, *refs),
        out_shape=pltpu.VMEM((2, rows, LANES), BF16),
        in_specs=[far] * 14,
        out_specs=whole,
        scratch_shapes=scratch,
        compiler_params=pltpu.CompilerParams(
            collective_id=0, has_side_effects=True, vmem_limit_bytes=60 * 1024 * 1024
        ),
    )(
        queries,
        key_rows,
        values,
        second_scale.reshape(1, 1),
        head_gain.reshape(1, -1),
        out_weight,
        routed_in,
        routed_gain.reshape(1, -1),
        expert_ids.T,
        group_logits.T,
        inner_logits.T,
        gate_weight[0],
        up_weight[0],
        down_weight[0],
    )
    return both[0], both[1]


def build(mesh, sizes):
    nz, nx, ny = sizes
    finer = Mesh(mesh.devices.reshape(nz, nx, ny, 2), ("z", "x", "y", "c"))
    ep, tp = ("z", "x"), ("y", "c")
    placed = (
        P(ep, tp),
        P(ep, tp),
        P(ep, tp),
        P(tp),
        P(),
        P(None, tp),
        P(ep, None),
        P(),
        P(ep, None),
        P(ep, None),
        P(ep, None),
        P(ep, None, tp),
        P(ep, None, tp),
        P(ep, tp, None),
    )
    return jax.shard_map(
        lambda *args: local(sizes, *args),
        mesh=finer,
        in_specs=placed,
        out_specs=(P(ep, tp), P(ep, tp)),
        check_vma=False,
    )


def solution(mesh):
    return build(mesh, (8, 4, mesh.shape["tp"] // 2))
```
